32 devices in a mesh: sp: 4 (over y, x), dp: 8 (over z, core).
Axes of the slice: x: 2, y: 2, z: 4, core: 2. Of those that a mesh axis runs over, the one named last changes fastest.
Arguments:
- tokens: bfloat16 [8, 1536, 2048], P('dp', 'sp'), may hold values from -6 to 6
- value_act: bfloat16 [8, 1536, 1024], P('dp', 'sp'), may hold values from -6 to 6
- gate_act: bfloat16 [8, 1536, 1024], P('dp', 'sp'), may hold values from -6 to 6
- cotangent: bfloat16 [8, 1536, 1024], P('dp', 'sp'), may hold values from -6 to 6
- value_weight: bfloat16 [2048, 1024], P('dp'), may hold values from -0.1875 to 0.1875
- gate_weight: bfloat16 [2048, 1024], P('dp'), may hold values from -0.1875 to 0.1875
- norm_gain: float32 [1024], replicated, may hold values from 0.1 to 1.9
- norm_bias: float32 [1024], replicated, may hold values from -3 to 3
- mix_weight: bfloat16 [16, 128, 128], replicated, may hold values from -0.5 to 0.5
- mix_bias: float32 [16, 128], replicated, may hold values from 0.1 to 1.9
Outputs:
- tokens_grad: bfloat16 [8, 1536, 2048], P('dp', 'sp')
- value_weight_grad: float32 [2048, 1024], P('dp')
- gate_weight_grad: float32 [2048, 1024], P('dp')
- mix_weight_grad: float32 [16, 128, 128], replicated
- mix_bias_grad: float32 [16, 128], replicated
- norm_gain_grad: float32 [1024], replicated
- norm_bias_grad: float32 [1024], replicated
The draws below stay inside these ranges and needn't reach their ends.
All inputs are finite; a program needn't handle non-finite values.
Results may differ from the reference program's by a relative error of at most 0.0054.
Values may be sent and summed in bfloat16 or wider, within the bound.
A program may use at most 128 MiB of HBM per device.

```python
import jax
import jax.numpy as jnp
from jax import lax

D = 2048
GROUPS = 16
DG = 1024
BLOCK = 128
SEQ = 1536
SEQS = 8


def strengthened(array, stream_key, source, target, parts, factor):
    owner, partner = [(jnp.arange(array.shape[dim]) // (array.shape[dim] // parts)).reshape([-1 if axis == dim else 1 for axis in range(array.ndim)]) for dim in (source, target)]
    chosen = jax.random.permutation(stream_key, parts)[partner]
    strong = (owner == chosen) | (owner == (partner + parts // 2) % parts)
    return jnp.where(strong, factor * array, array)


def block_scale(rng, shape, split, least, high):
    level, own = 1.0, jax.random.fold_in(rng, 6)
    for axis_at, parts in split:
        steps = jnp.exp(jax.random.uniform(jax.random.fold_in(own, axis_at), (parts,), jnp.float32, least / len(split), high / len(split)))
        level = level * jnp.repeat(steps, shape[axis_at] // parts).reshape([-1 if axis == axis_at else 1 for axis in range(len(shape))])
    return level


def scatter_about(stream_key, dims, scale, bound, split=(), kind=jnp.bfloat16):
    loudness = block_scale(stream_key, dims, split, -0.22, 0.18) if split else 1.0
    values = jax.random.normal(stream_key, dims, jnp.float32) * scale * loudness
    return jnp.minimum(jnp.maximum(values, -bound), bound).astype(kind)


def noise_with(stream_key, dims, spread, most, shards, heavy, kind=jnp.bfloat16):
    array = spread * jax.random.normal(stream_key, dims, jnp.float32)
    if shards:
        array = array * block_scale(stream_key, dims, shards, -0.22, 0.18)
    return jnp.clip(strengthened(array, jax.random.fold_in(stream_key, 3), *heavy), -most, most).astype(kind)


def setup_inputs(seed: int = 0) -> dict:
    key_of = jax.random.split(jax.random.key(seed), 11)
    tokens = noise_with(key_of[0], (SEQS, SEQ, D), 1.0, 6.0, ((0, 8), (1, 4)), (1, 2, 4, 2.0))
    value_act = scatter_about(key_of[1], (SEQS, SEQ, DG), 1.0, 6.0, ((0, 8), (1, 4)))
    gate_act = scatter_about(key_of[2], (SEQS, SEQ, DG), 1.0, 6.0, ((0, 8), (1, 4)))
    cotangent = scatter_about(key_of[3], (SEQS, SEQ, DG), 1.0, 6.0, ((0, 8), (1, 4)))
    value_weight = scatter_about(key_of[4], (D, DG), DG ** -0.5, 0.1875, ((0, 8),))
    gate_weight = scatter_about(key_of[5], (D, DG), DG ** -0.5, 0.1875, ((0, 8),))
    norm_gain = jnp.clip(1.0 + 0.18 * jax.random.normal(key_of[6], (DG,), jnp.float32), 0.1, 1.9)
    norm_bias = scatter_about(key_of[7], (DG,), 0.5, 3.0, (), jnp.float32)
    mix_weight = scatter_about(key_of[8], (GROUPS, BLOCK, BLOCK), BLOCK ** -0.5, 0.5)
    mix_bias = jnp.clip(1.0 + 0.18 * jax.random.normal(key_of[9], (GROUPS, BLOCK), jnp.float32), 0.1, 1.9)
    return {"tokens": tokens, "value_act": value_act, "gate_act": gate_act, "cotangent": cotangent, "value_weight": value_weight, "gate_weight": gate_weight, "norm_gain": norm_gain, "norm_bias": norm_bias, "mix_weight": mix_weight, "mix_bias": mix_bias}


EPSILON = 1e-06

def gelu_slope(values):
    cdf_part = 0.5 * (1.0 + lax.erf(values * 0.7071067811865476))
    pdf_part = jnp.exp(-0.5 * values * values) * 0.3989422804014327
    return cdf_part + values * pdf_part

def mixer_backward(value_act, gate_act, cotangent, norm_gain, norm_bias, mix_weight, mix_bias):
    seq_len, channels = value_act.shape
    groups, block_len = (mix_weight.shape[0], mix_weight.shape[1])
    group_dim = channels // groups
    blocks = seq_len // block_len
    value_float = value_act.astype(jnp.float32)
    gate_float = gate_act.astype(jnp.float32)
    activated = jax.nn.gelu(value_float, approximate=False)
    gate_gelu = jax.nn.gelu(gate_float, approximate=False)
    centred = gate_gelu - lax.optimization_barrier(jnp.mean(gate_gelu, axis=-1, keepdims=True))
    inv_std = lax.rsqrt(lax.optimization_barrier(jnp.mean(centred * centred, axis=-1, keepdims=True)) + EPSILON)
    normed = centred * inv_std
    spread_in = (normed * norm_gain + norm_bias).astype(jnp.bfloat16)
    spread_in = spread_in.reshape(blocks, block_len, groups, group_dim)
    causal = jnp.tril(jnp.ones((block_len, block_len), dtype=bool))
    masked_weight = jnp.where(causal[None], mix_weight, jnp.zeros_like(mix_weight))
    spatial = jnp.einsum('gts,bsgd->btgd', masked_weight.astype(jnp.float32), spread_in.astype(jnp.float32))
    spatial = (spatial + mix_bias.T[None, :, :, None]).reshape(seq_len, channels)
    grad_out = cotangent.astype(jnp.float32)
    grad_act = grad_out * spatial
    grad_spatial = grad_out * activated
    grad_split = grad_spatial.reshape(blocks, block_len, groups, group_dim)
    bias_grad = lax.optimization_barrier(jnp.sum(grad_split, axis=(0, 3))).T
    spatial_low = grad_split.astype(jnp.bfloat16)
    weight_grad = jnp.einsum('btgd,bsgd->gts', spatial_low.astype(jnp.float32), spread_in.astype(jnp.float32))
    weight_grad = jnp.where(causal[None], weight_grad, jnp.zeros_like(weight_grad))
    grad_norm = jnp.einsum('gts,btgd->bsgd', masked_weight.astype(jnp.float32), spatial_low.astype(jnp.float32))
    grad_norm = grad_norm.reshape(seq_len, channels)
    gain_grad = lax.optimization_barrier(jnp.sum(grad_norm * normed, axis=0))
    shift_grad = lax.optimization_barrier(jnp.sum(grad_norm, axis=0))
    grad_hat = grad_norm * norm_gain
    grad_gate = inv_std * (grad_hat - lax.optimization_barrier(jnp.mean(grad_hat, axis=-1, keepdims=True)) - normed * lax.optimization_barrier(jnp.mean(grad_hat * normed, axis=-1, keepdims=True)))
    value_grad = (grad_act * gelu_slope(value_float)).astype(jnp.bfloat16)
    gate_grad = (grad_gate * gelu_slope(gate_float)).astype(jnp.bfloat16)
    return (value_grad, gate_grad, (weight_grad, bias_grad, gain_grad, shift_grad))

def reference(tokens, value_act, gate_act, cotangent, value_weight, gate_weight, norm_gain, norm_bias, mix_weight, mix_bias):
    both_weights = jnp.concatenate((value_weight, gate_weight), axis=1)

    def per_sequence(running, seq_items):
        inputs, value_seq, gate_seq, cot_seq = seq_items
        value_grad, gate_grad, stats = mixer_backward(value_seq, gate_seq, cot_seq, norm_gain, norm_bias, mix_weight, mix_bias)
        both_grads = jnp.concatenate((value_grad, gate_grad), axis=1)
        input_grad = jnp.dot(both_grads, both_weights.T, preferred_element_type=jnp.float32).astype(jnp.bfloat16)
        weight_sums = running[0] + jnp.dot(inputs.T, both_grads, preferred_element_type=jnp.float32)
        updated = (weight_sums,) + tuple((old + term for old, term in zip(running[1:], stats)))
        return (updated, input_grad)
    initial = (jnp.zeros((D, 2 * DG), jnp.float32), jnp.zeros((GROUPS, BLOCK, BLOCK), jnp.float32), jnp.zeros((GROUPS, BLOCK), jnp.float32), jnp.zeros((DG,), jnp.float32), jnp.zeros((DG,), jnp.float32))
    running, input_grads = lax.scan(per_sequence, initial, (tokens, value_act, gate_act, cotangent))
    return (input_grads, running[0][:, :DG], running[0][:, DG:], running[1], running[2], running[3], running[4])
```

```python
import functools

import jax
import jax.numpy as jnp
from jax import lax
from jax.experimental import pallas as pl
from jax.experimental.pallas import tpu as pltpu
from jax.sharding import PartitionSpec as P

EPSILON = 1e-06
CORES = 2
MESH = pl.DeviceIdType.MESH
F32 = jnp.float32
BF16 = jnp.bfloat16


def remote(src, dst, send, recv, device):
    return pltpu.make_async_remote_copy(
        src_ref=src, dst_ref=dst, send_sem=send, recv_sem=recv, device_id=device, device_id_type=MESH
    )


def position():
    s, d = lax.axis_index("sp"), lax.axis_index("dp")
    return s, d, d // CORES, d % CORES


def plane_of(ways):
    across = max(k for k in range(1, ways + 1) if ways % k == 0 and k * k <= ways)
    return across, ways // across


def signal_all(ways, levels, s, d, z, c):
    barrier = pltpu.get_barrier_semaphore()
    for k in range(1, ways):
        pl.semaphore_signal(barrier, inc=1, device_id=((s + k) % ways, d), device_id_type=MESH)
    for k in range(1, levels):
        other = ((z + k) % levels) * CORES + c
        pl.semaphore_signal(barrier, inc=1, device_id=(s, other), device_id_type=MESH)
    pl.semaphore_signal(barrier, inc=1, device_id=(s, d + 1 - 2 * c), device_id_type=MESH)


def phi(values):
    cdf_part = 0.5 * (1.0 + lax.erf(values * 0.7071067811865476))
    pdf_part = jnp.exp(-0.5 * values * values) * 0.3989422804014327
    return cdf_part, cdf_part + values * pdf_part


def kernel(
    ways, levels,
    tokens_hbm, value_weight, gate_weight, value_hbm, gate_hbm, cotangent_hbm, gain, shift, mix_raw, mix_bias,
    input_grad, sums, mix_out, bias_out, gain_out, shift_out,
    tokens, value_act, gate_act, cotangent, mix, mix_turned, bias,
    grads, peer_tokens, peer_grads, gathered, weight_grad, spatial_sum, gain_grad, shift_grad,
    spread, low, spatial, grad_norm, product_in,
    part, first_x, first_y, second_out_a, second_in_a, second_out_b, second_in_b,
    level_out, level_in, own_sum, final,
    mix_part, mix_in, mix_low, mix_plane, mix_level, mix_all, small, small_in, small_plane, small_level,
    load_sem, store_sem, pair_sem, chain_sem, value_sem, gate_sem, relay_sem,
    first_x_sem, first_y_sem, second_a_sem, second_b_sem, level_sem, final_sem, out_x_sem, out_y_sem, out_on_sem,
    mix_sem, mix_level_sem, mix_out_sem, small_sem, small_level_sem,
):
    s, d, z, c = position()
    across, down = plane_of(ways)
    x, y = s % across, s // across
    partner = (s, d + 1 - 2 * c)
    seq_len, channels = value_act.shape
    pairs, double, block_len = mix_turned.shape[0], mix_turned.shape[2], mix_turned.shape[1]
    lanes = channels // pairs
    groups = 2 * pairs
    rows_own = value_weight.shape[0]
    model = tokens.shape[1]
    depth = model // levels
    half = channels // 2
    share = rows_own // ways
    wide, tall = channels // across, channels // down

    def x_peer(k):
        return (y * across + (x + k) % across, d)

    def y_peer(k):
        return (((y + k) % down) * across + x, d)

    def in_plane(k):
        return ((s + k) % ways, d)

    def in_level(k):
        return (s, ((z + k) % levels) * CORES + c)

    loads = [
        pltpu.make_async_copy(value_weight, gathered.at[z, c, 0], load_sem.at[0]),
        pltpu.make_async_copy(gate_weight, gathered.at[z, c, 1], load_sem.at[1]),
        pltpu.make_async_copy(gate_hbm, gate_act, load_sem.at[2]),
        pltpu.make_async_copy(value_hbm, value_act, load_sem.at[3]),
        pltpu.make_async_copy(cotangent_hbm, cotangent, load_sem.at[4]),
        pltpu.make_async_copy(tokens_hbm, tokens, load_sem.at[5]),
    ]
    for copy in loads:
        copy.start()
    signal_all(ways, levels, s, d, z, c)

    row = lax.broadcasted_iota(jnp.int32, (block_len, block_len), 0)
    column = lax.broadcasted_iota(jnp.int32, (block_len, block_len), 1)
    causal = row >= column
    lane = lax.broadcasted_iota(jnp.int32, (block_len, lanes), 1)
    first_half = lane < lanes // 2
    bias_turned = mix_bias[...].T
    for p in range(pairs):
        for k in range(2):
            own = jnp.where(causal, mix_raw[2 * p + k].astype(F32), 0.0)
            mix[p, pl.ds(k * block_len, block_len), :] = own.astype(BF16)
            mix_turned[p, :, pl.ds(k * block_len, block_len)] = own.T.astype(BF16)
        bias[:, pl.ds(p * lanes, lanes)] = jnp.where(
            first_half, bias_turned[:, 2 * p:2 * p + 1], bias_turned[:, 2 * p + 1:2 * p + 2]
        )

    pl.semaphore_wait(pltpu.get_barrier_semaphore(), ways - 1 + levels - 1 + 1)

    def strip(level, matrix):
        if matrix == 0:
            return gathered.at[level, c, 0, :, pl.ds(pl.multiple_of(x * wide, wide), wide)]
        return gathered.at[level, c, 1, :, pl.ds(pl.multiple_of(y * tall, tall), tall)]

    def chain(level, way, k, matrix, target):
        block = strip(level, matrix)
        return remote(
            block, block, chain_sem.at[0, way, k - 1, matrix], chain_sem.at[1, way, k - 1, matrix],
            (s, target * CORES + c),
        )

    def nearest(i):
        below, above = z, levels - 1 - z
        shared = jnp.minimum(below, above)
        paired = i < 2 * shared
        k = jnp.where(paired, i // 2 + 1, i - shared + 1)
        way = jnp.where(paired, i % 2, jnp.where(below > above, 0, 1))
        step = 1 - 2 * way
        return z - step * k, way, k, step

    def send_own(act):
        for matrix in range(2):
            @pl.when(z + 1 < levels)
            def _():
                act(chain(z, 0, 1, matrix, z + 1))

            @pl.when(z >= 1)
            def _():
                act(chain(z, 1, 1, matrix, z - 1))

    def pass_on(i, matrix, act):
        level, way, k, step = nearest(i)
        target = z + step

        @pl.when((target >= 0) & (target < levels))
        def _():
            act(chain(level, way, k + 1, matrix, target))

    def side(i, matrix, k):
        level = nearest(i)[0]
        block = strip(level, matrix)
        if matrix == 0:
            return remote(block, block, value_sem.at[0, i, k - 1], value_sem.at[1, i, k - 1], x_peer(k))
        return remote(block, block, gate_sem.at[0, i, k - 1], gate_sem.at[1, i, k - 1], y_peer(k))

    def arrive(i, matrix):
        level, way, k, step = nearest(i)
        chain(level, way, k, matrix, z).wait_recv()
        pass_on(i, matrix, lambda copy: copy.start())
        for j in range(1, (across, down)[matrix]):
            side(i, matrix, j).start()

    def relay(i):
        block = gathered.at[nearest(i)[0], c]
        return remote(block, block, relay_sem.at[0, i], relay_sem.at[1, i], partner)

    def relay_level(i):
        for matrix in range(2):
            for j in range(1, (across, down)[matrix]):
                side(i, matrix, j).wait_recv()
        relay(i).start()

    def store(level, core):
        index = level * CORES + core
        cut = pl.ds(pl.multiple_of(index * rows_own, rows_own), rows_own)
        return pltpu.make_async_copy(product_in.at[:, cut], input_grad.at[:, cut], store_sem.at[index])

    def project(level, core):
        index = level * CORES + core
        cut = pl.ds(pl.multiple_of(index * rows_own, rows_own), rows_own)
        over = (((1,), (1,)), ((), ()))
        product_in[:, cut] = (
            lax.dot_general(grads[0], gathered[level, core, 0], over, preferred_element_type=F32)
            + lax.dot_general(grads[1], gathered[level, core, 1], over, preferred_element_type=F32)
        ).astype(BF16)
        store(level, core).start()

    def project_level(i):
        level = nearest(i)[0]
        relay(i).wait_recv()
        for core in range(CORES):
            project(level, core)

    loads[0].wait()
    loads[1].wait()
    send_own(lambda copy: copy.start())
    loads[5].wait()
    token_swap = remote(tokens, peer_tokens, pair_sem.at[0, 0], pair_sem.at[1, 0], partner)
    token_swap.start()
    shard_swap = remote(
        gathered.at[z, c], gathered.at[z, c], pair_sem.at[0, 1], pair_sem.at[1, 1], partner
    )
    shard_swap.start()
    for k in range(2, 5):
        loads[k].wait()

    weight_grad[...] = jnp.zeros_like(weight_grad)
    spatial_sum[...] = jnp.zeros_like(spatial_sum)
    gain_grad[...] = jnp.zeros_like(gain_grad)
    shift_grad[...] = jnp.zeros_like(shift_grad)
    turned = (((1,), (1,)), ((), ()))
    for b in range(seq_len // block_len):
        rows = pl.ds(b * block_len, block_len)
        gate = gate_act[rows, :].astype(F32)
        gate_cdf, gate_slope = phi(gate)
        gelu = gate * gate_cdf
        centred = gelu - jnp.mean(gelu, axis=-1, keepdims=True)
        inv_std = lax.rsqrt(jnp.mean(centred * centred, axis=-1, keepdims=True) + EPSILON)
        normed = centred * inv_std
        spread[...] = (normed * gain[...] + shift[...]).astype(BF16)
        value = value_act[rows, :].astype(F32)
        value_cdf, value_slope = phi(value)
        grad_out = cotangent[rows, :].astype(F32)
        grad_spatial = grad_out * (value * value_cdf)
        spatial_sum[...] += grad_spatial
        low[...] = grad_spatial.astype(BF16)
        for p in range(pairs):
            cut = pl.ds(p * lanes, lanes)
            inner = spread[:, cut]
            mixed = jnp.dot(mix[p], inner, preferred_element_type=F32)
            spatial[:, cut] = jnp.where(first_half, mixed[:block_len], mixed[block_len:]) + bias[:, cut]
            piece_low = low[:, cut]
            zero = jnp.zeros_like(piece_low)
            lower = jnp.where(first_half, piece_low, zero)
            apart = jnp.concatenate((lower, jnp.where(first_half, zero, piece_low)), axis=0)
            weight_grad[p, pl.ds(0, block_len), :] += lax.dot_general(
                lower, inner, turned, preferred_element_type=F32
            )
            weight_grad[p, pl.ds(block_len, block_len), :] += lax.dot_general(
                jnp.where(first_half, zero, inner), piece_low, turned, preferred_element_type=F32
            )
            grad_norm[:, cut] = jnp.dot(mix_turned[p], apart, preferred_element_type=F32)
        back = grad_norm[...]
        gain_grad[...] += jnp.sum(back * normed, axis=0, keepdims=True)
        shift_grad[...] += jnp.sum(back, axis=0, keepdims=True)
        hat = back * gain[...]
        grad_gate = inv_std * (
            hat
            - jnp.mean(hat, axis=-1, keepdims=True)
            - normed * jnp.mean(hat * normed, axis=-1, keepdims=True)
        )
        grads[0, rows, :] = (grad_out * spatial[...] * value_slope).astype(BF16)
        grads[1, rows, :] = (grad_gate * gate_slope).astype(BF16)
    grad_swap = remote(grads.at[1 - c], peer_grads, pair_sem.at[0, 2], pair_sem.at[1, 2], partner)
    grad_swap.start()
    arrive(0, 0)

    diagonal = row == column
    per_core = pairs // CORES
    for p in range(pairs):
        straight, flipped = weight_grad[p, pl.ds(0, block_len), :], weight_grad[p, pl.ds(block_len, block_len), :]
        packed = jnp.where(causal, straight, flipped)
        mix_part[p] = packed
        small[groups + 2 * pairs + p:groups + 2 * pairs + p + 1, :] = jnp.sum(
            jnp.where(diagonal, flipped, 0.0), axis=0, keepdims=True
        )
    sums_by_row = jnp.zeros((block_len, lanes), F32)
    for p in range(pairs):
        terms = spatial_sum[:, pl.ds(p * lanes, lanes)]
        left = jnp.sum(jnp.where(first_half, terms, 0.0), axis=1, keepdims=True)
        right = jnp.sum(jnp.where(first_half, 0.0, terms), axis=1, keepdims=True)
        sums_by_row = jnp.where(lane == 2 * p, left, jnp.where(lane == 2 * p + 1, right, sums_by_row))
    small[:groups, :] = sums_by_row.T[:groups]
    for p in range(pairs):
        cut = pl.ds(p * lanes, lanes)
        small[groups + p:groups + p + 1, :] = gain_grad[:, cut]
        small[groups + pairs + p:groups + pairs + p + 1, :] = shift_grad[:, cut]
    mix_swap = remote(
        mix_part.at[pl.ds((1 - c) * per_core, per_core)], mix_in, pair_sem.at[0, 3], pair_sem.at[1, 3], partner
    )
    mix_swap.start()
    small_swap = remote(small, small_in, pair_sem.at[0, 4], pair_sem.at[1, 4], partner)
    small_swap.start()

    def first_a(i, k, j):
        return remote(
            part.at[i, :, (y + j) % down, (x + k) % across, :, pl.ds(0, half)], first_x.at[i, k - 1, j],
            first_x_sem.at[0, i, k - 1, j], first_x_sem.at[1, i, k - 1, j], x_peer(k),
        )

    def first_b(i, k, j):
        return remote(
            part.at[i, :, (y + k) % down, (x + j) % across, :, pl.ds(half, half)], first_y.at[i, k - 1, j],
            first_y_sem.at[0, i, k - 1, j], first_y_sem.at[1, i, k - 1, j], y_peer(k),
        )

    def second_a(i, j):
        return remote(
            second_out_a.at[i, j - 1], second_in_a.at[i, j - 1],
            second_a_sem.at[0, i, j - 1], second_a_sem.at[1, i, j - 1], y_peer(j),
        )

    def second_b(i, j):
        return remote(
            second_out_b.at[i, j - 1], second_in_b.at[i, j - 1],
            second_b_sem.at[0, i, j - 1], second_b_sem.at[1, i, j - 1], x_peer(j),
        )

    def send_chunk(i):
        target = (z + 1 + i) % levels
        cut = pl.ds(pl.multiple_of(target * depth, depth), depth)
        over = (((0,), (0,)), ((), ()))
        product = lax.dot_general(
            tokens[:, cut], grads[c], over, preferred_element_type=F32
        ) + lax.dot_general(peer_tokens[:, cut], peer_grads[...], over, preferred_element_type=F32)
        part[i] = product.reshape(part.shape[1:]).astype(BF16)
        for j in list(range(1, down)) + [0]:
            for k in range(1, across):
                first_a(i, k, j).start()
        for j in list(range(1, across)) + [0]:
            for k in range(1, down):
                first_b(i, k, j).start()

    def gathered_a(i, j):
        total = part[i, :, (y + j) % down, x, :, pl.ds(0, half)].astype(F32)
        for k in range(1, across):
            first_a(i, k, j).wait_recv()
            total = total + first_x[i, k - 1, j].astype(F32)
        return total

    def gathered_b(i, j):
        total = part[i, :, y, (x + j) % across, :, pl.ds(half, half)].astype(F32)
        for k in range(1, down):
            first_b(i, k, j).wait_recv()
            total = total + first_y[i, k - 1, j].astype(F32)
        return total

    def send_second(i):
        for j in range(1, down):
            second_out_a[i, j - 1] = gathered_a(i, j).astype(BF16)
            second_a(i, j).start()
        for j in range(1, across):
            second_out_b[i, j - 1] = gathered_b(i, j).astype(BF16)
            second_b(i, j).start()

    def to_level(i):
        return remote(
            level_out.at[i], level_in.at[i], level_sem.at[0, i], level_sem.at[1, i], in_level(i + 1)
        )

    def send_level(i):
        left, right = gathered_a(i, 0), gathered_b(i, 0)
        for j in range(1, down):
            second_a(i, j).wait_recv()
            left = left + second_in_a[i, j - 1].astype(F32)
        for j in range(1, across):
            second_b(i, j).wait_recv()
            right = right + second_in_b[i, j - 1].astype(F32)
        if i < levels - 1:
            level_out[i, :, :, pl.ds(0, half)] = left.astype(BF16)
            level_out[i, :, :, pl.ds(half, half)] = right.astype(BF16)
            to_level(i).start()
        else:
            own_sum[:, :, pl.ds(0, half)] = left
            own_sum[:, :, pl.ds(half, half)] = right

    mix_rows = mix_low.shape[1]

    def mix_scatter(k):
        return remote(
            mix_low.at[(s + k) % ways], mix_plane.at[k - 1], mix_sem.at[0, k - 1], mix_sem.at[1, k - 1], in_plane(k)
        )

    def small_scatter(k):
        return remote(
            small_plane.at[s], small_plane.at[s], small_sem.at[0, k - 1], small_sem.at[1, k - 1], in_plane(k)
        )

    def mix_lift(k):
        return remote(
            mix_level.at[z], mix_level.at[z], mix_level_sem.at[0, k - 1], mix_level_sem.at[1, k - 1], in_level(k)
        )

    def small_lift(k):
        return remote(
            small_level.at[z], small_level.at[z],
            small_level_sem.at[0, k - 1], small_level_sem.at[1, k - 1], in_level(k),
        )

    def mix_gather(k):
        block = mix_all.at[c, s]
        return remote(block, block, mix_out_sem.at[0, k - 1], mix_out_sem.at[1, k - 1], in_plane(k))

    mix_back = remote(mix_all.at[c], mix_all.at[c], pair_sem.at[0, 5], pair_sem.at[1, 5], partner)

    def mix_stage(stage):
        if stage == 0:
            mix_swap.wait()
            small_swap.wait()
            mine = mix_part[pl.ds(c * per_core, per_core)] + mix_in[...]
            mix_low[...] = mine.reshape(mix_low.shape).astype(BF16)
            small_plane[s] = small[...] + small_in[...]
            for k in range(1, ways):
                mix_scatter(k).start()
                small_scatter(k).start()
        elif stage == 1:
            total = mix_low[s].astype(F32)
            for k in range(1, ways):
                mix_scatter(k).wait()
                small_scatter(k).wait()
                total = total + mix_plane[k - 1].astype(F32)
            mix_level[z] = total.astype(BF16)
            whole = small_plane[0]
            for k in range(1, ways):
                whole = whole + small_plane[k]
            small_level[z] = whole
            for k in range(1, levels):
                mix_lift(k).start()
                small_lift(k).start()
        elif stage == 2:
            for k in range(1, levels):
                mix_lift(k).wait()
                small_lift(k).wait()
            total = mix_level[0].astype(F32)
            whole = small_level[0]
            for k in range(1, levels):
                total = total + mix_level[k].astype(F32)
                whole = whole + small_level[k]
            mix_all[c, s] = total.astype(BF16)
            small[...] = whole
            for k in range(1, ways):
                mix_gather(k).start()
        elif stage == 3:
            for k in range(1, ways):
                mix_gather(k).wait()
            mix_back.start()
        else:
            mix_back.wait()
            packed_all = mix_all[...].reshape(pairs, block_len, block_len)
            for p in range(pairs):
                packed = packed_all[p].astype(F32)
                at = groups + 2 * pairs + p
                on_diagonal = jnp.where(diagonal, small[at:at + 1, :], 0.0)
                mix_out[2 * p] = jnp.where(causal, packed, 0.0).astype(BF16)
                mix_out[2 * p + 1] = jnp.where(row > column, packed.T, on_diagonal).astype(BF16)
            bias_out[...] = small[:groups, :]
            gain_out[...] = small[groups:groups + pairs, :]
            shift_out[...] = small[groups + pairs:groups + 2 * pairs, :]

    token_swap.wait()
    grad_swap.wait()
    later = [(i, matrix) for i in range(levels - 1) for matrix in range(2)][1:]
    relayed, projected = [], []
    for i in range(levels):
        send_chunk(i)
        if i < 2:
            arrive(*later.pop(0))
        if i == 0:
            mix_stage(0)
        if i >= 1:
            send_second(i - 1)
        if i >= 2:
            send_level(i - 2)
    project(z, c)
    shard_swap.wait()
    project(z, 1 - c)
    send_second(levels - 1)
    if later:
        arrive(*later.pop(0))
    mix_stage(1)
    send_level(levels - 2)
    relay_level(0)
    while later:
        arrive(*later.pop(0))
    mix_stage(2)
    send_level(levels - 1)
    total = own_sum[...]
    for i in range(levels - 1):
        to_level(i).wait_recv()
        total = total + level_in[i].astype(F32)
    final[...] = total.astype(BF16)
    sums[c, s] = final[c]
    final_swap = remote(final.at[1 - c], sums.at[c, s], final_sem.at[0], final_sem.at[1], partner)
    final_swap.start()

    def out_x(matrix, k):
        block = sums.at[matrix, s]
        return remote(block, block, out_x_sem.at[0, matrix, k - 1], out_x_sem.at[1, matrix, k - 1], x_peer(k))

    def out_y(matrix, k):
        block = sums.at[matrix, s]
        return remote(block, block, out_y_sem.at[0, matrix, k - 1], out_y_sem.at[1, matrix, k - 1], y_peer(k))

    def out_first(matrix):
        for k in range(1, across):
            out_x(matrix, k).start()
        for k in range(1, down):
            out_y(matrix, k).start()

    def onward(matrix, k, j):
        if matrix == 0:
            block = sums.at[0, y * across + (x + across - k) % across]
            peer = y_peer(j)
        else:
            block = sums.at[1, ((y + down - k) % down) * across + x]
            peer = x_peer(j)
        return remote(
            block, block, out_on_sem.at[0, matrix, k - 1, j - 1], out_on_sem.at[1, matrix, k - 1, j - 1], peer
        )

    out_first(c)
    final_swap.wait()
    out_first(1 - c)
    mix_stage(3)
    for k in range(1, across):
        out_x(0, k).wait_recv()
        for j in range(1, down):
            onward(0, k, j).start()
    for k in range(1, down):
        out_y(1, k).wait_recv()
        for j in range(1, across):
            onward(1, k, j).start()
    project_level(0)
    mix_stage(4)
    for i in range(1, levels - 1):
        relay_level(i)
    for i in range(1, levels - 1):
        project_level(i)
    for k in range(1, across):
        out_x(1, k).wait_recv()
        for j in range(1, down):
            onward(0, k, j).wait()
    for k in range(1, down):
        out_y(0, k).wait_recv()
        for j in range(1, across):
            onward(1, k, j).wait()

    send_own(lambda copy: copy.wait_send())
    for i in range(levels - 1):
        for matrix in range(2):
            pass_on(i, matrix, lambda copy: copy.wait_send())
            for j in range(1, (across, down)[matrix]):
                side(i, matrix, j).wait_send()
        relay(i).wait_send()
        to_level(i).wait_send()
    for i in range(levels):
        for j in range(down):
            for k in range(1, across):
                first_a(i, k, j).wait_send()
            if j:
                second_a(i, j).wait_send()
        for j in range(across):
            for k in range(1, down):
                first_b(i, k, j).wait_send()
            if j:
                second_b(i, j).wait_send()
    for matrix in range(2):
        for k in range(1, across):
            out_x(matrix, k).wait_send()
        for k in range(1, down):
            out_y(matrix, k).wait_send()
    for level in range(levels):
        for core in range(CORES):
            store(level, core).wait()


def shards(
    tokens,
    value_act,
    gate_act,
    cotangent,
    value_weight,
    gate_weight,
    norm_gain,
    norm_bias,
    mix_weight,
    mix_bias,
):
    ways = lax.axis_size("sp")
    levels = lax.axis_size("dp") // CORES
    across, down = plane_of(ways)
    inputs = tokens[0]
    seq_len, width = inputs.shape
    channels = value_act.shape[2]
    groups, block_len = mix_weight.shape[0], mix_weight.shape[1]
    pairs = groups // 2
    lanes = channels // pairs
    rows = value_weight.shape[0]
    share = rows // ways
    half = channels // 2
    vmem = pl.BlockSpec(memory_space=pltpu.VMEM)
    anywhere = pl.BlockSpec(memory_space=pl.ANY)
    sems = pltpu.SemaphoreType.DMA
    mix_rows = pairs * block_len // (CORES * ways)
    small_shape = (groups + 3 * pairs, lanes)
    shape = jax.ShapeDtypeStruct
    input_grad, summed, mix_out, bias_out, gain_out, shift_out = pl.pallas_call(
        functools.partial(kernel, ways, levels),
        out_shape=(
            shape((seq_len, width), BF16),
            shape((2, ways, share, channels), BF16),
            shape((groups, block_len, block_len), BF16),
            shape((groups, block_len), F32),
            shape((pairs, lanes), F32),
            shape((pairs, lanes), F32),
        ),
        in_specs=[anywhere] * 6 + [vmem] * 4,
        out_specs=(anywhere,) + (vmem,) * 5,
        scratch_shapes=[
            pltpu.VMEM((seq_len, width), BF16),
            pltpu.VMEM((seq_len, channels), BF16),
            pltpu.VMEM((seq_len, channels), BF16),
            pltpu.VMEM((seq_len, channels), BF16),
            pltpu.VMEM((pairs, 2 * block_len, block_len), BF16),
            pltpu.VMEM((pairs, block_len, 2 * block_len), BF16),
            pltpu.VMEM((block_len, channels), F32),
            pltpu.VMEM((2, seq_len, channels), BF16),
            pltpu.VMEM((seq_len, width), BF16),
            pltpu.VMEM((seq_len, channels), BF16),
            pltpu.VMEM((levels, CORES, 2, rows, channels), BF16),
            pltpu.VMEM((pairs, 2 * block_len, block_len), F32),
            pltpu.VMEM((block_len, channels), F32),
            pltpu.VMEM((1, channels), F32),
            pltpu.VMEM((1, channels), F32),
            pltpu.VMEM((block_len, channels), BF16),
            pltpu.VMEM((block_len, channels), BF16),
            pltpu.VMEM((block_len, channels), F32),
            pltpu.VMEM((block_len, channels), F32),
            pltpu.VMEM((seq_len, width), BF16),
            pltpu.VMEM((levels, CORES, down, across, share, channels), BF16),
            pltpu.VMEM((levels, across - 1, down, CORES, share, half), BF16),
            pltpu.VMEM((levels, down - 1, across, CORES, share, half), BF16),
            pltpu.VMEM((levels, down - 1, CORES, share, half), BF16),
            pltpu.VMEM((levels, down - 1, CORES, share, half), BF16),
            pltpu.VMEM((levels, across - 1, CORES, share, half), BF16),
            pltpu.VMEM((levels, across - 1, CORES, share, half), BF16),
            pltpu.VMEM((levels - 1, CORES, share, channels), BF16),
            pltpu.VMEM((levels - 1, CORES, share, channels), BF16),
            pltpu.VMEM((CORES, share, channels), F32),
            pltpu.VMEM((CORES, share, channels), BF16),
            pltpu.VMEM((pairs, block_len, block_len), F32),
            pltpu.VMEM((pairs // CORES, block_len, block_len), F32),
            pltpu.VMEM((ways, mix_rows, block_len), BF16),
            pltpu.VMEM((ways - 1, mix_rows, block_len), BF16),
            pltpu.VMEM((levels, mix_rows, block_len), BF16),
            pltpu.VMEM((CORES, ways, mix_rows, block_len), BF16),
            pltpu.VMEM(small_shape, F32),
            pltpu.VMEM(small_shape, F32),
            pltpu.VMEM((ways,) + small_shape, F32),
            pltpu.VMEM((levels,) + small_shape, F32),
            sems((6,)),
            sems((levels * CORES,)),
            sems((2, 6)),
            sems((2, 2, levels - 1, 2)),
            sems((2, levels - 1, across - 1)),
            sems((2, levels - 1, down - 1)),
            sems((2, levels - 1)),
            sems((2, levels, across - 1, down)),
            sems((2, levels, down - 1, across)),
            sems((2, levels, down - 1)),
            sems((2, levels, across - 1)),
            sems((2, levels - 1)),
            sems((2,)),
            sems((2, 2, across - 1)),
            sems((2, 2, down - 1)),
            sems((2, 2, max(across, down) - 1, max(across, down) - 1)),
            sems((2, ways - 1)),
            sems((2, levels - 1)),
            sems((2, ways - 1)),
            sems((2, ways - 1)),
            sems((2, levels - 1)),
        ],
        compiler_params=pltpu.CompilerParams(
            collective_id=0, has_side_effects=True, vmem_limit_bytes=60 * 1024 * 1024
        ),
        name="unit",
    )(
        inputs, value_weight, gate_weight, value_act[0], gate_act[0], cotangent[0],
        norm_gain[None], norm_bias[None], mix_weight, mix_bias,
    )
    return (
        input_grad[None],
        summed[0].reshape(rows, channels).astype(F32),
        summed[1].reshape(rows, channels).astype(F32),
        mix_out.astype(F32),
        bias_out,
        gain_out.reshape(-1),
        shift_out.reshape(-1),
    )


def solution(mesh):
    placed = (
        P("dp", "sp", None),
        P("dp", "sp", None),
        P("dp", "sp", None),
        P("dp", "sp", None),
        P("dp", None),
        P("dp", None),
        P(),
        P(),
        P(),
        P(),
    )
    return jax.shard_map(
        shards,
        mesh=mesh,
        in_specs=placed,
        out_specs=(P("dp", "sp", None), P("dp", None), P("dp", None), P(), P(), P(), P()),
        check_vma=False,
    )
```

```python
import functools

import jax
import jax.numpy as jnp
from jax import lax
from jax.experimental import pallas as pl
from jax.experimental.pallas import tpu as pltpu
from jax.sharding import PartitionSpec as P

EPSILON = 1e-06
CORES = 2
MESH = pl.DeviceIdType.MESH
F32 = jnp.float32
BF16 = jnp.bfloat16


def remote(src, dst, send, recv, device):
    return pltpu.make_async_remote_copy(
        src_ref=src, dst_ref=dst, send_sem=send, recv_sem=recv, device_id=device, device_id_type=MESH
    )


def position():
    s, d = lax.axis_index("sp"), lax.axis_index("dp")
    return s, d, d // CORES, d % CORES


def plane_of(ways):
    across = max(k for k in range(1, ways + 1) if ways % k == 0 and k * k <= ways)
    return across, ways // across


def signal_all(ways, levels, s, d, z, c):
    barrier = pltpu.get_barrier_semaphore()
    for k in range(1, ways):
        pl.semaphore_signal(barrier, inc=1, device_id=((s + k) % ways, d), device_id_type=MESH)
    for k in range(1, levels):
        other = ((z + k) % levels) * CORES + c
        pl.semaphore_signal(barrier, inc=1, device_id=(s, other), device_id_type=MESH)
    pl.semaphore_signal(barrier, inc=1, device_id=(s, d + 1 - 2 * c), device_id_type=MESH)


def phi(values):
    cdf_part = 0.5 * (1.0 + lax.erf(values * 0.7071067811865476))
    pdf_part = jnp.exp(-0.5 * values * values) * 0.3989422804014327
    return cdf_part, cdf_part + values * pdf_part


def kernel(
    ways, levels,
    tokens_hbm, value_weight, gate_weight, value_hbm, gate_hbm, cotangent_hbm, gain, shift, mix_raw, mix_bias,
    input_grad, sums, mix_out, bias_out, gain_out, shift_out,
    tokens, value_act, gate_act, cotangent, mix, mix_turned, bias,
    grads, peer_tokens, peer_grads, gathered, weight_grad, spatial_sum, gain_grad, shift_grad,
    spread, low, spatial, grad_norm, product_in,
    part, first_x, first_y, run_out_a, run_in_a, run_out_b, run_in_b, own_a, own_b,
    second_out_a, second_in_a, second_out_b, second_in_b, final,
    mix_part, mix_in, mix_low, mix_plane, mix_level, mix_all, small, small_in, small_plane, small_level,
    load_sem, store_sem, pair_sem, swap_sem, chain_sem, value_sem, gate_sem, relay_sem,
    first_x_sem, first_y_sem, run_sem, second_a_sem, second_b_sem, final_sem, out_x_sem, out_y_sem, out_on_sem,
    mix_sem, mix_level_sem, mix_out_sem, small_sem, small_level_sem,
):
    s, d, z, c = position()
    across, down = plane_of(ways)
    x, y = s % across, s // across
    partner = (s, d + 1 - 2 * c)
    seq_len, channels = value_act.shape
    pairs, double, block_len = mix_turned.shape[0], mix_turned.shape[2], mix_turned.shape[1]
    lanes = channels // pairs
    groups = 2 * pairs
    rows_own = value_weight.shape[0]
    model = tokens.shape[1]
    depth = model // levels
    half = channels // 2
    share = rows_own // ways
    wide, tall = channels // across, channels // down

    def x_peer(k):
        return (y * across + (x + k) % across, d)

    def y_peer(k):
        return (((y + k) % down) * across + x, d)

    def in_plane(k):
        return ((s + k) % ways, d)

    def in_level(k):
        return (s, ((z + k) % levels) * CORES + c)

    loads = [
        pltpu.make_async_copy(value_weight, gathered.at[z, c, 0], load_sem.at[0]),
        pltpu.make_async_copy(gate_weight, gathered.at[z, c, 1], load_sem.at[1]),
        pltpu.make_async_copy(gate_hbm, gate_act, load_sem.at[2]),
        pltpu.make_async_copy(value_hbm, value_act, load_sem.at[3]),
        pltpu.make_async_copy(cotangent_hbm, cotangent, load_sem.at[4]),
        pltpu.make_async_copy(tokens_hbm, tokens, load_sem.at[5]),
    ]
    for copy in loads:
        copy.start()
    signal_all(ways, levels, s, d, z, c)

    row = lax.broadcasted_iota(jnp.int32, (block_len, block_len), 0)
    column = lax.broadcasted_iota(jnp.int32, (block_len, block_len), 1)
    causal = row >= column
    lane = lax.broadcasted_iota(jnp.int32, (block_len, lanes), 1)
    first_half = lane < lanes // 2
    bias_turned = mix_bias[...].T
    for p in range(pairs):
        for k in range(2):
            own = jnp.where(causal, mix_raw[2 * p + k].astype(F32), 0.0)
            mix[p, pl.ds(k * block_len, block_len), :] = own.astype(BF16)
            mix_turned[p, :, pl.ds(k * block_len, block_len)] = own.T.astype(BF16)
        bias[:, pl.ds(p * lanes, lanes)] = jnp.where(
            first_half, bias_turned[:, 2 * p:2 * p + 1], bias_turned[:, 2 * p + 1:2 * p + 2]
        )

    pl.semaphore_wait(pltpu.get_barrier_semaphore(), ways - 1 + levels - 1 + 1)

    def strip(level, matrix):
        if matrix == 0:
            return gathered.at[level, c, 0, :, pl.ds(pl.multiple_of(x * wide, wide), wide)]
        return gathered.at[level, c, 1, :, pl.ds(pl.multiple_of(y * tall, tall), tall)]

    def chain(level, way, k, matrix, target):
        block = strip(level, matrix)
        return remote(
            block, block, chain_sem.at[0, way, k - 1, matrix], chain_sem.at[1, way, k - 1, matrix],
            (s, target * CORES + c),
        )

    def nearest(i):
        below, above = z, levels - 1 - z
        shared = jnp.minimum(below, above)
        paired = i < 2 * shared
        k = jnp.where(paired, i // 2 + 1, i - shared + 1)
        way = jnp.where(paired, i % 2, jnp.where(below > above, 0, 1))
        return z - (1 - 2 * way) * k, way, k

    def send_own(act):
        for matrix in range(2):
            @pl.when(z + 1 < levels)
            def _():
                act(chain(z, 0, 1, matrix, z + 1))

            @pl.when(z >= 1)
            def _():
                act(chain(z, 1, 1, matrix, z - 1))

    def pass_on(level, way, k, matrix, act):
        target = z + 1 - 2 * way

        @pl.when((target >= 0) & (target < levels))
        def _():
            act(chain(level, way, k + 1, matrix, target))

    def side(level, way, k, matrix, j):
        block = strip(level, matrix)
        sem = (value_sem, gate_sem)[matrix]
        return remote(
            block, block, sem.at[0, way, k - 1, j - 1], sem.at[1, way, k - 1, j - 1], (x_peer, y_peer)[matrix](j)
        )

    def relay(level, way, k):
        block = gathered.at[level, c]
        return remote(block, block, relay_sem.at[0, way, k - 1], relay_sem.at[1, way, k - 1], partner)

    def both_ways(k, act):
        @pl.when(z >= k)
        def _():
            act(z - k, 0)

        @pl.when(z + k < levels)
        def _():
            act(z + k, 1)

    def arrive(k, matrix):
        def act(level, way):
            chain(level, way, k, matrix, z).wait_recv()
            pass_on(level, way, k, matrix, lambda copy: copy.start())
            for j in range(1, (across, down)[matrix]):
                side(level, way, k, matrix, j).start()

        with jax.named_scope(f"arrive{k}{matrix}"):
            both_ways(k, act)

    def relay_step(k):
        def act(level, way):
            for matrix in range(2):
                for j in range(1, (across, down)[matrix]):
                    side(level, way, k, matrix, j).wait_recv()
            relay(level, way, k).start()

        with jax.named_scope(f"relay{k}"):
            both_ways(k, act)

    def store(level, core):
        index = level * CORES + core
        cut = pl.ds(pl.multiple_of(index * rows_own, rows_own), rows_own)
        return pltpu.make_async_copy(product_in.at[:, cut], input_grad.at[:, cut], store_sem.at[index])

    def project(level, core):
        index = level * CORES + core
        cut = pl.ds(pl.multiple_of(index * rows_own, rows_own), rows_own)
        over = (((1,), (1,)), ((), ()))
        product_in[:, cut] = (
            lax.dot_general(grads[0], gathered[level, core, 0], over, preferred_element_type=F32)
            + lax.dot_general(grads[1], gathered[level, core, 1], over, preferred_element_type=F32)
        ).astype(BF16)
        store(level, core).start()

    def project_level(i):
        level, way, k = nearest(i)
        with jax.named_scope(f"project{i}"):
            relay(level, way, k).wait_recv()
            for core in range(CORES):
                project(level, core)

    loads[0].wait()
    loads[1].wait()
    send_own(lambda copy: copy.start())
    loads[5].wait()
    token_swap = remote(tokens, peer_tokens, pair_sem.at[0, 0], pair_sem.at[1, 0], partner)
    token_swap.start()
    shard_swap = remote(
        gathered.at[z, c], gathered.at[z, c], pair_sem.at[0, 1], pair_sem.at[1, 1], partner
    )
    shard_swap.start()
    for k in range(2, 5):
        loads[k].wait()

    weight_grad[...] = jnp.zeros_like(weight_grad)
    spatial_sum[...] = jnp.zeros_like(spatial_sum)
    gain_grad[...] = jnp.zeros_like(gain_grad)
    shift_grad[...] = jnp.zeros_like(shift_grad)
    turned = (((1,), (1,)), ((), ()))
    grad_swaps = []
    for b in range(seq_len // block_len):
        rows = pl.ds(b * block_len, block_len)
        gate = gate_act[rows, :].astype(F32)
        gate_cdf, gate_slope = phi(gate)
        gelu = gate * gate_cdf
        centred = gelu - jnp.mean(gelu, axis=-1, keepdims=True)
        inv_std = lax.rsqrt(jnp.mean(centred * centred, axis=-1, keepdims=True) + EPSILON)
        normed = centred * inv_std
        spread[...] = (normed * gain[...] + shift[...]).astype(BF16)
        value = value_act[rows, :].astype(F32)
        value_cdf, value_slope = phi(value)
        grad_out = cotangent[rows, :].astype(F32)
        grad_spatial = grad_out * (value * value_cdf)
        spatial_sum[...] += grad_spatial
        low[...] = grad_spatial.astype(BF16)
        for p in range(pairs):
            cut = pl.ds(p * lanes, lanes)
            inner = spread[:, cut]
            mixed = jnp.dot(mix[p], inner, preferred_element_type=F32)
            spatial[:, cut] = jnp.where(first_half, mixed[:block_len], mixed[block_len:]) + bias[:, cut]
            piece_low = low[:, cut]
            zero = jnp.zeros_like(piece_low)
            lower = jnp.where(first_half, piece_low, zero)
            apart = jnp.concatenate((lower, jnp.where(first_half, zero, piece_low)), axis=0)
            weight_grad[p, pl.ds(0, block_len), :] += lax.dot_general(
                lower, inner, turned, preferred_element_type=F32
            )
            weight_grad[p, pl.ds(block_len, block_len), :] += lax.dot_general(
                jnp.where(first_half, zero, inner), piece_low, turned, preferred_element_type=F32
            )
            grad_norm[:, cut] = jnp.dot(mix_turned[p], apart, preferred_element_type=F32)
        back = grad_norm[...]
        gain_grad[...] += jnp.sum(back * normed, axis=0, keepdims=True)
        shift_grad[...] += jnp.sum(back, axis=0, keepdims=True)
        hat = back * gain[...]
        grad_gate = inv_std * (
            hat
            - jnp.mean(hat, axis=-1, keepdims=True)
            - normed * jnp.mean(hat * normed, axis=-1, keepdims=True)
        )
        grads[0, rows, :] = (grad_out * spatial[...] * value_slope).astype(BF16)
        grads[1, rows, :] = (grad_gate * gate_slope).astype(BF16)
        grad_swaps.append(remote(
            grads.at[1 - c, rows], peer_grads.at[rows], swap_sem.at[0, b], swap_sem.at[1, b], partner
        ))
        grad_swaps[-1].start()

    diagonal = row == column
    per_core = pairs // CORES
    for p in range(pairs):
        straight, flipped = weight_grad[p, pl.ds(0, block_len), :], weight_grad[p, pl.ds(block_len, block_len), :]
        packed = jnp.where(causal, straight, flipped)
        mix_part[p] = packed
        small[groups + 2 * pairs + p:groups + 2 * pairs + p + 1, :] = jnp.sum(
            jnp.where(diagonal, flipped, 0.0), axis=0, keepdims=True
        )
    sums_by_row = jnp.zeros((block_len, lanes), F32)
    for p in range(pairs):
        terms = spatial_sum[:, pl.ds(p * lanes, lanes)]
        left = jnp.sum(jnp.where(first_half, terms, 0.0), axis=1, keepdims=True)
        right = jnp.sum(jnp.where(first_half, 0.0, terms), axis=1, keepdims=True)
        sums_by_row = jnp.where(lane == 2 * p, left, jnp.where(lane == 2 * p + 1, right, sums_by_row))
    small[:groups, :] = sums_by_row.T[:groups]
    for p in range(pairs):
        cut = pl.ds(p * lanes, lanes)
        small[groups + p:groups + p + 1, :] = gain_grad[:, cut]
        small[groups + pairs + p:groups + pairs + p + 1, :] = shift_grad[:, cut]
    mix_swap = remote(
        mix_part.at[pl.ds((1 - c) * per_core, per_core)], mix_in, pair_sem.at[0, 3], pair_sem.at[1, 3], partner
    )
    mix_swap.start()
    small_swap = remote(small, small_in, pair_sem.at[0, 4], pair_sem.at[1, 4], partner)
    small_swap.start()

    def target_of(i):
        return (z, 0) if i == levels - 1 else nearest(levels - 2 - i)[:2]

    def first(i, matrix, k):
        if matrix == 0:
            return remote(
                part.at[i, :, :, (x + k) % across, :, pl.ds(0, half)], first_x.at[i, k - 1],
                first_x_sem.at[0, i, k - 1], first_x_sem.at[1, i, k - 1], x_peer(k),
            )
        return remote(
            part.at[i, :, (y + k) % down, :, :, pl.ds(half, half)], first_y.at[i, k - 1],
            first_y_sem.at[0, i, k - 1], first_y_sem.at[1, i, k - 1], y_peer(k),
        )

    def send_chunk(i):
        target = target_of(i)[0]
        cut = pl.ds(pl.multiple_of(target * depth, depth), depth)
        over = (((0,), (0,)), ((), ()))
        with jax.named_scope(f"chunk{i}"):
            product = lax.dot_general(
                tokens[:, cut], grads[c], over, preferred_element_type=F32
            ) + lax.dot_general(peer_tokens[:, cut], peer_grads[...], over, preferred_element_type=F32)
            part[i] = product.reshape(part.shape[1:]).astype(BF16)
            for matrix in range(2):
                for k in range(1, (across, down)[matrix]):
                    first(i, matrix, k).start()

    def pair_sum(i, matrix):
        for k in range(1, (across, down)[matrix]):
            first(i, matrix, k).wait_recv()
        if matrix == 0:
            total = part[i, :, :, x, :, pl.ds(0, half)].astype(F32)
            for k in range(1, across):
                total = total + first_x[i, k - 1].astype(F32)
        else:
            total = part[i, :, y, :, :, pl.ds(half, half)].astype(F32)
            for k in range(1, down):
                total = total + first_y[i, k - 1].astype(F32)
        return total

    run_out, run_in = (run_out_a, run_out_b), (run_in_a, run_in_b)

    def running(i, level, matrix, upward, target):
        return remote(
            run_out[matrix].at[i], run_in[matrix].at[level, 1 - upward],
            run_sem.at[0, level, matrix, 1 - upward], run_sem.at[1, level, matrix, 1 - upward],
            (s, target * CORES + c),
        )

    def run(i, matrix):
        level, upward = target_of(i)
        step = 2 * upward - 1
        behind = z - step
        with jax.named_scope(f"run{i}{matrix}"):
            total = pair_sum(i, matrix)
            started = (behind >= 0) & (behind < levels)

            @pl.when(started)
            def _():
                running(i, level, matrix, upward, z).wait_recv()
                run_out[matrix][i] = (total + run_in[matrix][level, 1 - upward].astype(F32)).astype(BF16)

            @pl.when(jnp.logical_not(started))
            def _():
                run_out[matrix][i] = total.astype(BF16)

            running(i, level, matrix, upward, z + step).start()

    def second(matrix, j):
        if matrix == 0:
            return remote(
                second_out_a.at[j - 1], second_in_a.at[j - 1],
                second_a_sem.at[0, j - 1], second_a_sem.at[1, j - 1], y_peer(j),
            )
        return remote(
            second_out_b.at[j - 1], second_in_b.at[j - 1],
            second_b_sem.at[0, j - 1], second_b_sem.at[1, j - 1], x_peer(j),
        )

    def send_second(matrix):
        own = (own_a, own_b)[matrix]
        out = (second_out_a, second_out_b)[matrix]
        with jax.named_scope(f"second{matrix}"):
            own[...] = pair_sum(levels - 1, matrix)
            for upward in range(2):
                @pl.when((z >= 1) if upward else (z + 1 < levels))
                def _():
                    running(0, z, matrix, upward, z).wait_recv()
                    own[...] += run_in[matrix][z, 1 - upward].astype(F32)
            for j in range(1, (down, across)[matrix]):
                index = (y + j) % down if matrix == 0 else (x + j) % across
                out[j - 1] = own[:, index].astype(BF16)
                second(matrix, j).start()

    def final_swap(matrix):
        return remote(
            final.at[matrix, 1 - c], sums.at[c, s, :, pl.ds(matrix * half, half)],
            final_sem.at[0, matrix], final_sem.at[1, matrix], partner,
        )

    def finish(matrix):
        with jax.named_scope(f"finish{matrix}"):
            if matrix == 0:
                total = own_a[:, y]
            else:
                total = own_b[:, x]
            for j in range(1, (down, across)[matrix]):
                second(matrix, j).wait_recv()
                total = total + (second_in_a, second_in_b)[matrix][j - 1].astype(F32)
            final[matrix] = total.astype(BF16)
            sums[c, s, :, pl.ds(matrix * half, half)] = final[matrix, c]
            final_swap(matrix).start()
            out_first(c, matrix)

    def finish_other(matrix):
        with jax.named_scope(f"other{matrix}"):
            final_swap(matrix).wait()
            out_first(1 - c, matrix)

    def out_x(matrix, part_at, k):
        block = sums.at[matrix, s, :, pl.ds(part_at * half, half)]
        return remote(
            block, block, out_x_sem.at[0, part_at, matrix, k - 1], out_x_sem.at[1, part_at, matrix, k - 1], x_peer(k)
        )

    def out_y(matrix, part_at, k):
        block = sums.at[matrix, s, :, pl.ds(part_at * half, half)]
        return remote(
            block, block, out_y_sem.at[0, part_at, matrix, k - 1], out_y_sem.at[1, part_at, matrix, k - 1], y_peer(k)
        )

    def out_first(matrix, part_at):
        for k in range(1, across):
            out_x(matrix, part_at, k).start()
        for k in range(1, down):
            out_y(matrix, part_at, k).start()

    def onward(matrix, part_at, k, j):
        columns = pl.ds(part_at * half, half)
        if matrix == 0:
            block = sums.at[0, y * across + (x + across - k) % across, :, columns]
            peer = y_peer(j)
        else:
            block = sums.at[1, ((y + down - k) % down) * across + x, :, columns]
            peer = x_peer(j)
        return remote(
            block, block, out_on_sem.at[0, part_at, matrix, k - 1, j - 1],
            out_on_sem.at[1, part_at, matrix, k - 1, j - 1], peer,
        )

    def out_forward(part_at):
        with jax.named_scope(f"forward{part_at}"):
            for k in range(1, across):
                out_x(0, part_at, k).wait_recv()
                for j in range(1, down):
                    onward(0, part_at, k, j).start()
            for k in range(1, down):
                out_y(1, part_at, k).wait_recv()
                for j in range(1, across):
                    onward(1, part_at, k, j).start()

    def out_end(part_at):
        with jax.named_scope(f"end{part_at}"):
            for k in range(1, across):
                out_x(1, part_at, k).wait_recv()
                for j in range(1, down):
                    onward(0, part_at, k, j).wait()
            for k in range(1, down):
                out_y(0, part_at, k).wait_recv()
                for j in range(1, across):
                    onward(1, part_at, k, j).wait()

    def mix_scatter(k):
        return remote(
            mix_low.at[(s + k) % ways], mix_plane.at[k - 1], mix_sem.at[0, k - 1], mix_sem.at[1, k - 1], in_plane(k)
        )

    def small_scatter(k):
        return remote(
            small_plane.at[s], small_plane.at[s], small_sem.at[0, k - 1], small_sem.at[1, k - 1], in_plane(k)
        )

    def mix_lift(k):
        return remote(
            mix_level.at[z], mix_level.at[z], mix_level_sem.at[0, k - 1], mix_level_sem.at[1, k - 1], in_level(k)
        )

    def small_lift(k):
        return remote(
            small_level.at[z], small_level.at[z],
            small_level_sem.at[0, k - 1], small_level_sem.at[1, k - 1], in_level(k),
        )

    def mix_gather(k):
        block = mix_all.at[c, s]
        return remote(block, block, mix_out_sem.at[0, k - 1], mix_out_sem.at[1, k - 1], in_plane(k))

    mix_back = remote(mix_all.at[c], mix_all.at[c], pair_sem.at[0, 5], pair_sem.at[1, 5], partner)

    def mix_stage(stage):
        if stage == 0:
            mix_swap.wait()
            small_swap.wait()
            mine = mix_part[pl.ds(c * per_core, per_core)] + mix_in[...]
            mix_low[...] = mine.reshape(mix_low.shape).astype(BF16)
            small_plane[s] = small[...] + small_in[...]
            for k in range(1, ways):
                mix_scatter(k).start()
                small_scatter(k).start()
        elif stage == 1:
            total = mix_low[s].astype(F32)
            for k in range(1, ways):
                mix_scatter(k).wait()
                small_scatter(k).wait()
                total = total + mix_plane[k - 1].astype(F32)
            mix_level[z] = total.astype(BF16)
            whole = small_plane[0]
            for k in range(1, ways):
                whole = whole + small_plane[k]
            small_level[z] = whole
            for k in range(1, levels):
                mix_lift(k).start()
                small_lift(k).start()
        elif stage == 2:
            for k in range(1, levels):
                mix_lift(k).wait()
                small_lift(k).wait()
            total = mix_level[0].astype(F32)
            whole = small_level[0]
            for k in range(1, levels):
                total = total + mix_level[k].astype(F32)
                whole = whole + small_level[k]
            mix_all[c, s] = total.astype(BF16)
            small[...] = whole
            for k in range(1, ways):
                mix_gather(k).start()
        elif stage == 3:
            for k in range(1, ways):
                mix_gather(k).wait()
            mix_back.start()
        else:
            mix_back.wait()
            packed_all = mix_all[...].reshape(pairs, block_len, block_len)
            for p in range(pairs):
                packed = packed_all[p].astype(F32)
                at = groups + 2 * pairs + p
                on_diagonal = jnp.where(diagonal, small[at:at + 1, :], 0.0)
                mix_out[2 * p] = jnp.where(causal, packed, 0.0).astype(BF16)
                mix_out[2 * p + 1] = jnp.where(row > column, packed.T, on_diagonal).astype(BF16)
            bias_out[...] = small[:groups, :]
            gain_out[...] = small[groups:groups + pairs, :]
            shift_out[...] = small[groups + pairs:groups + 2 * pairs, :]

    with jax.named_scope("swaps"):
        token_swap.wait()
        for copy in grad_swaps:
            copy.wait()
    for i in range(levels):
        send_chunk(i)
        if i == 0:
            mix_stage(0)
            arrive(1, 0)
        if i == 1:
            arrive(1, 1)
    mix_stage(1)
    for i in range(levels - 1):
        if i:
            arrive(i + 1, 0)
            arrive(i + 1, 1)
        run(i, 0)
        run(i, 1)
    mix_stage(2)
    with jax.named_scope("project_own"):
        project(z, c)
        shard_swap.wait()
        project(z, 1 - c)
    send_second(0)
    for k in range(1, levels - 1):
        relay_step(k)
    mix_stage(3)
    send_second(1)
    finish(0)
    relay_step(levels - 1)
    finish(1)
    finish_other(0)
    finish_other(1)
    out_forward(0)
    project_level(0)
    out_forward(1)
    mix_stage(4)
    for i in range(1, levels - 1):
        project_level(i)
    out_end(0)
    out_end(1)

    send_own(lambda copy: copy.wait_send())
    for i in range(levels - 1):
        level, way, k = nearest(i)
        for matrix in range(2):
            pass_on(level, way, k, matrix, lambda copy: copy.wait_send())
            for j in range(1, (across, down)[matrix]):
                side(level, way, k, matrix, j).wait_send()
        relay(level, way, k).wait_send()
        level, upward = target_of(i)
        for matrix in range(2):
            running(i, level, matrix, upward, z + 2 * upward - 1).wait_send()
    for matrix in range(2):
        for i in range(levels):
            for k in range(1, (across, down)[matrix]):
                first(i, matrix, k).wait_send()
        for j in range(1, (down, across)[matrix]):
            second(matrix, j).wait_send()
        for part_at in range(2):
            for k in range(1, across):
                out_x(matrix, part_at, k).wait_send()
            for k in range(1, down):
                out_y(matrix, part_at, k).wait_send()
    with jax.named_scope("stores"):
        for level in range(levels):
            for core in range(CORES):
                store(level, core).wait()


def shards(
    tokens,
    value_act,
    gate_act,
    cotangent,
    value_weight,
    gate_weight,
    norm_gain,
    norm_bias,
    mix_weight,
    mix_bias,
):
    ways = lax.axis_size("sp")
    levels = lax.axis_size("dp") // CORES
    across, down = plane_of(ways)
    inputs = tokens[0]
    seq_len, width = inputs.shape
    channels = value_act.shape[2]
    groups, block_len = mix_weight.shape[0], mix_weight.shape[1]
    pairs = groups // 2
    lanes = channels // pairs
    rows = value_weight.shape[0]
    share = rows // ways
    half = channels // 2
    vmem = pl.BlockSpec(memory_space=pltpu.VMEM)
    anywhere = pl.BlockSpec(memory_space=pl.ANY)
    sems = pltpu.SemaphoreType.DMA
    mix_rows = pairs * block_len // (CORES * ways)
    small_shape = (groups + 3 * pairs, lanes)
    shape = jax.ShapeDtypeStruct
    input_grad, summed, mix_out, bias_out, gain_out, shift_out = pl.pallas_call(
        functools.partial(kernel, ways, levels),
        out_shape=(
            shape((seq_len, width), BF16),
            shape((2, ways, share, channels), BF16),
            shape((groups, block_len, block_len), BF16),
            shape((groups, block_len), F32),
            shape((pairs, lanes), F32),
            shape((pairs, lanes), F32),
        ),
        in_specs=[anywhere] * 6 + [vmem] * 4,
        out_specs=(anywhere,) + (vmem,) * 5,
        scratch_shapes=[
            pltpu.VMEM((seq_len, width), BF16),
            pltpu.VMEM((seq_len, channels), BF16),
            pltpu.VMEM((seq_len, channels), BF16),
            pltpu.VMEM((seq_len, channels), BF16),
            pltpu.VMEM((pairs, 2 * block_len, block_len), BF16),
            pltpu.VMEM((pairs, block_len, 2 * block_len), BF16),
            pltpu.VMEM((block_len, channels), F32),
            pltpu.VMEM((2, seq_len, channels), BF16),
            pltpu.VMEM((seq_len, width), BF16),
            pltpu.VMEM((seq_len, channels), BF16),
            pltpu.VMEM((levels, CORES, 2, rows, channels), BF16),
            pltpu.VMEM((pairs, 2 * block_len, block_len), F32),
            pltpu.VMEM((block_len, channels), F32),
            pltpu.VMEM((1, channels), F32),
            pltpu.VMEM((1, channels), F32),
            pltpu.VMEM((block_len, channels), BF16),
            pltpu.VMEM((block_len, channels), BF16),
            pltpu.VMEM((block_len, channels), F32),
            pltpu.VMEM((block_len, channels), F32),
            pltpu.VMEM((seq_len, width), BF16),
            pltpu.VMEM((levels, CORES, down, across, share, channels), BF16),
            pltpu.VMEM((levels, across - 1, CORES, down, share, half), BF16),
            pltpu.VMEM((levels, down - 1, CORES, across, share, half), BF16),
            pltpu.VMEM((levels - 1, CORES, down, share, half), BF16),
            pltpu.VMEM((levels, 2, CORES, down, share, half), BF16),
            pltpu.VMEM((levels - 1, CORES, across, share, half), BF16),
            pltpu.VMEM((levels, 2, CORES, across, share, half), BF16),
            pltpu.VMEM((CORES, down, share, half), F32),
            pltpu.VMEM((CORES, across, share, half), F32),
            pltpu.VMEM((down - 1, CORES, share, half), BF16),
            pltpu.VMEM((down - 1, CORES, share, half), BF16),
            pltpu.VMEM((across - 1, CORES, share, half), BF16),
            pltpu.VMEM((across - 1, CORES, share, half), BF16),
            pltpu.VMEM((2, CORES, share, half), BF16),
            pltpu.VMEM((pairs, block_len, block_len), F32),
            pltpu.VMEM((pairs // CORES, block_len, block_len), F32),
            pltpu.VMEM((ways, mix_rows, block_len), BF16),
            pltpu.VMEM((ways - 1, mix_rows, block_len), BF16),
            pltpu.VMEM((levels, mix_rows, block_len), BF16),
            pltpu.VMEM((CORES, ways, mix_rows, block_len), BF16),
            pltpu.VMEM(small_shape, F32),
            pltpu.VMEM(small_shape, F32),
            pltpu.VMEM((ways,) + small_shape, F32),
            pltpu.VMEM((levels,) + small_shape, F32),
            sems((6,)),
            sems((levels * CORES,)),
            sems((2, 6)),
            sems((2, seq_len // block_len)),
            sems((2, 2, levels - 1, 2)),
            sems((2, 2, levels - 1, across - 1)),
            sems((2, 2, levels - 1, down - 1)),
            sems((2, 2, levels - 1)),
            sems((2, levels, across - 1)),
            sems((2, levels, down - 1)),
            sems((2, levels, 2, 2)),
            sems((2, down - 1)),
            sems((2, across - 1)),
            sems((2, 2)),
            sems((2, 2, 2, across - 1)),
            sems((2, 2, 2, down - 1)),
            sems((2, 2, 2, max(across, down) - 1, max(across, down) - 1)),
            sems((2, ways - 1)),
            sems((2, levels - 1)),
            sems((2, ways - 1)),
            sems((2, ways - 1)),
            sems((2, levels - 1)),
        ],
        compiler_params=pltpu.CompilerParams(
            collective_id=0, has_side_effects=True, vmem_limit_bytes=60 * 1024 * 1024
        ),
        name="unit",
    )(
        inputs, value_weight, gate_weight, value_act[0], gate_act[0], cotangent[0],
        norm_gain[None], norm_bias[None], mix_weight, mix_bias,
    )
    return (
        input_grad[None],
        summed[0].reshape(rows, channels).astype(F32),
        summed[1].reshape(rows, channels).astype(F32),
        mix_out.astype(F32),
        bias_out,
        gain_out.reshape(-1),
        shift_out.reshape(-1),
    )


def solution(mesh):
    placed = (
        P("dp", "sp", None),
        P("dp", "sp", None),
        P("dp", "sp", None),
        P("dp", "sp", None),
        P("dp", None),
        P("dp", None),
        P(),
        P(),
        P(),
        P(),
    )
    return jax.shard_map(
        shards,
        mesh=mesh,
        in_specs=placed,
        out_specs=(P("dp", "sp", None), P("dp", None), P("dp", None), P(), P(), P(), P()),
        check_vma=False,
    )
```

```python
import functools

import jax
import jax.numpy as jnp
from jax import lax
from jax.experimental import pallas as pl
from jax.experimental.pallas import tpu as pltpu
from jax.sharding import PartitionSpec as P

EPSILON = 1e-06
CORES = 2
MESH = pl.DeviceIdType.MESH
F32 = jnp.float32
BF16 = jnp.bfloat16


def remote(src, dst, send, recv, device):
    return pltpu.make_async_remote_copy(
        src_ref=src, dst_ref=dst, send_sem=send, recv_sem=recv, device_id=device, device_id_type=MESH
    )


def position():
    s, d = lax.axis_index("sp"), lax.axis_index("dp")
    return s, d, d // CORES, d % CORES


def plane_of(ways):
    across = max(k for k in range(1, ways + 1) if ways % k == 0 and k * k <= ways)
    return across, ways // across


def signal_all(ways, levels, s, d, z, c):
    barrier = pltpu.get_barrier_semaphore()
    for k in range(1, ways):
        pl.semaphore_signal(barrier, inc=1, device_id=((s + k) % ways, d), device_id_type=MESH)
    for k in range(1, levels):
        other = ((z + k) % levels) * CORES + c
        pl.semaphore_signal(barrier, inc=1, device_id=(s, other), device_id_type=MESH)
    pl.semaphore_signal(barrier, inc=1, device_id=(s, d + 1 - 2 * c), device_id_type=MESH)


def phi(values):
    cdf_part = 0.5 * (1.0 + lax.erf(values * 0.7071067811865476))
    pdf_part = jnp.exp(-0.5 * values * values) * 0.3989422804014327
    return cdf_part, cdf_part + values * pdf_part


def kernel(
    ways, levels,
    tokens_hbm, value_weight, gate_weight, value_hbm, gate_hbm, cotangent_hbm,
    gain_hbm, shift_hbm, mix_hbm, mix_bias_hbm,
    input_grad, value_out, gate_out, mix_out, small_out,
    tokens, value_act, gate_act, cotangent, gain, shift, mix_raw, mix_bias, mix, mix_turned, bias,
    grads, peer_tokens, peer_grads, gathered, weight_grad, spatial_sum, gain_grad, shift_grad,
    spread, low, spatial, grad_norm, product_in,
    part, first_x, first_y, run_out_a, run_in_a, run_out_b, run_in_b, own_a, own_b,
    second_out_a, second_in_a, second_out_b, second_in_b, final, sums,
    mix_part, mix_in, mix_low, mix_plane, mix_level, mix_all, mix_ready,
    small, small_in, small_plane, small_level, small_all,
    load_sem, store_sem, result_sem, pair_sem, swap_sem, chain_sem, value_sem, gate_sem, relay_sem,
    first_x_sem, first_y_sem, run_sem, second_a_sem, second_b_sem, final_sem, out_x_sem, out_y_sem, out_on_sem,
    mix_sem, mix_level_sem, mix_out_sem, small_sem, small_level_sem,
):
    s, d, z, c = position()
    across, down = plane_of(ways)
    x, y = s % across, s // across
    partner = (s, d + 1 - 2 * c)
    seq_len, channels = value_act.shape
    pairs, double, block_len = mix_turned.shape[0], mix_turned.shape[2], mix_turned.shape[1]
    lanes = channels // pairs
    groups = 2 * pairs
    rows_own = value_weight.shape[0]
    model = tokens.shape[1]
    depth = model // levels
    half = channels // 2
    share = rows_own // ways
    wide, tall = channels // across, channels // down

    def x_peer(k):
        return (y * across + (x + k) % across, d)

    def y_peer(k):
        return (((y + k) % down) * across + x, d)

    def in_plane(k):
        return ((s + k) % ways, d)

    def in_level(k):
        return (s, ((z + k) % levels) * CORES + c)

    loads = [
        pltpu.make_async_copy(value_weight, gathered.at[z, c, 0], load_sem.at[0]),
        pltpu.make_async_copy(gate_weight, gathered.at[z, c, 1], load_sem.at[1]),
        pltpu.make_async_copy(gate_hbm, gate_act, load_sem.at[2]),
        pltpu.make_async_copy(value_hbm, value_act, load_sem.at[3]),
        pltpu.make_async_copy(cotangent_hbm, cotangent, load_sem.at[4]),
        pltpu.make_async_copy(tokens_hbm, tokens, load_sem.at[5]),
        pltpu.make_async_copy(gain_hbm, gain, load_sem.at[6]),
        pltpu.make_async_copy(shift_hbm, shift, load_sem.at[7]),
        pltpu.make_async_copy(mix_hbm, mix_raw, load_sem.at[8]),
        pltpu.make_async_copy(mix_bias_hbm, mix_bias, load_sem.at[9]),
    ]
    signal_all(ways, levels, s, d, z, c)
    for k in (9, 8, 0, 1, 5, 2, 3, 4, 6, 7):
        loads[k].start()

    row = lax.broadcasted_iota(jnp.int32, (block_len, block_len), 0)
    column = lax.broadcasted_iota(jnp.int32, (block_len, block_len), 1)
    causal = row >= column
    lane = lax.broadcasted_iota(jnp.int32, (block_len, lanes), 1)
    first_half = lane < lanes // 2
    with jax.named_scope("load_mix"):
        loads[9].wait()
        loads[8].wait()
    bias_turned = mix_bias[...].T
    for p in range(pairs):
        for k in range(2):
            own = jnp.where(causal, mix_raw[2 * p + k].astype(F32), 0.0)
            mix[p, pl.ds(k * block_len, block_len), :] = own.astype(BF16)
            mix_turned[p, :, pl.ds(k * block_len, block_len)] = own.T.astype(BF16)
        bias[:, pl.ds(p * lanes, lanes)] = jnp.where(
            first_half, bias_turned[:, 2 * p:2 * p + 1], bias_turned[:, 2 * p + 1:2 * p + 2]
        )

    with jax.named_scope("barrier"):
        pl.semaphore_wait(pltpu.get_barrier_semaphore(), ways - 1 + levels - 1 + 1)

    def strip(level, matrix):
        if matrix == 0:
            return gathered.at[level, c, 0, :, pl.ds(pl.multiple_of(x * wide, wide), wide)]
        return gathered.at[level, c, 1, :, pl.ds(pl.multiple_of(y * tall, tall), tall)]

    def chain(level, way, k, matrix, target):
        block = strip(level, matrix)
        return remote(
            block, block, chain_sem.at[0, way, k - 1, matrix], chain_sem.at[1, way, k - 1, matrix],
            (s, target * CORES + c),
        )

    def nearest(i):
        below, above = z, levels - 1 - z
        shared = jnp.minimum(below, above)
        paired = i < 2 * shared
        k = jnp.where(paired, i // 2 + 1, i - shared + 1)
        way = jnp.where(paired, i % 2, jnp.where(below > above, 0, 1))
        return z - (1 - 2 * way) * k, way, k

    def send_own(act):
        for matrix in range(2):
            @pl.when(z + 1 < levels)
            def _():
                act(chain(z, 0, 1, matrix, z + 1))

            @pl.when(z >= 1)
            def _():
                act(chain(z, 1, 1, matrix, z - 1))

    def pass_on(level, way, k, matrix, act):
        target = z + 1 - 2 * way

        @pl.when((target >= 0) & (target < levels))
        def _():
            act(chain(level, way, k + 1, matrix, target))

    def side(level, way, k, matrix, j):
        block = strip(level, matrix)
        sem = (value_sem, gate_sem)[matrix]
        return remote(
            block, block, sem.at[0, way, k - 1, j - 1], sem.at[1, way, k - 1, j - 1], (x_peer, y_peer)[matrix](j)
        )

    def relay(level, way, k):
        block = gathered.at[level, c]
        return remote(block, block, relay_sem.at[0, way, k - 1], relay_sem.at[1, way, k - 1], partner)

    def both_ways(k, act):
        @pl.when(z >= k)
        def _():
            act(z - k, 0)

        @pl.when(z + k < levels)
        def _():
            act(z + k, 1)

    def arrive(k, matrix):
        def act(level, way):
            chain(level, way, k, matrix, z).wait_recv()
            pass_on(level, way, k, matrix, lambda copy: copy.start())
            for j in range(1, (across, down)[matrix]):
                side(level, way, k, matrix, j).start()

        with jax.named_scope(f"arrive{k}{matrix}"):
            both_ways(k, act)

    def relay_step(k):
        def act(level, way):
            for matrix in range(2):
                for j in range(1, (across, down)[matrix]):
                    side(level, way, k, matrix, j).wait_recv()
            relay(level, way, k).start()

        with jax.named_scope(f"relay{k}"):
            both_ways(k, act)

    def store(level, core):
        index = level * CORES + core
        cut = pl.ds(pl.multiple_of(index * rows_own, rows_own), rows_own)
        return pltpu.make_async_copy(product_in.at[:, cut], input_grad.at[:, cut], store_sem.at[index])

    def project(level, core):
        index = level * CORES + core
        cut = pl.ds(pl.multiple_of(index * rows_own, rows_own), rows_own)
        over = (((1,), (1,)), ((), ()))
        product_in[:, cut] = (
            lax.dot_general(grads[0], gathered[level, core, 0], over, preferred_element_type=F32)
            + lax.dot_general(grads[1], gathered[level, core, 1], over, preferred_element_type=F32)
        ).astype(BF16)
        store(level, core).start()

    def project_level(i):
        level, way, k = nearest(i)
        with jax.named_scope(f"project{i}"):
            relay(level, way, k).wait_recv()
            for core in range(CORES):
                project(level, core)

    loads[0].wait()
    loads[1].wait()
    send_own(lambda copy: copy.start())
    loads[5].wait()
    token_swap = remote(tokens, peer_tokens, pair_sem.at[0, 0], pair_sem.at[1, 0], partner)
    token_swap.start()
    shard_swap = remote(
        gathered.at[z, c], gathered.at[z, c], pair_sem.at[0, 1], pair_sem.at[1, 1], partner
    )
    for k in (2, 3, 4, 6, 7):
        loads[k].wait()

    weight_grad[...] = jnp.zeros_like(weight_grad)
    spatial_sum[...] = jnp.zeros_like(spatial_sum)
    gain_grad[...] = jnp.zeros_like(gain_grad)
    shift_grad[...] = jnp.zeros_like(shift_grad)
    turned = (((1,), (1,)), ((), ()))
    grad_swaps = []
    for b in range(seq_len // block_len):
        rows = pl.ds(b * block_len, block_len)
        gate = gate_act[rows, :].astype(F32)
        gate_cdf, gate_slope = phi(gate)
        gelu = gate * gate_cdf
        centred = gelu - jnp.mean(gelu, axis=-1, keepdims=True)
        inv_std = lax.rsqrt(jnp.mean(centred * centred, axis=-1, keepdims=True) + EPSILON)
        normed = centred * inv_std
        spread[...] = (normed * gain[...] + shift[...]).astype(BF16)
        value = value_act[rows, :].astype(F32)
        value_cdf, value_slope = phi(value)
        grad_out = cotangent[rows, :].astype(F32)
        grad_spatial = grad_out * (value * value_cdf)
        spatial_sum[...] += grad_spatial
        low[...] = grad_spatial.astype(BF16)
        for p in range(pairs):
            cut = pl.ds(p * lanes, lanes)
            inner = spread[:, cut]
            mixed = jnp.dot(mix[p], inner, preferred_element_type=F32)
            spatial[:, cut] = jnp.where(first_half, mixed[:block_len], mixed[block_len:]) + bias[:, cut]
            piece_low = low[:, cut]
            zero = jnp.zeros_like(piece_low)
            lower = jnp.where(first_half, piece_low, zero)
            apart = jnp.concatenate((lower, jnp.where(first_half, zero, piece_low)), axis=0)
            weight_grad[p, pl.ds(0, block_len), :] += lax.dot_general(
                lower, inner, turned, preferred_element_type=F32
            )
            weight_grad[p, pl.ds(block_len, block_len), :] += lax.dot_general(
                jnp.where(first_half, zero, inner), piece_low, turned, preferred_element_type=F32
            )
            grad_norm[:, cut] = jnp.dot(mix_turned[p], apart, preferred_element_type=F32)
        back = grad_norm[...]
        gain_grad[...] += jnp.sum(back * normed, axis=0, keepdims=True)
        shift_grad[...] += jnp.sum(back, axis=0, keepdims=True)
        hat = back * gain[...]
        grad_gate = inv_std * (
            hat
            - jnp.mean(hat, axis=-1, keepdims=True)
            - normed * jnp.mean(hat * normed, axis=-1, keepdims=True)
        )
        grads[0, rows, :] = (grad_out * spatial[...] * value_slope).astype(BF16)
        grads[1, rows, :] = (grad_gate * gate_slope).astype(BF16)
        grad_swaps.append(remote(
            grads.at[1 - c, rows], peer_grads.at[rows], swap_sem.at[0, b], swap_sem.at[1, b], partner
        ))
        grad_swaps[-1].start()

    diagonal = row == column
    per_core = pairs // CORES
    small[1, pl.ds(2 * pairs, pairs), :] = jnp.zeros((pairs, lanes), F32)
    for p in range(pairs):
        straight, flipped = weight_grad[p, pl.ds(0, block_len), :], weight_grad[p, pl.ds(block_len, block_len), :]
        mix_part[p] = jnp.where(causal, straight, flipped)
        small[1, pairs + p:pairs + p + 1, :] = jnp.sum(jnp.where(diagonal, flipped, 0.0), axis=0, keepdims=True)
    sums_by_row = jnp.zeros((block_len, lanes), F32)
    for p in range(pairs):
        terms = spatial_sum[:, pl.ds(p * lanes, lanes)]
        left = jnp.sum(jnp.where(first_half, terms, 0.0), axis=1, keepdims=True)
        right = jnp.sum(jnp.where(first_half, 0.0, terms), axis=1, keepdims=True)
        sums_by_row = jnp.where(lane == 2 * p, left, jnp.where(lane == 2 * p + 1, right, sums_by_row))
    small[0, pl.ds(0, groups), :] = sums_by_row.T[:groups]
    for p in range(pairs):
        cut = pl.ds(p * lanes, lanes)
        small[0, groups + p:groups + p + 1, :] = gain_grad[:, cut]
        small[1, p:p + 1, :] = shift_grad[:, cut]
    mix_swap = remote(
        mix_part.at[pl.ds((1 - c) * per_core, per_core)], mix_in, pair_sem.at[0, 3], pair_sem.at[1, 3], partner
    )
    mix_swap.start()
    small_swap = remote(small.at[1 - c], small_in, pair_sem.at[0, 4], pair_sem.at[1, 4], partner)
    small_swap.start()

    def target_of(i):
        return (z, 0) if i == levels - 1 else nearest(levels - 2 - i)[:2]

    def first(i, matrix, k):
        if matrix == 0:
            return remote(
                part.at[i, :, :, (x + k) % across, :, pl.ds(0, half)], first_x.at[i, k - 1],
                first_x_sem.at[0, i, k - 1], first_x_sem.at[1, i, k - 1], x_peer(k),
            )
        return remote(
            part.at[i, :, (y + k) % down, :, :, pl.ds(half, half)], first_y.at[i, k - 1],
            first_y_sem.at[0, i, k - 1], first_y_sem.at[1, i, k - 1], y_peer(k),
        )

    def send_chunk(i):
        target = target_of(i)[0]
        cut = pl.ds(pl.multiple_of(target * depth, depth), depth)
        over = (((0,), (0,)), ((), ()))
        with jax.named_scope(f"chunk{i}"):
            for matrix in range(2):
                side_half = pl.ds(matrix * half, half)
                product = lax.dot_general(
                    tokens[:, cut], grads[c, :, side_half], over, preferred_element_type=F32
                ) + lax.dot_general(peer_tokens[:, cut], peer_grads[:, side_half], over, preferred_element_type=F32)
                part[i, :, :, :, :, side_half] = product.reshape(part.shape[1:-1] + (half,)).astype(BF16)
                for k in range(1, (across, down)[matrix]):
                    first(i, matrix, k).start()

    def pair_sum(i, matrix):
        for k in range(1, (across, down)[matrix]):
            first(i, matrix, k).wait_recv()
        if matrix == 0:
            total = part[i, :, :, x, :, pl.ds(0, half)].astype(F32)
            for k in range(1, across):
                total = total + first_x[i, k - 1].astype(F32)
        else:
            total = part[i, :, y, :, :, pl.ds(half, half)].astype(F32)
            for k in range(1, down):
                total = total + first_y[i, k - 1].astype(F32)
        return total

    run_out, run_in = (run_out_a, run_out_b), (run_in_a, run_in_b)

    def running(i, level, matrix, upward, target):
        return remote(
            run_out[matrix].at[i], run_in[matrix].at[level, 1 - upward],
            run_sem.at[0, level, matrix, 1 - upward], run_sem.at[1, level, matrix, 1 - upward],
            (s, target * CORES + c),
        )

    def run(i, matrix):
        level, upward = target_of(i)
        step = 2 * upward - 1
        behind = z - step
        with jax.named_scope(f"run{i}{matrix}"):
            total = pair_sum(i, matrix)
            started = (behind >= 0) & (behind < levels)

            @pl.when(started)
            def _():
                running(i, level, matrix, upward, z).wait_recv()
                run_out[matrix][i] = (total + run_in[matrix][level, 1 - upward].astype(F32)).astype(BF16)

            @pl.when(jnp.logical_not(started))
            def _():
                run_out[matrix][i] = total.astype(BF16)

            running(i, level, matrix, upward, z + step).start()

    def second(matrix, j):
        if matrix == 0:
            return remote(
                second_out_a.at[j - 1], second_in_a.at[j - 1],
                second_a_sem.at[0, j - 1], second_a_sem.at[1, j - 1], y_peer(j),
            )
        return remote(
            second_out_b.at[j - 1], second_in_b.at[j - 1],
            second_b_sem.at[0, j - 1], second_b_sem.at[1, j - 1], x_peer(j),
        )

    def send_second(matrix):
        own = (own_a, own_b)[matrix]
        out = (second_out_a, second_out_b)[matrix]
        with jax.named_scope(f"second{matrix}"):
            own[...] = pair_sum(levels - 1, matrix)
            for upward in range(2):
                @pl.when((z >= 1) if upward else (z + 1 < levels))
                def _():
                    running(0, z, matrix, upward, z).wait_recv()
                    own[...] += run_in[matrix][z, 1 - upward].astype(F32)
            for j in range(1, (down, across)[matrix]):
                index = (y + j) % down if matrix == 0 else (x + j) % across
                out[j - 1] = own[:, index].astype(BF16)
                second(matrix, j).start()

    def final_swap(matrix):
        return remote(
            final.at[matrix, 1 - c], sums.at[c, s, :, pl.ds(matrix * half, half)],
            final_sem.at[0, matrix], final_sem.at[1, matrix], partner,
        )

    def finish(matrix):
        with jax.named_scope(f"finish{matrix}"):
            if matrix == 0:
                total = own_a[:, y]
            else:
                total = own_b[:, x]
            for j in range(1, (down, across)[matrix]):
                second(matrix, j).wait_recv()
                total = total + (second_in_a, second_in_b)[matrix][j - 1].astype(F32)
            final[matrix] = total.astype(BF16)
            sums[c, s, :, pl.ds(matrix * half, half)] = final[matrix, c]
            final_swap(matrix).start()
            out_first(c, matrix)

    def finish_other(matrix):
        with jax.named_scope(f"other{matrix}"):
            final_swap(matrix).wait()
            out_first(1 - c, matrix)

    def out_x(matrix, part_at, k):
        block = sums.at[matrix, s, :, pl.ds(part_at * half, half)]
        return remote(
            block, block, out_x_sem.at[0, part_at, matrix, k - 1], out_x_sem.at[1, part_at, matrix, k - 1], x_peer(k)
        )

    def out_y(matrix, part_at, k):
        block = sums.at[matrix, s, :, pl.ds(part_at * half, half)]
        return remote(
            block, block, out_y_sem.at[0, part_at, matrix, k - 1], out_y_sem.at[1, part_at, matrix, k - 1], y_peer(k)
        )

    def out_first(matrix, part_at):
        for k in range(1, across):
            out_x(matrix, part_at, k).start()
        for k in range(1, down):
            out_y(matrix, part_at, k).start()

    def onward(matrix, part_at, k, j):
        columns = pl.ds(part_at * half, half)
        if matrix == 0:
            block = sums.at[0, y * across + (x + across - k) % across, :, columns]
            peer = y_peer(j)
        else:
            block = sums.at[1, ((y + down - k) % down) * across + x, :, columns]
            peer = x_peer(j)
        return remote(
            block, block, out_on_sem.at[0, part_at, matrix, k - 1, j - 1],
            out_on_sem.at[1, part_at, matrix, k - 1, j - 1], peer,
        )

    def out_forward(part_at):
        with jax.named_scope(f"forward{part_at}"):
            for k in range(1, across):
                out_x(0, part_at, k).wait_recv()
                for j in range(1, down):
                    onward(0, part_at, k, j).start()
            for k in range(1, down):
                out_y(1, part_at, k).wait_recv()
                for j in range(1, across):
                    onward(1, part_at, k, j).start()

    def out_end(part_at):
        with jax.named_scope(f"end{part_at}"):
            for k in range(1, across):
                out_x(1, part_at, k).wait_recv()
                for j in range(1, down):
                    onward(0, part_at, k, j).wait()
            for k in range(1, down):
                out_y(0, part_at, k).wait_recv()
                for j in range(1, across):
                    onward(1, part_at, k, j).wait()
            for matrix in range(2):
                results[2 * part_at + matrix].start()

    def mix_scatter(k):
        return remote(
            mix_low.at[(s + k) % ways], mix_plane.at[k - 1], mix_sem.at[0, k - 1], mix_sem.at[1, k - 1], in_plane(k)
        )

    def small_scatter(k):
        return remote(
            small_plane.at[s], small_plane.at[s], small_sem.at[0, k - 1], small_sem.at[1, k - 1], in_plane(k)
        )

    def mix_lift(k):
        return remote(
            mix_level.at[z], mix_level.at[z], mix_level_sem.at[0, k - 1], mix_level_sem.at[1, k - 1], in_level(k)
        )

    def small_lift(k):
        return remote(
            small_level.at[z], small_level.at[z],
            small_level_sem.at[0, k - 1], small_level_sem.at[1, k - 1], in_level(k),
        )

    def mix_gather(k):
        block = mix_all.at[c, s]
        return remote(block, block, mix_out_sem.at[0, k - 1], mix_out_sem.at[1, k - 1], in_plane(k))

    small_back = remote(small_all.at[c], small_all.at[c], pair_sem.at[0, 2], pair_sem.at[1, 2], partner)
    mix_back = remote(mix_all.at[c], mix_all.at[c], pair_sem.at[0, 5], pair_sem.at[1, 5], partner)

    def mix_stage(stage):
        if stage == 0:
            mix_swap.wait()
            small_swap.wait()
            mine = mix_part[pl.ds(c * per_core, per_core)] + mix_in[...]
            mix_low[...] = mine.reshape(mix_low.shape).astype(BF16)
            small_plane[s] = small[c] + small_in[...]
            for k in range(1, ways):
                mix_scatter(k).start()
                small_scatter(k).start()
        elif stage == 1:
            total = mix_low[s].astype(F32)
            for k in range(1, ways):
                mix_scatter(k).wait()
                small_scatter(k).wait()
                total = total + mix_plane[k - 1].astype(F32)
            mix_level[z] = total.astype(BF16)
            whole = small_plane[0]
            for k in range(1, ways):
                whole = whole + small_plane[k]
            small_level[z] = whole
            for k in range(1, levels):
                mix_lift(k).start()
                small_lift(k).start()
        elif stage == 2:
            for k in range(1, levels):
                mix_lift(k).wait()
                small_lift(k).wait()
            total = mix_level[0].astype(F32)
            whole = small_level[0]
            for k in range(1, levels):
                total = total + mix_level[k].astype(F32)
                whole = whole + small_level[k]
            mix_all[c, s] = total.astype(BF16)
            small_all[c] = whole
            for k in range(1, ways):
                mix_gather(k).start()
        elif stage == 3:
            for k in range(1, ways):
                mix_gather(k).wait()
            mix_back.start()
            small_back.start()
        else:
            mix_back.wait()
            small_back.wait()
            packed_all = mix_all[...].reshape(pairs, block_len, block_len)
            for p in range(pairs):
                packed = packed_all[p].astype(F32)
                on_diagonal = jnp.where(diagonal, small_all[1, pairs + p:pairs + p + 1, :], 0.0)
                mix_ready[2 * p] = jnp.where(causal, packed, 0.0).astype(BF16)
                mix_ready[2 * p + 1] = jnp.where(row > column, packed.T, on_diagonal).astype(BF16)
            results[4].start()
            results[5].start()

    results = [
        pltpu.make_async_copy(
            sums.at[matrix, :, :, pl.ds(part_at * half, half)],
            (value_out, gate_out)[matrix].at[:, :, pl.ds(part_at * half, half)],
            result_sem.at[2 * part_at + matrix],
        )
        for part_at in range(2) for matrix in range(2)
    ] + [
        pltpu.make_async_copy(mix_ready, mix_out, result_sem.at[4]),
        pltpu.make_async_copy(small_all, small_out, result_sem.at[5]),
    ]

    with jax.named_scope("swaps"):
        token_swap.wait()
        for copy in grad_swaps:
            copy.wait()
    shard_swap.start()
    chunks = list(range(levels))
    send_chunk(chunks.pop(0))
    send_chunk(chunks.pop(0))
    arrive(1, 0)
    if chunks:
        send_chunk(chunks.pop(0))
    arrive(1, 1)
    run(0, 0)
    run(0, 1)
    for i in range(1, levels - 1):
        last = i == levels - 2
        if last:
            run(i, 0)
        arrive(i + 1, 0)
        arrive(i + 1, 1)
        if not last:
            run(i, 0)
        if chunks:
            send_chunk(chunks.pop(0))
        run(i, 1)
        if i == 1:
            mix_stage(0)
    with jax.named_scope("project_own"):
        project(z, c)
        shard_swap.wait()
        project(z, 1 - c)
    for k in range(1, levels - 1):
        relay_step(k)
    send_second(0)
    send_second(1)
    mix_stage(1)
    finish(0)
    relay_step(levels - 1)
    finish(1)
    mix_stage(2)
    finish_other(0)
    finish_other(1)
    out_forward(0)
    project_level(0)
    out_forward(1)
    mix_stage(3)
    for i in range(1, levels - 1):
        project_level(i)
    mix_stage(4)
    out_end(0)
    out_end(1)

    send_own(lambda copy: copy.wait_send())
    for i in range(levels - 1):
        level, way, k = nearest(i)
        for matrix in range(2):
            pass_on(level, way, k, matrix, lambda copy: copy.wait_send())
            for j in range(1, (across, down)[matrix]):
                side(level, way, k, matrix, j).wait_send()
        relay(level, way, k).wait_send()
        level, upward = target_of(i)
        for matrix in range(2):
            running(i, level, matrix, upward, z + 2 * upward - 1).wait_send()
    for matrix in range(2):
        for i in range(levels):
            for k in range(1, (across, down)[matrix]):
                first(i, matrix, k).wait_send()
        for j in range(1, (down, across)[matrix]):
            second(matrix, j).wait_send()
        for part_at in range(2):
            for k in range(1, across):
                out_x(matrix, part_at, k).wait_send()
            for k in range(1, down):
                out_y(matrix, part_at, k).wait_send()
    with jax.named_scope("stores"):
        for level in range(levels):
            for core in range(CORES):
                store(level, core).wait()
        for copy in results:
            copy.wait()


def shards(
    tokens,
    value_act,
    gate_act,
    cotangent,
    value_weight,
    gate_weight,
    norm_gain,
    norm_bias,
    mix_weight,
    mix_bias,
):
    ways = lax.axis_size("sp")
    levels = lax.axis_size("dp") // CORES
    across, down = plane_of(ways)
    inputs = tokens[0]
    seq_len, width = inputs.shape
    channels = value_act.shape[2]
    groups, block_len = mix_weight.shape[0], mix_weight.shape[1]
    pairs = groups // 2
    lanes = channels // pairs
    rows = value_weight.shape[0]
    share = rows // ways
    half = channels // 2
    anywhere = pl.BlockSpec(memory_space=pl.ANY)
    sems = pltpu.SemaphoreType.DMA
    mix_rows = pairs * block_len // (CORES * ways)
    small_shape = (CORES, 3 * pairs, lanes)
    shape = jax.ShapeDtypeStruct
    input_grad, value_sums, gate_sums, mix_out, small = pl.pallas_call(
        functools.partial(kernel, ways, levels),
        out_shape=(
            shape((seq_len, width), BF16),
            shape((ways, share, channels), BF16),
            shape((ways, share, channels), BF16),
            shape((groups, block_len, block_len), BF16),
            shape(small_shape, F32),
        ),
        in_specs=[anywhere] * 10,
        out_specs=(anywhere,) * 5,
        scratch_shapes=[
            pltpu.VMEM((seq_len, width), BF16),
            pltpu.VMEM((seq_len, channels), BF16),
            pltpu.VMEM((seq_len, channels), BF16),
            pltpu.VMEM((seq_len, channels), BF16),
            pltpu.VMEM((1, channels), F32),
            pltpu.VMEM((1, channels), F32),
            pltpu.VMEM((groups, block_len, block_len), BF16),
            pltpu.VMEM((groups, block_len), F32),
            pltpu.VMEM((pairs, 2 * block_len, block_len), BF16),
            pltpu.VMEM((pairs, block_len, 2 * block_len), BF16),
            pltpu.VMEM((block_len, channels), F32),
            pltpu.VMEM((2, seq_len, channels), BF16),
            pltpu.VMEM((seq_len, width), BF16),
            pltpu.VMEM((seq_len, channels), BF16),
            pltpu.VMEM((levels, CORES, 2, rows, channels), BF16),
            pltpu.VMEM((pairs, 2 * block_len, block_len), F32),
            pltpu.VMEM((block_len, channels), F32),
            pltpu.VMEM((1, channels), F32),
            pltpu.VMEM((1, channels), F32),
            pltpu.VMEM((block_len, channels), BF16),
            pltpu.VMEM((block_len, channels), BF16),
            pltpu.VMEM((block_len, channels), F32),
            pltpu.VMEM((block_len, channels), F32),
            pltpu.VMEM((seq_len, width), BF16),
            pltpu.VMEM((levels, CORES, down, across, share, channels), BF16),
            pltpu.VMEM((levels, across - 1, CORES, down, share, half), BF16),
            pltpu.VMEM((levels, down - 1, CORES, across, share, half), BF16),
            pltpu.VMEM((levels - 1, CORES, down, share, half), BF16),
            pltpu.VMEM((levels, 2, CORES, down, share, half), BF16),
            pltpu.VMEM((levels - 1, CORES, across, share, half), BF16),
            pltpu.VMEM((levels, 2, CORES, across, share, half), BF16),
            pltpu.VMEM((CORES, down, share, half), F32),
            pltpu.VMEM((CORES, across, share, half), F32),
            pltpu.VMEM((down - 1, CORES, share, half), BF16),
            pltpu.VMEM((down - 1, CORES, share, half), BF16),
            pltpu.VMEM((across - 1, CORES, share, half), BF16),
            pltpu.VMEM((across - 1, CORES, share, half), BF16),
            pltpu.VMEM((2, CORES, share, half), BF16),
            pltpu.VMEM((2, ways, share, channels), BF16),
            pltpu.VMEM((pairs, block_len, block_len), F32),
            pltpu.VMEM((pairs // CORES, block_len, block_len), F32),
            pltpu.VMEM((ways, mix_rows, block_len), BF16),
            pltpu.VMEM((ways - 1, mix_rows, block_len), BF16),
            pltpu.VMEM((levels, mix_rows, block_len), BF16),
            pltpu.VMEM((CORES, ways, mix_rows, block_len), BF16),
            pltpu.VMEM((groups, block_len, block_len), BF16),
            pltpu.VMEM(small_shape, F32),
            pltpu.VMEM(small_shape[1:], F32),
            pltpu.VMEM((ways,) + small_shape[1:], F32),
            pltpu.VMEM((levels,) + small_shape[1:], F32),
            pltpu.VMEM(small_shape, F32),
            sems((10,)),
            sems((levels * CORES,)),
            sems((6,)),
            sems((2, 6)),
            sems((2, seq_len // block_len)),
            sems((2, 2, levels - 1, 2)),
            sems((2, 2, levels - 1, across - 1)),
            sems((2, 2, levels - 1, down - 1)),
            sems((2, 2, levels - 1)),
            sems((2, levels, across - 1)),
            sems((2, levels, down - 1)),
            sems((2, levels, 2, 2)),
            sems((2, down - 1)),
            sems((2, across - 1)),
            sems((2, 2)),
            sems((2, 2, 2, across - 1)),
            sems((2, 2, 2, down - 1)),
            sems((2, 2, 2, max(across, down) - 1, max(across, down) - 1)),
            sems((2, ways - 1)),
            sems((2, levels - 1)),
            sems((2, ways - 1)),
            sems((2, ways - 1)),
            sems((2, levels - 1)),
        ],
        compiler_params=pltpu.CompilerParams(
            collective_id=0, has_side_effects=True, vmem_limit_bytes=60 * 1024 * 1024
        ),
        name="unit",
    )(
        inputs, value_weight, gate_weight, value_act[0], gate_act[0], cotangent[0],
        norm_gain[None], norm_bias[None], mix_weight, mix_bias,
    )
    return (
        input_grad[None],
        value_sums.reshape(rows, channels).astype(F32),
        gate_sums.reshape(rows, channels).astype(F32),
        mix_out.astype(F32),
        small[0, :groups],
        small[0, groups:].reshape(-1),
        small[1, :pairs].reshape(-1),
    )


def solution(mesh):
    placed = (
        P("dp", "sp", None),
        P("dp", "sp", None),
        P("dp", "sp", None),
        P("dp", "sp", None),
        P("dp", None),
        P("dp", None),
        P(),
        P(),
        P(),
        P(),
    )
    return jax.shard_map(
        shards,
        mesh=mesh,
        in_specs=placed,
        out_specs=(P("dp", "sp", None), P("dp", None), P("dp", None), P(), P(), P(), P()),
        check_vma=False,
    )
```

```python
import functools

import jax
import jax.numpy as jnp
from jax import lax
from jax.experimental import pallas as pl
from jax.experimental.pallas import tpu as pltpu
from jax.sharding import PartitionSpec as P

EPSILON = 1e-06
CORES = 2
MESH = pl.DeviceIdType.MESH
F32 = jnp.float32
BF16 = jnp.bfloat16


def remote(src, dst, send, recv, device):
    return pltpu.make_async_remote_copy(
        src_ref=src, dst_ref=dst, send_sem=send, recv_sem=recv, device_id=device, device_id_type=MESH
    )


def position():
    s, d = lax.axis_index("sp"), lax.axis_index("dp")
    return s, d, d // CORES, d % CORES


def plane_of(ways):
    across = max(k for k in range(1, ways + 1) if ways % k == 0 and k * k <= ways)
    return across, ways // across


def signal_all(ways, levels, s, d, z, c):
    barrier = pltpu.get_barrier_semaphore()
    for k in range(1, ways):
        pl.semaphore_signal(barrier, inc=1, device_id=((s + k) % ways, d), device_id_type=MESH)
    for k in range(1, levels):
        other = ((z + k) % levels) * CORES + c
        pl.semaphore_signal(barrier, inc=1, device_id=(s, other), device_id_type=MESH)
    pl.semaphore_signal(barrier, inc=1, device_id=(s, d + 1 - 2 * c), device_id_type=MESH)
    across, down = plane_of(ways)
    x, y, beside = s % across, s // across, d + 1 - 2 * c
    for k in range(1, across):
        pl.semaphore_signal(barrier, inc=1, device_id=(y * across + (x + k) % across, beside), device_id_type=MESH)
    for k in range(1, down):
        pl.semaphore_signal(barrier, inc=1, device_id=(((y + k) % down) * across + x, beside), device_id_type=MESH)
    return ways - 1 + levels - 1 + 1 + across - 1 + down - 1


def phi(values):
    cdf_part = 0.5 * (1.0 + lax.erf(values * 0.7071067811865476))
    pdf_part = jnp.exp(-0.5 * values * values) * 0.3989422804014327
    return cdf_part, cdf_part + values * pdf_part


def kernel(
    ways, levels,
    tokens_hbm, value_weight, gate_weight, value_hbm, gate_hbm, cotangent_hbm,
    gain_hbm, shift_hbm, mix_hbm, mix_bias_hbm,
    input_grad, value_out, gate_out, mix_out, small_out,
    tokens, value_act, gate_act, cotangent, gain, shift, mix_raw, mix_bias, mix, mix_turned, bias,
    grads, peer_tokens, peer_grads, gathered, spatial_sum, gain_grad, shift_grad,
    spread, low, spatial, grad_norm, product_in,
    part, first_x, first_y, run_out_a, run_in_a, run_out_b, run_in_b, own_a, own_b,
    second_out_a, second_in_a, second_out_b, second_in_b, final, sums,
    mix_part, mix_in, mix_low, mix_plane, mix_level, mix_all, mix_ready,
    small, small_in, small_plane, small_level, small_all,
    load_sem, store_sem, result_sem, pair_sem, swap_sem, chain_sem, value_sem, gate_sem, relay_sem,
    first_x_sem, first_y_sem, run_sem, second_a_sem, second_b_sem, final_sem, out_x_sem, out_y_sem, out_on_sem,
    mix_sem, mix_level_sem, mix_out_sem, small_sem, small_level_sem,
):
    s, d, z, c = position()
    across, down = plane_of(ways)
    x, y = s % across, s // across
    partner = (s, d + 1 - 2 * c)
    seq_len, channels = value_act.shape
    pairs, double, block_len = mix_turned.shape[0], mix_turned.shape[2], mix_turned.shape[1]
    lanes = channels // pairs
    groups = 2 * pairs
    rows_own = value_weight.shape[0]
    model = tokens.shape[1]
    depth = model // levels
    half = channels // 2
    share = rows_own // ways
    wide, tall = channels // across, channels // down

    def x_peer(k):
        return (y * across + (x + k) % across, d)

    def y_peer(k):
        return (((y + k) % down) * across + x, d)

    def in_plane(k):
        return ((s + k) % ways, d)

    def in_level(k):
        return (s, ((z + k) % levels) * CORES + c)

    loads = [
        pltpu.make_async_copy(value_weight, gathered.at[z, c, 0], load_sem.at[0]),
        pltpu.make_async_copy(gate_weight, gathered.at[z, c, 1], load_sem.at[1]),
        pltpu.make_async_copy(gate_hbm, gate_act, load_sem.at[2]),
        pltpu.make_async_copy(value_hbm, value_act, load_sem.at[3]),
        pltpu.make_async_copy(cotangent_hbm, cotangent, load_sem.at[4]),
        pltpu.make_async_copy(tokens_hbm, tokens, load_sem.at[5]),
        pltpu.make_async_copy(gain_hbm, gain, load_sem.at[6]),
        pltpu.make_async_copy(shift_hbm, shift, load_sem.at[7]),
        pltpu.make_async_copy(mix_hbm, mix_raw, load_sem.at[8]),
        pltpu.make_async_copy(mix_bias_hbm, mix_bias, load_sem.at[9]),
    ]
    greeted = signal_all(ways, levels, s, d, z, c)
    for k in (9, 8, 2, 3, 4, 6, 7, 0, 1, 5):
        loads[k].start()

    row = lax.broadcasted_iota(jnp.int32, (block_len, block_len), 0)
    column = lax.broadcasted_iota(jnp.int32, (block_len, block_len), 1)
    causal = row >= column
    lane = lax.broadcasted_iota(jnp.int32, (block_len, lanes), 1)
    first_half = lane < lanes // 2
    with jax.named_scope("load_mix"):
        loads[9].wait()
        loads[8].wait()
    bias_turned = mix_bias[...].T
    for p in range(pairs):
        for k in range(2):
            own = jnp.where(causal, mix_raw[2 * p + k].astype(F32), 0.0)
            mix[p, pl.ds(k * block_len, block_len), :] = own.astype(BF16)
            mix_turned[p, :, pl.ds(k * block_len, block_len)] = own.T.astype(BF16)
        bias[:, pl.ds(p * lanes, lanes)] = jnp.where(
            first_half, bias_turned[:, 2 * p:2 * p + 1], bias_turned[:, 2 * p + 1:2 * p + 2]
        )

    def strip(level, matrix):
        if matrix == 0:
            return gathered.at[level, c, 0, :, pl.ds(pl.multiple_of(x * wide, wide), wide)]
        return gathered.at[level, c, 1, :, pl.ds(pl.multiple_of(y * tall, tall), tall)]

    def chain(level, way, k, matrix, target):
        block = strip(level, matrix)
        return remote(
            block, block, chain_sem.at[0, way, k - 1, matrix], chain_sem.at[1, way, k - 1, matrix],
            (s, target * CORES + c),
        )

    def nearest(i):
        below, above = z, levels - 1 - z
        shared = jnp.minimum(below, above)
        paired = i < 2 * shared
        k = jnp.where(paired, i // 2 + 1, i - shared + 1)
        way = jnp.where(paired, i % 2, jnp.where(below > above, 0, 1))
        return z - (1 - 2 * way) * k, way, k

    def send_own(act):
        for matrix in range(2):
            @pl.when(z + 1 < levels)
            def _():
                act(chain(z, 0, 1, matrix, z + 1))

            @pl.when(z >= 1)
            def _():
                act(chain(z, 1, 1, matrix, z - 1))

    def pass_on(level, way, k, matrix, act):
        target = z + 1 - 2 * way

        @pl.when((target >= 0) & (target < levels))
        def _():
            act(chain(level, way, k + 1, matrix, target))

    def side(level, way, k, matrix, j):
        block = strip(level, matrix)
        sem = (value_sem, gate_sem)[matrix]
        return remote(
            block, block, sem.at[0, way, k - 1, j - 1], sem.at[1, way, k - 1, j - 1], (x_peer, y_peer)[matrix](j)
        )

    def relay(level, way, k):
        block = gathered.at[level, c]
        return remote(block, block, relay_sem.at[0, way, k - 1], relay_sem.at[1, way, k - 1], partner)

    def both_ways(k, act):
        @pl.when(z >= k)
        def _():
            act(z - k, 0)

        @pl.when(z + k < levels)
        def _():
            act(z + k, 1)

    def arrive(k, matrix):
        def act(level, way):
            chain(level, way, k, matrix, z).wait_recv()
            pass_on(level, way, k, matrix, lambda copy: copy.start())
            for j in range(1, (across, down)[matrix]):
                side(level, way, k, matrix, j).start()

        with jax.named_scope(f"arrive{k}{matrix}"):
            both_ways(k, act)

    def relay_step(k):
        def act(level, way):
            for matrix in range(2):
                for j in range(1, (across, down)[matrix]):
                    side(level, way, k, matrix, j).wait_recv()
            relay(level, way, k).start()

        with jax.named_scope(f"relay{k}"):
            both_ways(k, act)

    def store(level, core):
        index = level * CORES + core
        cut = pl.ds(pl.multiple_of(index * rows_own, rows_own), rows_own)
        return pltpu.make_async_copy(product_in.at[:, cut], input_grad.at[:, cut], store_sem.at[index])

    def project(level, core):
        index = level * CORES + core
        cut = pl.ds(pl.multiple_of(index * rows_own, rows_own), rows_own)
        over = (((1,), (1,)), ((), ()))
        product_in[:, cut] = (
            lax.dot_general(grads[0], gathered[level, core, 0], over, preferred_element_type=F32)
            + lax.dot_general(grads[1], gathered[level, core, 1], over, preferred_element_type=F32)
        ).astype(BF16)
        store(level, core).start()

    def project_level(i):
        level, way, k = nearest(i)
        with jax.named_scope(f"project{i}"):
            relay(level, way, k).wait_recv()
            for core in range(CORES):
                project(level, core)

    token_swap = remote(tokens, peer_tokens, pair_sem.at[0, 0], pair_sem.at[1, 0], partner)
    shard_swap = remote(
        gathered.at[z, c], gathered.at[z, c], pair_sem.at[0, 1], pair_sem.at[1, 1], partner
    )
    with jax.named_scope("load_acts"):
        for k in (2, 3, 4, 6, 7):
            loads[k].wait()

    gain_grad[...] = jnp.zeros_like(gain_grad)
    shift_grad[...] = jnp.zeros_like(shift_grad)
    turned = (((1,), (1,)), ((), ()))
    grad_swaps = []
    blocks = seq_len // block_len

    def block_grads(b):
        rows = pl.ds(b * block_len, block_len)
        gate = gate_act[rows, :].astype(F32)
        gate_cdf, gate_slope = phi(gate)
        gelu = gate * gate_cdf
        centred = gelu - jnp.mean(gelu, axis=-1, keepdims=True)
        inv_std = lax.rsqrt(jnp.mean(centred * centred, axis=-1, keepdims=True) + EPSILON)
        normed = centred * inv_std
        spread[rows, :] = (normed * gain[...] + shift[...]).astype(BF16)
        value = value_act[rows, :].astype(F32)
        value_cdf, value_slope = phi(value)
        grad_out = cotangent[rows, :].astype(F32)
        grad_spatial = grad_out * (value * value_cdf)
        if b == 0:
            spatial_sum[...] = grad_spatial
        else:
            spatial_sum[...] += grad_spatial
        low[rows, :] = grad_spatial.astype(BF16)
        for p in range(pairs):
            cut = pl.ds(p * lanes, lanes)
            mixed = jnp.dot(mix[p], spread[rows, cut], preferred_element_type=F32)
            spatial[:, cut] = jnp.where(first_half, mixed[:block_len], mixed[block_len:]) + bias[:, cut]
            piece_low = low[rows, cut]
            zero = jnp.zeros_like(piece_low)
            apart = jnp.concatenate(
                (jnp.where(first_half, piece_low, zero), jnp.where(first_half, zero, piece_low)), axis=0
            )
            grad_norm[:, cut] = jnp.dot(mix_turned[p], apart, preferred_element_type=F32)
        back = grad_norm[...]
        gain_grad[...] += jnp.sum(back * normed, axis=0, keepdims=True)
        shift_grad[...] += jnp.sum(back, axis=0, keepdims=True)
        hat = back * gain[...]
        grad_gate = inv_std * (
            hat
            - jnp.mean(hat, axis=-1, keepdims=True)
            - normed * jnp.mean(hat * normed, axis=-1, keepdims=True)
        )
        grads[0, rows, :] = (grad_out * spatial[...] * value_slope).astype(BF16)
        grads[1, rows, :] = (grad_gate * gate_slope).astype(BF16)

    def swap_grads(b):
        rows = pl.ds(b * block_len, block_len)
        grad_swaps.append(remote(
            grads.at[1 - c, rows], peer_grads.at[rows], swap_sem.at[0, b], swap_sem.at[1, b], partner
        ))
        grad_swaps[-1].start()

    with jax.named_scope("block0"):
        block_grads(0)
    with jax.named_scope("barrier"):
        pl.semaphore_wait(pltpu.get_barrier_semaphore(), greeted)
    with jax.named_scope("load_weights"):
        loads[0].wait()
        loads[1].wait()
        send_own(lambda copy: copy.start())
        loads[5].wait()
        token_swap.start()
    swap_grads(0)
    for b in range(1, blocks):
        with jax.named_scope(f"block{b}"):
            block_grads(b)
        swap_grads(b)

    diagonal = row == column
    per_core = pairs // CORES
    mix_swap = remote(
        mix_part.at[pl.ds((1 - c) * per_core, per_core)], mix_in, pair_sem.at[0, 3], pair_sem.at[1, 3], partner
    )
    small_swap = remote(small.at[1 - c], small_in, pair_sem.at[0, 4], pair_sem.at[1, 4], partner)

    def mix_terms():
        for p in range(pairs):
            cut = pl.ds(p * lanes, lanes)
            straight = jnp.zeros((block_len, block_len), F32)
            flipped = jnp.zeros((block_len, block_len), F32)
            for b in range(blocks):
                rows = pl.ds(b * block_len, block_len)
                inner, piece_low = spread[rows, cut], low[rows, cut]
                zero = jnp.zeros_like(inner)
                straight += lax.dot_general(
                    jnp.where(first_half, piece_low, zero), inner, turned, preferred_element_type=F32
                )
                flipped += lax.dot_general(
                    jnp.where(first_half, zero, inner), piece_low, turned, preferred_element_type=F32
                )
            mix_part[p] = jnp.where(causal, straight, flipped)
            small[1, pairs + p:pairs + p + 1, :] = jnp.sum(jnp.where(diagonal, flipped, 0.0), axis=0, keepdims=True)
        mix_swap.start()
        small[1, pl.ds(2 * pairs, pairs), :] = jnp.zeros((pairs, lanes), F32)
        sums_by_row = jnp.zeros((block_len, lanes), F32)
        for p in range(pairs):
            terms = spatial_sum[:, pl.ds(p * lanes, lanes)]
            left = jnp.sum(jnp.where(first_half, terms, 0.0), axis=1, keepdims=True)
            right = jnp.sum(jnp.where(first_half, 0.0, terms), axis=1, keepdims=True)
            sums_by_row = jnp.where(lane == 2 * p, left, jnp.where(lane == 2 * p + 1, right, sums_by_row))
        small[0, pl.ds(0, groups), :] = sums_by_row.T[:groups]
        for p in range(pairs):
            cut = pl.ds(p * lanes, lanes)
            small[0, groups + p:groups + p + 1, :] = gain_grad[:, cut]
            small[1, p:p + 1, :] = shift_grad[:, cut]
        small_swap.start()

    def target_of(i):
        return (z, 0) if i == levels - 1 else nearest(levels - 2 - i)[:2]

    def first(i, matrix, k):
        if matrix == 0:
            return remote(
                part.at[i, :, :, (x + k) % across, :, pl.ds(0, half)], first_x.at[i, k - 1],
                first_x_sem.at[0, i, k - 1], first_x_sem.at[1, i, k - 1], x_peer(k),
            )
        return remote(
            part.at[i, :, (y + k) % down, :, :, pl.ds(half, half)], first_y.at[i, k - 1],
            first_y_sem.at[0, i, k - 1], first_y_sem.at[1, i, k - 1], y_peer(k),
        )

    def send_chunk(i):
        target = target_of(i)[0]
        cut = pl.ds(pl.multiple_of(target * depth, depth), depth)
        over = (((0,), (0,)), ((), ()))
        def product(left, right, matrix):
            return lax.dot_general(
                left[:, cut], right[:, pl.ds(matrix * half, half)], over, preferred_element_type=F32
            )

        with jax.named_scope(f"chunk{i}"):
            if i == 0:
                held = [product(tokens, grads.at[c], matrix) for matrix in range(2)]
                with jax.named_scope("swaps"):
                    token_swap.wait()
                    for copy in grad_swaps:
                        copy.wait()
            for matrix in range(2):
                total = held[matrix] if i == 0 else product(tokens, grads.at[c], matrix)
                total = total + product(peer_tokens, peer_grads, matrix)
                part[i, :, :, :, :, pl.ds(matrix * half, half)] = total.reshape(
                    part.shape[1:-1] + (half,)
                ).astype(BF16)
                for k in range(1, (across, down)[matrix]):
                    first(i, matrix, k).start()

    def pair_sum(i, matrix):
        for k in range(1, (across, down)[matrix]):
            first(i, matrix, k).wait_recv()
        if matrix == 0:
            total = part[i, :, :, x, :, pl.ds(0, half)].astype(F32)
            for k in range(1, across):
                total = total + first_x[i, k - 1].astype(F32)
        else:
            total = part[i, :, y, :, :, pl.ds(half, half)].astype(F32)
            for k in range(1, down):
                total = total + first_y[i, k - 1].astype(F32)
        return total

    run_out, run_in = (run_out_a, run_out_b), (run_in_a, run_in_b)

    def running(i, level, matrix, upward, target):
        return remote(
            run_out[matrix].at[i], run_in[matrix].at[level, 1 - upward],
            run_sem.at[0, level, matrix, 1 - upward], run_sem.at[1, level, matrix, 1 - upward],
            (s, target * CORES + c),
        )

    def run(i, matrix):
        level, upward = target_of(i)
        step = 2 * upward - 1
        behind = z - step
        with jax.named_scope(f"run{i}{matrix}"):
            total = pair_sum(i, matrix)
            started = (behind >= 0) & (behind < levels)

            @pl.when(started)
            def _():
                running(i, level, matrix, upward, z).wait_recv()
                run_out[matrix][i] = (total + run_in[matrix][level, 1 - upward].astype(F32)).astype(BF16)

            @pl.when(jnp.logical_not(started))
            def _():
                run_out[matrix][i] = total.astype(BF16)

            running(i, level, matrix, upward, z + step).start()

    def second(matrix, j):
        if matrix == 0:
            return remote(
                second_out_a.at[j - 1], second_in_a.at[j - 1],
                second_a_sem.at[0, j - 1], second_a_sem.at[1, j - 1], y_peer(j),
            )
        return remote(
            second_out_b.at[j - 1], second_in_b.at[j - 1],
            second_b_sem.at[0, j - 1], second_b_sem.at[1, j - 1], x_peer(j),
        )

    def send_second(matrix):
        own = (own_a, own_b)[matrix]
        out = (second_out_a, second_out_b)[matrix]
        with jax.named_scope(f"second{matrix}"):
            own[...] = pair_sum(levels - 1, matrix)
            for upward in range(2):
                @pl.when((z >= 1) if upward else (z + 1 < levels))
                def _():
                    running(0, z, matrix, upward, z).wait_recv()
                    own[...] += run_in[matrix][z, 1 - upward].astype(F32)
            for j in range(1, (down, across)[matrix]):
                index = (y + j) % down if matrix == 0 else (x + j) % across
                out[j - 1] = own[:, index].astype(BF16)
                second(matrix, j).start()

    def final_swap(matrix):
        return remote(
            final.at[matrix, 1 - c], sums.at[c, s, :, pl.ds(matrix * half, half)],
            final_sem.at[0, matrix], final_sem.at[1, matrix], partner,
        )

    def finish(matrix):
        with jax.named_scope(f"finish{matrix}"):
            if matrix == 0:
                total = own_a[:, y]
            else:
                total = own_b[:, x]
            for j in range(1, (down, across)[matrix]):
                second(matrix, j).wait_recv()
                total = total + (second_in_a, second_in_b)[matrix][j - 1].astype(F32)
            final[matrix] = total.astype(BF16)
            sums[c, s, :, pl.ds(matrix * half, half)] = final[matrix, c]
            for core in range(CORES):
                for k in range(1, across):
                    out_x(core, c, matrix, k).start()
                for k in range(1, down):
                    out_y(core, c, matrix, k).start()
            final_swap(matrix).start()

    def out_x(core, matrix, part_at, k):
        return remote(
            final.at[part_at, core], sums.at[matrix, s, :, pl.ds(part_at * half, half)],
            out_x_sem.at[0, part_at, core, k - 1], out_x_sem.at[1, part_at, matrix, k - 1],
            (x_peer(k)[0], z * CORES + core),
        )

    def out_y(core, matrix, part_at, k):
        return remote(
            final.at[part_at, core], sums.at[matrix, s, :, pl.ds(part_at * half, half)],
            out_y_sem.at[0, part_at, core, k - 1], out_y_sem.at[1, part_at, matrix, k - 1],
            (y_peer(k)[0], z * CORES + core),
        )

    def onward(matrix, part_at, k, j):
        columns = pl.ds(part_at * half, half)
        if matrix == 0:
            block = sums.at[0, y * across + (x + across - k) % across, :, columns]
            peer = y_peer(j)
        else:
            block = sums.at[1, ((y + down - k) % down) * across + x, :, columns]
            peer = x_peer(j)
        return remote(
            block, block, out_on_sem.at[0, part_at, matrix, k - 1, j - 1],
            out_on_sem.at[1, part_at, matrix, k - 1, j - 1], peer,
        )

    def out_forward(part_at):
        with jax.named_scope(f"forward{part_at}"):
            for k in range(1, across):
                out_x(0, 0, part_at, k).wait_recv()
                for j in range(1, down):
                    onward(0, part_at, k, j).start()
            for k in range(1, down):
                out_y(0, 1, part_at, k).wait_recv()
                for j in range(1, across):
                    onward(1, part_at, k, j).start()

    def out_end(part_at):
        with jax.named_scope(f"end{part_at}"):
            for k in range(1, across):
                out_x(0, 1, part_at, k).wait_recv()
                for j in range(1, down):
                    onward(0, part_at, k, j).wait()
            for k in range(1, down):
                out_y(0, 0, part_at, k).wait_recv()
                for j in range(1, across):
                    onward(1, part_at, k, j).wait()
            final_swap(part_at).wait()
            for matrix in range(2):
                results[2 * part_at + matrix].start()

    def mix_scatter(k):
        return remote(
            mix_low.at[(s + k) % ways], mix_plane.at[k - 1], mix_sem.at[0, k - 1], mix_sem.at[1, k - 1], in_plane(k)
        )

    def small_scatter(k):
        return remote(
            small_plane.at[s], small_plane.at[s], small_sem.at[0, k - 1], small_sem.at[1, k - 1], in_plane(k)
        )

    def mix_lift(k):
        return remote(
            mix_level.at[z], mix_level.at[z], mix_level_sem.at[0, k - 1], mix_level_sem.at[1, k - 1], in_level(k)
        )

    def small_lift(k):
        return remote(
            small_level.at[z], small_level.at[z],
            small_level_sem.at[0, k - 1], small_level_sem.at[1, k - 1], in_level(k),
        )

    def mix_gather(k):
        block = mix_all.at[c, s]
        return remote(block, block, mix_out_sem.at[0, k - 1], mix_out_sem.at[1, k - 1], in_plane(k))

    small_back = remote(small_all.at[c], small_all.at[c], pair_sem.at[0, 2], pair_sem.at[1, 2], partner)
    mix_back = remote(mix_all.at[c], mix_all.at[c], pair_sem.at[0, 5], pair_sem.at[1, 5], partner)

    def mix_stage(stage):
        if stage == 0:
            mix_swap.wait()
            small_swap.wait()
            mine = mix_part[pl.ds(c * per_core, per_core)] + mix_in[...]
            mix_low[...] = mine.reshape(mix_low.shape).astype(BF16)
            small_plane[s] = small[c] + small_in[...]
            for k in range(1, ways):
                mix_scatter(k).start()
                small_scatter(k).start()
        elif stage == 1:
            total = mix_low[s].astype(F32)
            for k in range(1, ways):
                mix_scatter(k).wait()
                small_scatter(k).wait()
                total = total + mix_plane[k - 1].astype(F32)
            mix_level[z] = total.astype(BF16)
            whole = small_plane[0]
            for k in range(1, ways):
                whole = whole + small_plane[k]
            small_level[z] = whole
            for k in range(1, levels):
                mix_lift(k).start()
                small_lift(k).start()
        elif stage == 2:
            for k in range(1, levels):
                mix_lift(k).wait()
                small_lift(k).wait()
            total = mix_level[0].astype(F32)
            whole = small_level[0]
            for k in range(1, levels):
                total = total + mix_level[k].astype(F32)
                whole = whole + small_level[k]
            mix_all[c, s] = total.astype(BF16)
            small_all[c] = whole
            for k in range(1, ways):
                mix_gather(k).start()
        elif stage == 3:
            for k in range(1, ways):
                mix_gather(k).wait()
            mix_back.start()
            small_back.start()
        else:
            mix_back.wait()
            small_back.wait()
            packed_all = mix_all[...].reshape(pairs, block_len, block_len)
            for p in range(pairs):
                packed = packed_all[p].astype(F32)
                on_diagonal = jnp.where(diagonal, small_all[1, pairs + p:pairs + p + 1, :], 0.0)
                mix_ready[2 * p] = jnp.where(causal, packed, 0.0).astype(BF16)
                mix_ready[2 * p + 1] = jnp.where(row > column, packed.T, on_diagonal).astype(BF16)
            results[4].start()
            results[5].start()

    results = [
        pltpu.make_async_copy(
            sums.at[matrix, :, :, pl.ds(part_at * half, half)],
            (value_out, gate_out)[matrix].at[:, :, pl.ds(part_at * half, half)],
            result_sem.at[2 * part_at + matrix],
        )
        for part_at in range(2) for matrix in range(2)
    ] + [
        pltpu.make_async_copy(mix_ready, mix_out, result_sem.at[4]),
        pltpu.make_async_copy(small_all, small_out, result_sem.at[5]),
    ]

    chunks = list(range(levels))
    send_chunk(chunks.pop(0))
    shard_swap.start()
    send_chunk(chunks.pop(0))
    with jax.named_scope("mix_terms"):
        mix_terms()
    arrive(1, 0)
    if chunks:
        send_chunk(chunks.pop(0))
    arrive(1, 1)
    run(0, 0)
    run(0, 1)
    for i in range(1, levels - 1):
        last = i == levels - 2
        if last:
            run(i, 0)
        arrive(i + 1, 0)
        arrive(i + 1, 1)
        if not last:
            run(i, 0)
        if chunks:
            send_chunk(chunks.pop(0))
        run(i, 1)
        if i == 1:
            mix_stage(0)
    with jax.named_scope("project_own"):
        project(z, c)
        shard_swap.wait()
        project(z, 1 - c)
    for k in range(1, levels - 1):
        relay_step(k)
    send_second(0)
    send_second(1)
    mix_stage(1)
    finish(0)
    relay_step(levels - 1)
    finish(1)
    mix_stage(2)
    out_forward(0)
    project_level(0)
    out_forward(1)
    mix_stage(3)
    for i in range(1, levels - 1):
        project_level(i)
    mix_stage(4)
    out_end(0)
    out_end(1)

    send_own(lambda copy: copy.wait_send())
    for i in range(levels - 1):
        level, way, k = nearest(i)
        for matrix in range(2):
            pass_on(level, way, k, matrix, lambda copy: copy.wait_send())
            for j in range(1, (across, down)[matrix]):
                side(level, way, k, matrix, j).wait_send()
        relay(level, way, k).wait_send()
        level, upward = target_of(i)
        for matrix in range(2):
            running(i, level, matrix, upward, z + 2 * upward - 1).wait_send()
    for matrix in range(2):
        for i in range(levels):
            for k in range(1, (across, down)[matrix]):
                first(i, matrix, k).wait_send()
        for j in range(1, (down, across)[matrix]):
            second(matrix, j).wait_send()
        for part_at in range(2):
            for k in range(1, across):
                out_x(matrix, 0, part_at, k).wait_send()
            for k in range(1, down):
                out_y(matrix, 0, part_at, k).wait_send()
    with jax.named_scope("stores"):
        for level in range(levels):
            for core in range(CORES):
                store(level, core).wait()
        for copy in results:
            copy.wait()


def write_out(
    input_grad, value_sums, gate_sums, mix_grad, small,
    input_out, value_out, gate_out, mix_out, bias_out, gain_out, shift_out,
    held, value_low, gate_low, mix_low, few, value_full, gate_full, mix_full, load_sem, store_sem,
):
    cuts = held.shape[0]
    tall = held.shape[1]
    groups = bias_out.shape[0]
    pairs = groups // 2
    loads = [
        pltpu.make_async_copy(value_sums, value_low, load_sem.at[0]),
        pltpu.make_async_copy(gate_sums, gate_low, load_sem.at[1]),
        pltpu.make_async_copy(mix_grad, mix_low, load_sem.at[2]),
        pltpu.make_async_copy(small, few, load_sem.at[3]),
    ] + [
        pltpu.make_async_copy(input_grad.at[pl.ds(i * tall, tall)], held.at[i], load_sem.at[4 + i]) for i in range(cuts)
    ]
    stores = [
        pltpu.make_async_copy(value_full, value_out, store_sem.at[0]),
        pltpu.make_async_copy(gate_full, gate_out, store_sem.at[1]),
        pltpu.make_async_copy(mix_full, mix_out, store_sem.at[2]),
        pltpu.make_async_copy(few.at[0, pl.ds(0, groups)], bias_out, store_sem.at[3]),
        pltpu.make_async_copy(few.at[0, pl.ds(groups, pairs)], gain_out, store_sem.at[4]),
        pltpu.make_async_copy(few.at[1, pl.ds(0, pairs)], shift_out, store_sem.at[5]),
    ] + [
        pltpu.make_async_copy(held.at[i], input_out.at[pl.ds(i * tall, tall)], store_sem.at[6 + i]) for i in range(cuts)
    ]
    for copy in loads:
        copy.start()
    for i, (low, full) in enumerate(((value_low, value_full), (gate_low, gate_full), (mix_low, mix_full))):
        loads[i].wait()
        full[...] = low[...].reshape(full.shape).astype(F32)
        stores[i].start()
    loads[3].wait()
    for i in range(3, 6):
        stores[i].start()
    for i in range(cuts):
        loads[4 + i].wait()
        stores[6 + i].start()
    for copy in stores:
        copy.wait()


def shards(
    tokens,
    value_act,
    gate_act,
    cotangent,
    value_weight,
    gate_weight,
    norm_gain,
    norm_bias,
    mix_weight,
    mix_bias,
):
    ways = lax.axis_size("sp")
    levels = lax.axis_size("dp") // CORES
    across, down = plane_of(ways)
    inputs = tokens[0]
    seq_len, width = inputs.shape
    channels = value_act.shape[2]
    groups, block_len = mix_weight.shape[0], mix_weight.shape[1]
    pairs = groups // 2
    lanes = channels // pairs
    rows = value_weight.shape[0]
    share = rows // ways
    half = channels // 2
    anywhere = pl.BlockSpec(memory_space=pl.ANY)
    sems = pltpu.SemaphoreType.DMA
    mix_rows = pairs * block_len // (CORES * ways)
    small_shape = (CORES, 3 * pairs, lanes)
    shape = jax.ShapeDtypeStruct
    input_grad, value_sums, gate_sums, mix_out, small = pl.pallas_call(
        functools.partial(kernel, ways, levels),
        out_shape=(
            shape((seq_len, width), BF16),
            shape((ways, share, channels), BF16),
            shape((ways, share, channels), BF16),
            shape((groups, block_len, block_len), BF16),
            shape(small_shape, F32),
        ),
        in_specs=[anywhere] * 10,
        out_specs=(anywhere,) * 5,
        scratch_shapes=[
            pltpu.VMEM((seq_len, width), BF16),
            pltpu.VMEM((seq_len, channels), BF16),
            pltpu.VMEM((seq_len, channels), BF16),
            pltpu.VMEM((seq_len, channels), BF16),
            pltpu.VMEM((1, channels), F32),
            pltpu.VMEM((1, channels), F32),
            pltpu.VMEM((groups, block_len, block_len), BF16),
            pltpu.VMEM((groups, block_len), F32),
            pltpu.VMEM((pairs, 2 * block_len, block_len), BF16),
            pltpu.VMEM((pairs, block_len, 2 * block_len), BF16),
            pltpu.VMEM((block_len, channels), F32),
            pltpu.VMEM((2, seq_len, channels), BF16),
            pltpu.VMEM((seq_len, width), BF16),
            pltpu.VMEM((seq_len, channels), BF16),
            pltpu.VMEM((levels, CORES, 2, rows, channels), BF16),
            pltpu.VMEM((block_len, channels), F32),
            pltpu.VMEM((1, channels), F32),
            pltpu.VMEM((1, channels), F32),
            pltpu.VMEM((seq_len, channels), BF16),
            pltpu.VMEM((seq_len, channels), BF16),
            pltpu.VMEM((block_len, channels), F32),
            pltpu.VMEM((block_len, channels), F32),
            pltpu.VMEM((seq_len, width), BF16),
            pltpu.VMEM((levels, CORES, down, across, share, channels), BF16),
            pltpu.VMEM((levels, across - 1, CORES, down, share, half), BF16),
            pltpu.VMEM((levels, down - 1, CORES, across, share, half), BF16),
            pltpu.VMEM((levels - 1, CORES, down, share, half), BF16),
            pltpu.VMEM((levels, 2, CORES, down, share, half), BF16),
            pltpu.VMEM((levels - 1, CORES, across, share, half), BF16),
            pltpu.VMEM((levels, 2, CORES, across, share, half), BF16),
            pltpu.VMEM((CORES, down, share, half), F32),
            pltpu.VMEM((CORES, across, share, half), F32),
            pltpu.VMEM((down - 1, CORES, share, half), BF16),
            pltpu.VMEM((down - 1, CORES, share, half), BF16),
            pltpu.VMEM((across - 1, CORES, share, half), BF16),
            pltpu.VMEM((across - 1, CORES, share, half), BF16),
            pltpu.VMEM((2, CORES, share, half), BF16),
            pltpu.VMEM((2, ways, share, channels), BF16),
            pltpu.VMEM((pairs, block_len, block_len), F32),
            pltpu.VMEM((pairs // CORES, block_len, block_len), F32),
            pltpu.VMEM((ways, mix_rows, block_len), BF16),
            pltpu.VMEM((ways - 1, mix_rows, block_len), BF16),
            pltpu.VMEM((levels, mix_rows, block_len), BF16),
            pltpu.VMEM((CORES, ways, mix_rows, block_len), BF16),
            pltpu.VMEM((groups, block_len, block_len), BF16),
            pltpu.VMEM(small_shape, F32),
            pltpu.VMEM(small_shape[1:], F32),
            pltpu.VMEM((ways,) + small_shape[1:], F32),
            pltpu.VMEM((levels,) + small_shape[1:], F32),
            pltpu.VMEM(small_shape, F32),
            sems((10,)),
            sems((levels * CORES,)),
            sems((6,)),
            sems((2, 6)),
            sems((2, seq_len // block_len)),
            sems((2, 2, levels - 1, 2)),
            sems((2, 2, levels - 1, across - 1)),
            sems((2, 2, levels - 1, down - 1)),
            sems((2, 2, levels - 1)),
            sems((2, levels, across - 1)),
            sems((2, levels, down - 1)),
            sems((2, levels, 2, 2)),
            sems((2, down - 1)),
            sems((2, across - 1)),
            sems((2, 2)),
            sems((2, 2, 2, across - 1)),
            sems((2, 2, 2, down - 1)),
            sems((2, 2, 2, max(across, down) - 1, max(across, down) - 1)),
            sems((2, ways - 1)),
            sems((2, levels - 1)),
            sems((2, ways - 1)),
            sems((2, ways - 1)),
            sems((2, levels - 1)),
        ],
        compiler_params=pltpu.CompilerParams(
            collective_id=0, has_side_effects=True, vmem_limit_bytes=60 * 1024 * 1024
        ),
        name="unit",
    )(
        inputs, value_weight, gate_weight, value_act[0], gate_act[0], cotangent[0],
        norm_gain[None], norm_bias[None], mix_weight, mix_bias,
    )
    cuts = 3
    low_shape, full_shape, mix_full = (ways, share, channels), (rows, channels), (groups, block_len, block_len)
    input_grad, value_grad, gate_grad, mix_grad, bias_grad, gain_grad, shift_grad = pl.pallas_call(
        write_out,
        out_shape=(
            shape((seq_len, width), BF16),
            shape(full_shape, F32),
            shape(full_shape, F32),
            shape(mix_full, F32),
            shape((groups, block_len), F32),
            shape((pairs, lanes), F32),
            shape((pairs, lanes), F32),
        ),
        in_specs=[anywhere] * 5,
        out_specs=(anywhere,) * 7,
        scratch_shapes=[
            pltpu.VMEM((cuts, seq_len // cuts, width), BF16),
            pltpu.VMEM(low_shape, BF16),
            pltpu.VMEM(low_shape, BF16),
            pltpu.VMEM(mix_full, BF16),
            pltpu.VMEM(small_shape, F32),
            pltpu.VMEM(full_shape, F32),
            pltpu.VMEM(full_shape, F32),
            pltpu.VMEM(mix_full, F32),
            sems((4 + cuts,)),
            sems((6 + cuts,)),
        ],
        name="write_out",
    )(input_grad, value_sums, gate_sums, mix_out, small)
    return (
        input_grad[None],
        value_grad,
        gate_grad,
        mix_grad,
        bias_grad,
        gain_grad.reshape(-1),
        shift_grad.reshape(-1),
    )


def solution(mesh):
    placed = (
        P("dp", "sp", None),
        P("dp", "sp", None),
        P("dp", "sp", None),
        P("dp", "sp", None),
        P("dp", None),
        P("dp", None),
        P(),
        P(),
        P(),
        P(),
    )
    return jax.shard_map(
        shards,
        mesh=mesh,
        in_specs=placed,
        out_specs=(P("dp", "sp", None), P("dp", None), P("dp", None), P(), P(), P(), P()),
        check_vma=False,
    )
```

```python
import functools

import jax
import jax.numpy as jnp
from jax import lax
from jax.experimental import pallas as pl
from jax.experimental.pallas import tpu as pltpu
from jax.sharding import PartitionSpec as P

EPSILON = 1e-06
CORES = 2
MESH = pl.DeviceIdType.MESH
F32 = jnp.float32
BF16 = jnp.bfloat16


def remote(src, dst, send, recv, device):
    return pltpu.make_async_remote_copy(
        src_ref=src, dst_ref=dst, send_sem=send, recv_sem=recv, device_id=device, device_id_type=MESH
    )


def position():
    s, d = lax.axis_index("sp"), lax.axis_index("dp")
    return s, d, d // CORES, d % CORES


def plane_of(ways):
    across = max(k for k in range(1, ways + 1) if ways % k == 0 and k * k <= ways)
    return across, ways // across


def signal_all(ways, levels, s, d, z, c):
    barrier = pltpu.get_barrier_semaphore()
    for k in range(1, ways):
        pl.semaphore_signal(barrier, inc=1, device_id=((s + k) % ways, d), device_id_type=MESH)
    for k in range(1, levels):
        other = ((z + k) % levels) * CORES + c
        pl.semaphore_signal(barrier, inc=1, device_id=(s, other), device_id_type=MESH)
    pl.semaphore_signal(barrier, inc=1, device_id=(s, d + 1 - 2 * c), device_id_type=MESH)
    across, down = plane_of(ways)
    x, y, beside = s % across, s // across, d + 1 - 2 * c
    for k in range(1, across):
        pl.semaphore_signal(barrier, inc=1, device_id=(y * across + (x + k) % across, beside), device_id_type=MESH)
    for k in range(1, down):
        pl.semaphore_signal(barrier, inc=1, device_id=(((y + k) % down) * across + x, beside), device_id_type=MESH)
    return ways - 1 + levels - 1 + 1 + across - 1 + down - 1


def phi(values):
    cdf_part = 0.5 * (1.0 + lax.erf(values * 0.7071067811865476))
    pdf_part = jnp.exp(-0.5 * values * values) * 0.3989422804014327
    return cdf_part, cdf_part + values * pdf_part


def kernel(
    ways, levels,
    tokens_hbm, value_weight, gate_weight, value_hbm, gate_hbm, cotangent_hbm,
    gain_hbm, shift_hbm, mix_hbm, mix_bias_hbm,
    input_grad, value_out, gate_out, mix_out, small_out,
    tokens, value_act, gate_act, cotangent, gain, shift, mix_raw, mix_bias, mix, mix_turned, bias,
    grads, peer_tokens, peer_grads, gathered, spatial_sum, gain_grad, shift_grad,
    spread, low, spatial, grad_norm, product_in,
    held, part, first_x, first_y, run_out_a, run_in_a, run_out_b, run_in_b, own_a, own_b,
    second_out_a, second_in_a, second_out_b, second_in_b, final, sums,
    mix_part, mix_in, mix_low, mix_plane, mix_level, mix_all, mix_ready,
    small, small_in, small_plane, small_level, small_all,
    load_sem, store_sem, result_sem, token_sem, pair_sem, swap_sem, chain_sem, value_sem, gate_sem, relay_sem,
    first_x_sem, first_y_sem, run_sem, second_a_sem, second_b_sem, final_sem, out_x_sem, out_y_sem, out_on_sem,
    mix_sem, mix_level_sem, mix_out_sem, small_sem, small_level_sem,
):
    s, d, z, c = position()
    across, down = plane_of(ways)
    x, y = s % across, s // across
    partner = (s, d + 1 - 2 * c)
    seq_len, channels = value_act.shape
    pairs, double, block_len = mix_turned.shape[0], mix_turned.shape[2], mix_turned.shape[1]
    lanes = channels // pairs
    groups = 2 * pairs
    rows_own = value_weight.shape[0]
    model = tokens.shape[1]
    depth = model // levels
    half = channels // 2
    share = rows_own // ways
    wide, tall = channels // across, channels // down

    def x_peer(k):
        return (y * across + (x + k) % across, d)

    def y_peer(k):
        return (((y + k) % down) * across + x, d)

    def in_plane(k):
        return ((s + k) % ways, d)

    def in_level(k):
        return (s, ((z + k) % levels) * CORES + c)

    loads = [
        pltpu.make_async_copy(value_weight, gathered.at[z, c, 0], load_sem.at[0]),
        pltpu.make_async_copy(gate_weight, gathered.at[z, c, 1], load_sem.at[1]),
        pltpu.make_async_copy(gate_hbm, gate_act, load_sem.at[2]),
        pltpu.make_async_copy(value_hbm, value_act, load_sem.at[3]),
        pltpu.make_async_copy(cotangent_hbm, cotangent, load_sem.at[4]),
        pltpu.make_async_copy(tokens_hbm, tokens, load_sem.at[5]),
        pltpu.make_async_copy(gain_hbm, gain, load_sem.at[6]),
        pltpu.make_async_copy(shift_hbm, shift, load_sem.at[7]),
        pltpu.make_async_copy(mix_hbm, mix_raw, load_sem.at[8]),
        pltpu.make_async_copy(mix_bias_hbm, mix_bias, load_sem.at[9]),
    ]
    greeted = signal_all(ways, levels, s, d, z, c)
    for k in (9, 8, 2, 3, 4, 6, 7, 0, 1, 5):
        loads[k].start()

    row = lax.broadcasted_iota(jnp.int32, (block_len, block_len), 0)
    column = lax.broadcasted_iota(jnp.int32, (block_len, block_len), 1)
    causal = row >= column
    lane = lax.broadcasted_iota(jnp.int32, (block_len, lanes), 1)
    first_half = lane < lanes // 2
    with jax.named_scope("load_mix"):
        loads[9].wait()
        loads[8].wait()
    bias_turned = mix_bias[...].T
    for p in range(pairs):
        for k in range(2):
            own = jnp.where(causal, mix_raw[2 * p + k].astype(F32), 0.0)
            mix[p, pl.ds(k * block_len, block_len), :] = own.astype(BF16)
            mix_turned[p, :, pl.ds(k * block_len, block_len)] = own.T.astype(BF16)
        bias[:, pl.ds(p * lanes, lanes)] = jnp.where(
            first_half, bias_turned[:, 2 * p:2 * p + 1], bias_turned[:, 2 * p + 1:2 * p + 2]
        )

    def strip(level, matrix):
        if matrix == 0:
            return gathered.at[level, c, 0, :, pl.ds(pl.multiple_of(x * wide, wide), wide)]
        return gathered.at[level, c, 1, :, pl.ds(pl.multiple_of(y * tall, tall), tall)]

    def chain(level, way, k, matrix, target):
        block = strip(level, matrix)
        return remote(
            block, block, chain_sem.at[0, way, k - 1, matrix], chain_sem.at[1, way, k - 1, matrix],
            (s, target * CORES + c),
        )

    def nearest(i):
        below, above = z, levels - 1 - z
        shared = jnp.minimum(below, above)
        paired = i < 2 * shared
        k = jnp.where(paired, i // 2 + 1, i - shared + 1)
        way = jnp.where(paired, i % 2, jnp.where(below > above, 0, 1))
        return z - (1 - 2 * way) * k, way, k

    def target_of(i):
        return (z, 0) if i == levels - 1 else nearest(levels - 2 - i)[:2]

    def send_own(act):
        for matrix in range(2):
            @pl.when(z + 1 < levels)
            def _():
                act(chain(z, 0, 1, matrix, z + 1))

            @pl.when(z >= 1)
            def _():
                act(chain(z, 1, 1, matrix, z - 1))

    def pass_on(level, way, k, matrix, act):
        target = z + 1 - 2 * way

        @pl.when((target >= 0) & (target < levels))
        def _():
            act(chain(level, way, k + 1, matrix, target))

    def side(level, way, k, matrix, j):
        block = strip(level, matrix)
        sem = (value_sem, gate_sem)[matrix]
        return remote(
            block, block, sem.at[0, way, k - 1, j - 1], sem.at[1, way, k - 1, j - 1], (x_peer, y_peer)[matrix](j)
        )

    def relay(level, way, k):
        block = gathered.at[level, c]
        return remote(block, block, relay_sem.at[0, way, k - 1], relay_sem.at[1, way, k - 1], partner)

    def both_ways(k, act):
        @pl.when(z >= k)
        def _():
            act(z - k, 0)

        @pl.when(z + k < levels)
        def _():
            act(z + k, 1)

    def arrive(k, matrix):
        def act(level, way):
            chain(level, way, k, matrix, z).wait_recv()
            pass_on(level, way, k, matrix, lambda copy: copy.start())
            for j in range(1, (across, down)[matrix]):
                side(level, way, k, matrix, j).start()

        with jax.named_scope(f"arrive{k}{matrix}"):
            both_ways(k, act)

    def relay_step(k):
        def act(level, way):
            for matrix in range(2):
                for j in range(1, (across, down)[matrix]):
                    side(level, way, k, matrix, j).wait_recv()
            relay(level, way, k).start()

        with jax.named_scope(f"relay{k}"):
            both_ways(k, act)

    def store(level, core):
        index = level * CORES + core
        cut = pl.ds(pl.multiple_of(index * rows_own, rows_own), rows_own)
        return pltpu.make_async_copy(product_in.at[:, cut], input_grad.at[:, cut], store_sem.at[index])

    def project(level, core):
        index = level * CORES + core
        cut = pl.ds(pl.multiple_of(index * rows_own, rows_own), rows_own)
        over = (((1,), (1,)), ((), ()))
        product_in[:, cut] = (
            lax.dot_general(grads[0], gathered[level, core, 0], over, preferred_element_type=F32)
            + lax.dot_general(grads[1], gathered[level, core, 1], over, preferred_element_type=F32)
        ).astype(BF16)
        store(level, core).start()

    def project_level(i):
        level, way, k = nearest(i)
        with jax.named_scope(f"project{i}"):
            relay(level, way, k).wait_recv()
            for core in range(CORES):
                project(level, core)

    def token_swap(i):
        cut = pl.ds(pl.multiple_of(target_of(i)[0] * depth, depth), depth)
        return remote(tokens.at[:, cut], peer_tokens.at[:, cut], token_sem.at[0, i], token_sem.at[1, i], partner)

    shard_swap = remote(
        gathered.at[z, c], gathered.at[z, c], pair_sem.at[0, 1], pair_sem.at[1, 1], partner
    )
    with jax.named_scope("load_acts"):
        for k in (2, 3, 4, 6, 7):
            loads[k].wait()

    gain_grad[...] = jnp.zeros_like(gain_grad)
    shift_grad[...] = jnp.zeros_like(shift_grad)
    turned = (((1,), (1,)), ((), ()))
    grad_swaps = []
    blocks = seq_len // block_len

    def block_grads(b):
        rows = pl.ds(b * block_len, block_len)
        gate = gate_act[rows, :].astype(F32)
        gate_cdf, gate_slope = phi(gate)
        gelu = gate * gate_cdf
        centred = gelu - jnp.mean(gelu, axis=-1, keepdims=True)
        inv_std = lax.rsqrt(jnp.mean(centred * centred, axis=-1, keepdims=True) + EPSILON)
        normed = centred * inv_std
        spread[rows, :] = (normed * gain[...] + shift[...]).astype(BF16)
        value = value_act[rows, :].astype(F32)
        value_cdf, value_slope = phi(value)
        grad_out = cotangent[rows, :].astype(F32)
        grad_spatial = grad_out * (value * value_cdf)
        if b == 0:
            spatial_sum[...] = grad_spatial
        else:
            spatial_sum[...] += grad_spatial
        low[rows, :] = grad_spatial.astype(BF16)
        for p in range(pairs):
            cut = pl.ds(p * lanes, lanes)
            mixed = jnp.dot(mix[p], spread[rows, cut], preferred_element_type=F32)
            spatial[:, cut] = jnp.where(first_half, mixed[:block_len], mixed[block_len:]) + bias[:, cut]
            piece_low = low[rows, cut]
            zero = jnp.zeros_like(piece_low)
            apart = jnp.concatenate(
                (jnp.where(first_half, piece_low, zero), jnp.where(first_half, zero, piece_low)), axis=0
            )
            grad_norm[:, cut] = jnp.dot(mix_turned[p], apart, preferred_element_type=F32)
        back = grad_norm[...]
        gain_grad[...] += jnp.sum(back * normed, axis=0, keepdims=True)
        shift_grad[...] += jnp.sum(back, axis=0, keepdims=True)
        hat = back * gain[...]
        grad_gate = inv_std * (
            hat
            - jnp.mean(hat, axis=-1, keepdims=True)
            - normed * jnp.mean(hat * normed, axis=-1, keepdims=True)
        )
        grads[0, rows, :] = (grad_out * spatial[...] * value_slope).astype(BF16)
        grads[1, rows, :] = (grad_gate * gate_slope).astype(BF16)

    def swap_grads(b):
        rows = pl.ds(b * block_len, block_len)
        grad_swaps.append(remote(
            grads.at[1 - c, rows], peer_grads.at[rows], swap_sem.at[0, b], swap_sem.at[1, b], partner
        ))
        grad_swaps[-1].start()

    with jax.named_scope("block0"):
        block_grads(0)
    with jax.named_scope("barrier"):
        pl.semaphore_wait(pltpu.get_barrier_semaphore(), greeted)
    with jax.named_scope("load_weights"):
        loads[0].wait()
        loads[1].wait()
        send_own(lambda copy: copy.start())
        loads[5].wait()
        token_swap(0).start()
    swap_grads(0)
    for b in range(1, blocks):
        with jax.named_scope(f"block{b}"):
            block_grads(b)
        swap_grads(b)
    for i in range(1, levels):
        token_swap(i).start()

    diagonal = row == column
    per_core = pairs // CORES
    mix_swap = remote(
        mix_part.at[pl.ds((1 - c) * per_core, per_core)], mix_in, pair_sem.at[0, 3], pair_sem.at[1, 3], partner
    )
    small_swap = remote(small.at[1 - c], small_in, pair_sem.at[0, 4], pair_sem.at[1, 4], partner)

    def mix_terms():
        for p in range(pairs):
            cut = pl.ds(p * lanes, lanes)
            straight = jnp.zeros((block_len, block_len), F32)
            flipped = jnp.zeros((block_len, block_len), F32)
            for b in range(blocks):
                rows = pl.ds(b * block_len, block_len)
                inner, piece_low = spread[rows, cut], low[rows, cut]
                zero = jnp.zeros_like(inner)
                straight += lax.dot_general(
                    jnp.where(first_half, piece_low, zero), inner, turned, preferred_element_type=F32
                )
                flipped += lax.dot_general(
                    jnp.where(first_half, zero, inner), piece_low, turned, preferred_element_type=F32
                )
            mix_part[p] = jnp.where(causal, straight, flipped)
            small[1, pairs + p:pairs + p + 1, :] = jnp.sum(jnp.where(diagonal, flipped, 0.0), axis=0, keepdims=True)
        mix_swap.start()
        small[1, pl.ds(2 * pairs, pairs), :] = jnp.zeros((pairs, lanes), F32)
        sums_by_row = jnp.zeros((block_len, lanes), F32)
        for p in range(pairs):
            terms = spatial_sum[:, pl.ds(p * lanes, lanes)]
            left = jnp.sum(jnp.where(first_half, terms, 0.0), axis=1, keepdims=True)
            right = jnp.sum(jnp.where(first_half, 0.0, terms), axis=1, keepdims=True)
            sums_by_row = jnp.where(lane == 2 * p, left, jnp.where(lane == 2 * p + 1, right, sums_by_row))
        small[0, pl.ds(0, groups), :] = sums_by_row.T[:groups]
        for p in range(pairs):
            cut = pl.ds(p * lanes, lanes)
            small[0, groups + p:groups + p + 1, :] = gain_grad[:, cut]
            small[1, p:p + 1, :] = shift_grad[:, cut]
        small_swap.start()

    def first(i, matrix, k):
        if matrix == 0:
            return remote(
                part.at[i, :, :, (x + k) % across, :, pl.ds(0, half)], first_x.at[i, k - 1],
                first_x_sem.at[0, i, k - 1], first_x_sem.at[1, i, k - 1], x_peer(k),
            )
        return remote(
            part.at[i, :, (y + k) % down, :, :, pl.ds(half, half)], first_y.at[i, k - 1],
            first_y_sem.at[0, i, k - 1], first_y_sem.at[1, i, k - 1], y_peer(k),
        )

    def send_chunk(i):
        target = target_of(i)[0]
        cut = pl.ds(pl.multiple_of(target * depth, depth), depth)
        over = (((0,), (0,)), ((), ()))
        def product(left, right, matrix):
            return lax.dot_general(
                left[:, cut], right[:, pl.ds(matrix * half, half)], over, preferred_element_type=F32
            )

        with jax.named_scope(f"chunk{i}"):
            if i == 0:
                for matrix in range(2):
                    held[matrix] = product(tokens, grads.at[c], matrix)
                with jax.named_scope("swaps"):
                    for copy in grad_swaps:
                        copy.wait()
            token_swap(i).wait()
            for matrix in range(2):
                total = held[matrix] if i == 0 else product(tokens, grads.at[c], matrix)
                total = total + product(peer_tokens, peer_grads, matrix)
                part[i, :, :, :, :, pl.ds(matrix * half, half)] = total.reshape(
                    part.shape[1:-1] + (half,)
                ).astype(BF16)
                for k in range(1, (across, down)[matrix]):
                    first(i, matrix, k).start()

    def first_wait(i, matrix):
        for k in range(1, (across, down)[matrix]):
            first(i, matrix, k).wait_recv()

    def pair_sum(i, matrix, r):
        if matrix == 0:
            total = part[i, r, :, x, :, pl.ds(0, half)].astype(F32)
            for k in range(1, across):
                total = total + first_x[i, k - 1, r].astype(F32)
        else:
            total = part[i, r, y, :, :, pl.ds(half, half)].astype(F32)
            for k in range(1, down):
                total = total + first_y[i, k - 1, r].astype(F32)
        return total

    run_out, run_in = (run_out_a, run_out_b), (run_in_a, run_in_b)

    def running(i, level, matrix, upward, r, target):
        return remote(
            run_out[matrix].at[i, r], run_in[matrix].at[level, 1 - upward, r],
            run_sem.at[0, level, matrix, 1 - upward, r], run_sem.at[1, level, matrix, 1 - upward, r],
            (s, target * CORES + c),
        )

    def run(i, matrix):
        level, upward = target_of(i)
        step = 2 * upward - 1
        behind = z - step
        started = (behind >= 0) & (behind < levels)
        with jax.named_scope(f"run{i}{matrix}"):
            first_wait(i, matrix)
            for r in range(CORES):
                total = pair_sum(i, matrix, r)

                @pl.when(started)
                def _():
                    running(i, level, matrix, upward, r, z).wait_recv()
                    run_out[matrix][i, r] = (total + run_in[matrix][level, 1 - upward, r].astype(F32)).astype(BF16)

                @pl.when(jnp.logical_not(started))
                def _():
                    run_out[matrix][i, r] = total.astype(BF16)

                running(i, level, matrix, upward, r, z + step).start()

    def second(matrix, r, j):
        if matrix == 0:
            return remote(
                second_out_a.at[j - 1, r], second_in_a.at[j - 1, r],
                second_a_sem.at[0, j - 1, r], second_a_sem.at[1, j - 1, r], y_peer(j),
            )
        return remote(
            second_out_b.at[j - 1, r], second_in_b.at[j - 1, r],
            second_b_sem.at[0, j - 1, r], second_b_sem.at[1, j - 1, r], x_peer(j),
        )

    def send_second(matrix, r):
        own = (own_a, own_b)[matrix]
        out = (second_out_a, second_out_b)[matrix]
        with jax.named_scope(f"second{matrix}{r}"):
            if r == 0:
                first_wait(levels - 1, matrix)
            own[r] = pair_sum(levels - 1, matrix, r)
            for upward in range(2):
                @pl.when((z >= 1) if upward else (z + 1 < levels))
                def _():
                    running(0, z, matrix, upward, r, z).wait_recv()
                    own[r] += run_in[matrix][z, 1 - upward, r].astype(F32)
            for j in range(1, (down, across)[matrix]):
                index = (y + j) % down if matrix == 0 else (x + j) % across
                out[j - 1, r] = own[r, index].astype(BF16)
                second(matrix, r, j).start()

    def final_swap(matrix):
        return remote(
            final.at[matrix, 1 - c], sums.at[c, s, :, pl.ds(matrix * half, half)],
            final_sem.at[0, matrix], final_sem.at[1, matrix], partner,
        )

    def finish(matrix, r):
        with jax.named_scope(f"finish{matrix}{r}"):
            if matrix == 0:
                total = own_a[r, y]
            else:
                total = own_b[r, x]
            for j in range(1, (down, across)[matrix]):
                second(matrix, r, j).wait_recv()
                total = total + (second_in_a, second_in_b)[matrix][j - 1, r].astype(F32)
            final[matrix, r] = total.astype(BF16)
            for k in range(1, across):
                out_x(r, c, matrix, k).start()
            for k in range(1, down):
                out_y(r, c, matrix, k).start()

            @pl.when(c == r)
            def _():
                sums[c, s, :, pl.ds(matrix * half, half)] = final[matrix, r]

            @pl.when(c != r)
            def _():
                final_swap(matrix).start()

    def out_x(core, matrix, part_at, k):
        return remote(
            final.at[part_at, core], sums.at[matrix, s, :, pl.ds(part_at * half, half)],
            out_x_sem.at[0, part_at, core, k - 1], out_x_sem.at[1, part_at, matrix, k - 1],
            (x_peer(k)[0], z * CORES + core),
        )

    def out_y(core, matrix, part_at, k):
        return remote(
            final.at[part_at, core], sums.at[matrix, s, :, pl.ds(part_at * half, half)],
            out_y_sem.at[0, part_at, core, k - 1], out_y_sem.at[1, part_at, matrix, k - 1],
            (y_peer(k)[0], z * CORES + core),
        )

    def onward(matrix, part_at, k, j):
        columns = pl.ds(part_at * half, half)
        if matrix == 0:
            block = sums.at[0, y * across + (x + across - k) % across, :, columns]
            peer = y_peer(j)
        else:
            block = sums.at[1, ((y + down - k) % down) * across + x, :, columns]
            peer = x_peer(j)
        return remote(
            block, block, out_on_sem.at[0, part_at, matrix, k - 1, j - 1],
            out_on_sem.at[1, part_at, matrix, k - 1, j - 1], peer,
        )

    def out_forward(part_at):
        with jax.named_scope(f"forward{part_at}"):
            for k in range(1, across):
                out_x(0, 0, part_at, k).wait_recv()
                for j in range(1, down):
                    onward(0, part_at, k, j).start()
            for k in range(1, down):
                out_y(0, 1, part_at, k).wait_recv()
                for j in range(1, across):
                    onward(1, part_at, k, j).start()

    def out_end(part_at):
        with jax.named_scope(f"end{part_at}"):
            for k in range(1, across):
                out_x(0, 1, part_at, k).wait_recv()
                for j in range(1, down):
                    onward(0, part_at, k, j).wait()
            for k in range(1, down):
                out_y(0, 0, part_at, k).wait_recv()
                for j in range(1, across):
                    onward(1, part_at, k, j).wait()
            final_swap(part_at).wait()
            for matrix in range(2):
                results[2 * part_at + matrix].start()

    def mix_scatter(k):
        return remote(
            mix_low.at[(z + k) % levels], mix_level.at[k - 1],
            mix_level_sem.at[0, k - 1], mix_level_sem.at[1, k - 1], in_level(k),
        )

    def small_scatter(k):
        return remote(
            small_level.at[z], small_level.at[z],
            small_level_sem.at[0, k - 1], small_level_sem.at[1, k - 1], in_level(k),
        )

    def mix_spread(k):
        return remote(
            mix_plane.at[s], mix_plane.at[s], mix_sem.at[0, k - 1], mix_sem.at[1, k - 1], in_plane(k)
        )

    def small_spread(k):
        return remote(
            small_plane.at[s], small_plane.at[s], small_sem.at[0, k - 1], small_sem.at[1, k - 1], in_plane(k)
        )

    def mix_gather(k):
        block = mix_all.at[c, z]
        return remote(block, block, mix_out_sem.at[0, k - 1], mix_out_sem.at[1, k - 1], in_level(k))

    small_back = remote(small_all.at[c], small_all.at[c], pair_sem.at[0, 2], pair_sem.at[1, 2], partner)
    mix_back = remote(mix_all.at[c], mix_all.at[c], pair_sem.at[0, 5], pair_sem.at[1, 5], partner)

    def mix_stage(stage):
        with jax.named_scope(f"mix{stage}"):
            mix_step(stage)

    def mix_step(stage):
        if stage == 0:
            mix_swap.wait()
            small_swap.wait()
            mine = mix_part[pl.ds(c * per_core, per_core)] + mix_in[...]
            mix_low[...] = mine.reshape(mix_low.shape).astype(BF16)
            small_level[z] = small[c] + small_in[...]
            for k in range(1, levels):
                mix_scatter(k).start()
                small_scatter(k).start()
        elif stage == 1:
            total = mix_low[z].astype(F32)
            for k in range(1, levels):
                mix_scatter(k).wait()
                small_scatter(k).wait()
                total = total + mix_level[k - 1].astype(F32)
            mix_plane[s] = total.astype(BF16)
            whole = small_level[0]
            for k in range(1, levels):
                whole = whole + small_level[k]
            small_plane[s] = whole
            for k in range(1, ways):
                mix_spread(k).start()
                small_spread(k).start()
        elif stage == 2:
            for k in range(1, ways):
                mix_spread(k).wait()
                small_spread(k).wait()
            total = mix_plane[0].astype(F32)
            whole = small_plane[0]
            for k in range(1, ways):
                total = total + mix_plane[k].astype(F32)
                whole = whole + small_plane[k]
            mix_all[c, z] = total.astype(BF16)
            small_all[c] = whole
            for k in range(1, levels):
                mix_gather(k).start()
        elif stage == 3:
            for k in range(1, levels):
                mix_gather(k).wait()
            mix_back.start()
            small_back.start()
        else:
            mix_back.wait()
            small_back.wait()
            packed_all = mix_all[...].reshape(pairs, block_len, block_len)
            for p in range(pairs):
                packed = packed_all[p].astype(F32)
                on_diagonal = jnp.where(diagonal, small_all[1, pairs + p:pairs + p + 1, :], 0.0)
                mix_ready[2 * p] = jnp.where(causal, packed, 0.0).astype(BF16)
                mix_ready[2 * p + 1] = jnp.where(row > column, packed.T, on_diagonal).astype(BF16)
            results[4].start()
            results[5].start()

    results = [
        pltpu.make_async_copy(
            sums.at[matrix, :, :, pl.ds(part_at * half, half)],
            (value_out, gate_out)[matrix].at[:, :, pl.ds(part_at * half, half)],
            result_sem.at[2 * part_at + matrix],
        )
        for part_at in range(2) for matrix in range(2)
    ] + [
        pltpu.make_async_copy(mix_ready, mix_out, result_sem.at[4]),
        pltpu.make_async_copy(small_all, small_out, result_sem.at[5]),
    ]

    chunks = list(range(levels))
    send_chunk(chunks.pop(0))
    shard_swap.start()
    send_chunk(chunks.pop(0))
    with jax.named_scope("mix_terms"):
        mix_terms()
    arrive(1, 0)
    if chunks:
        send_chunk(chunks.pop(0))
    arrive(1, 1)
    run(0, 0)
    run(0, 1)
    for i in range(1, levels - 1):
        last = i == levels - 2
        if last:
            run(i, 0)
        arrive(i + 1, 0)
        arrive(i + 1, 1)
        if not last:
            run(i, 0)
        if chunks:
            send_chunk(chunks.pop(0))
        run(i, 1)
    mix_stage(0)
    with jax.named_scope("project_own"):
        project(z, c)
        shard_swap.wait()
        project(z, 1 - c)
    for k in range(1, levels - 1):
        relay_step(k)
    send_second(0, 0)
    send_second(0, 1)
    send_second(1, 0)
    send_second(1, 1)
    mix_stage(1)
    finish(0, 0)
    finish(0, 1)
    relay_step(levels - 1)
    finish(1, 0)
    finish(1, 1)
    mix_stage(2)
    out_forward(0)
    project_level(0)
    out_forward(1)
    mix_stage(3)
    for i in range(1, levels - 1):
        project_level(i)
    mix_stage(4)
    out_end(0)
    out_end(1)

    send_own(lambda copy: copy.wait_send())
    for i in range(levels - 1):
        level, way, k = nearest(i)
        for matrix in range(2):
            pass_on(level, way, k, matrix, lambda copy: copy.wait_send())
            for j in range(1, (across, down)[matrix]):
                side(level, way, k, matrix, j).wait_send()
        relay(level, way, k).wait_send()
        level, upward = target_of(i)
        for matrix in range(2):
            for r in range(CORES):
                running(i, level, matrix, upward, r, z + 2 * upward - 1).wait_send()
    for matrix in range(2):
        for i in range(levels):
            for k in range(1, (across, down)[matrix]):
                first(i, matrix, k).wait_send()
        for j in range(1, (down, across)[matrix]):
            for r in range(CORES):
                second(matrix, r, j).wait_send()
        for part_at in range(2):
            for k in range(1, across):
                out_x(matrix, 0, part_at, k).wait_send()
            for k in range(1, down):
                out_y(matrix, 0, part_at, k).wait_send()
    with jax.named_scope("stores"):
        for level in range(levels):
            for core in range(CORES):
                store(level, core).wait()
        for copy in results:
            copy.wait()


def write_out(
    input_grad, value_sums, gate_sums, mix_grad, small,
    input_out, value_out, gate_out, mix_out, bias_out, gain_out, shift_out,
    held, value_low, gate_low, mix_low, few, value_full, gate_full, mix_full, load_sem, store_sem,
):
    cuts = held.shape[0]
    tall = held.shape[1]
    groups = bias_out.shape[0]
    pairs = groups // 2
    loads = [
        pltpu.make_async_copy(value_sums, value_low, load_sem.at[0]),
        pltpu.make_async_copy(gate_sums, gate_low, load_sem.at[1]),
        pltpu.make_async_copy(mix_grad, mix_low, load_sem.at[2]),
        pltpu.make_async_copy(small, few, load_sem.at[3]),
    ] + [
        pltpu.make_async_copy(input_grad.at[pl.ds(i * tall, tall)], held.at[i], load_sem.at[4 + i]) for i in range(cuts)
    ]
    stores = [
        pltpu.make_async_copy(value_full, value_out, store_sem.at[0]),
        pltpu.make_async_copy(gate_full, gate_out, store_sem.at[1]),
        pltpu.make_async_copy(mix_full, mix_out, store_sem.at[2]),
        pltpu.make_async_copy(few.at[0, pl.ds(0, groups)], bias_out, store_sem.at[3]),
        pltpu.make_async_copy(few.at[0, pl.ds(groups, pairs)], gain_out, store_sem.at[4]),
        pltpu.make_async_copy(few.at[1, pl.ds(0, pairs)], shift_out, store_sem.at[5]),
    ] + [
        pltpu.make_async_copy(held.at[i], input_out.at[pl.ds(i * tall, tall)], store_sem.at[6 + i]) for i in range(cuts)
    ]
    for copy in loads[4:] + loads[:4]:
        copy.start()
    for i in range(cuts):
        loads[4 + i].wait()
        stores[6 + i].start()
    for i, (low, full) in enumerate(((value_low, value_full), (gate_low, gate_full), (mix_low, mix_full))):
        loads[i].wait()
        full[...] = low[...].reshape(full.shape).astype(F32)
        stores[i].start()
    loads[3].wait()
    for i in range(3, 6):
        stores[i].start()
    for copy in stores:
        copy.wait()


def shards(
    tokens,
    value_act,
    gate_act,
    cotangent,
    value_weight,
    gate_weight,
    norm_gain,
    norm_bias,
    mix_weight,
    mix_bias,
):
    ways = lax.axis_size("sp")
    levels = lax.axis_size("dp") // CORES
    across, down = plane_of(ways)
    inputs = tokens[0]
    seq_len, width = inputs.shape
    channels = value_act.shape[2]
    groups, block_len = mix_weight.shape[0], mix_weight.shape[1]
    pairs = groups // 2
    lanes = channels // pairs
    rows = value_weight.shape[0]
    share = rows // ways
    half = channels // 2
    anywhere = pl.BlockSpec(memory_space=pl.ANY)
    sems = pltpu.SemaphoreType.DMA
    mix_rows = pairs * block_len // (CORES * levels)
    small_shape = (CORES, 3 * pairs, lanes)
    shape = jax.ShapeDtypeStruct
    input_grad, value_sums, gate_sums, mix_out, small = pl.pallas_call(
        functools.partial(kernel, ways, levels),
        out_shape=(
            shape((seq_len, width), BF16),
            shape((ways, share, channels), BF16),
            shape((ways, share, channels), BF16),
            shape((groups, block_len, block_len), BF16),
            shape(small_shape, F32),
        ),
        in_specs=[anywhere] * 10,
        out_specs=(anywhere,) * 5,
        scratch_shapes=[
            pltpu.VMEM((seq_len, width), BF16),
            pltpu.VMEM((seq_len, channels), BF16),
            pltpu.VMEM((seq_len, channels), BF16),
            pltpu.VMEM((seq_len, channels), BF16),
            pltpu.VMEM((1, channels), F32),
            pltpu.VMEM((1, channels), F32),
            pltpu.VMEM((groups, block_len, block_len), BF16),
            pltpu.VMEM((groups, block_len), F32),
            pltpu.VMEM((pairs, 2 * block_len, block_len), BF16),
            pltpu.VMEM((pairs, block_len, 2 * block_len), BF16),
            pltpu.VMEM((block_len, channels), F32),
            pltpu.VMEM((2, seq_len, channels), BF16),
            pltpu.VMEM((seq_len, width), BF16),
            pltpu.VMEM((seq_len, channels), BF16),
            pltpu.VMEM((levels, CORES, 2, rows, channels), BF16),
            pltpu.VMEM((block_len, channels), F32),
            pltpu.VMEM((1, channels), F32),
            pltpu.VMEM((1, channels), F32),
            pltpu.VMEM((seq_len, channels), BF16),
            pltpu.VMEM((seq_len, channels), BF16),
            pltpu.VMEM((block_len, channels), F32),
            pltpu.VMEM((block_len, channels), F32),
            pltpu.VMEM((seq_len, width), BF16),
            pltpu.VMEM((2, width // levels, half), F32),
            pltpu.VMEM((levels, CORES, down, across, share, channels), BF16),
            pltpu.VMEM((levels, across - 1, CORES, down, share, half), BF16),
            pltpu.VMEM((levels, down - 1, CORES, across, share, half), BF16),
            pltpu.VMEM((levels - 1, CORES, down, share, half), BF16),
            pltpu.VMEM((levels, 2, CORES, down, share, half), BF16),
            pltpu.VMEM((levels - 1, CORES, across, share, half), BF16),
            pltpu.VMEM((levels, 2, CORES, across, share, half), BF16),
            pltpu.VMEM((CORES, down, share, half), F32),
            pltpu.VMEM((CORES, across, share, half), F32),
            pltpu.VMEM((down - 1, CORES, share, half), BF16),
            pltpu.VMEM((down - 1, CORES, share, half), BF16),
            pltpu.VMEM((across - 1, CORES, share, half), BF16),
            pltpu.VMEM((across - 1, CORES, share, half), BF16),
            pltpu.VMEM((2, CORES, share, half), BF16),
            pltpu.VMEM((2, ways, share, channels), BF16),
            pltpu.VMEM((pairs, block_len, block_len), F32),
            pltpu.VMEM((pairs // CORES, block_len, block_len), F32),
            pltpu.VMEM((levels, mix_rows, block_len), BF16),
            pltpu.VMEM((ways, mix_rows, block_len), BF16),
            pltpu.VMEM((levels - 1, mix_rows, block_len), BF16),
            pltpu.VMEM((CORES, levels, mix_rows, block_len), BF16),
            pltpu.VMEM((groups, block_len, block_len), BF16),
            pltpu.VMEM(small_shape, F32),
            pltpu.VMEM(small_shape[1:], F32),
            pltpu.VMEM((ways,) + small_shape[1:], F32),
            pltpu.VMEM((levels,) + small_shape[1:], F32),
            pltpu.VMEM(small_shape, F32),
            sems((10,)),
            sems((levels * CORES,)),
            sems((6,)),
            sems((2, levels)),
            sems((2, 6)),
            sems((2, seq_len // block_len)),
            sems((2, 2, levels - 1, 2)),
            sems((2, 2, levels - 1, across - 1)),
            sems((2, 2, levels - 1, down - 1)),
            sems((2, 2, levels - 1)),
            sems((2, levels, across - 1)),
            sems((2, levels, down - 1)),
            sems((2, levels, 2, 2, CORES)),
            sems((2, down - 1, CORES)),
            sems((2, across - 1, CORES)),
            sems((2, 2)),
            sems((2, 2, 2, across - 1)),
            sems((2, 2, 2, down - 1)),
            sems((2, 2, 2, max(across, down) - 1, max(across, down) - 1)),
            sems((2, ways - 1)),
            sems((2, levels - 1)),
            sems((2, levels - 1)),
            sems((2, ways - 1)),
            sems((2, levels - 1)),
        ],
        compiler_params=pltpu.CompilerParams(
            collective_id=0, has_side_effects=True, vmem_limit_bytes=60 * 1024 * 1024
        ),
        name="unit",
    )(
        inputs, value_weight, gate_weight, value_act[0], gate_act[0], cotangent[0],
        norm_gain[None], norm_bias[None], mix_weight, mix_bias,
    )
    cuts = 6
    low_shape, full_shape, mix_full = (ways, share, channels), (rows, channels), (groups, block_len, block_len)
    input_grad, value_grad, gate_grad, mix_grad, bias_grad, gain_grad, shift_grad = pl.pallas_call(
        write_out,
        out_shape=(
            shape((seq_len, width), BF16),
            shape(full_shape, F32),
            shape(full_shape, F32),
            shape(mix_full, F32),
            shape((groups, block_len), F32),
            shape((pairs, lanes), F32),
            shape((pairs, lanes), F32),
        ),
        in_specs=[anywhere] * 5,
        out_specs=(anywhere,) * 7,
        scratch_shapes=[
            pltpu.VMEM((cuts, seq_len // cuts, width), BF16),
            pltpu.VMEM(low_shape, BF16),
            pltpu.VMEM(low_shape, BF16),
            pltpu.VMEM(mix_full, BF16),
            pltpu.VMEM(small_shape, F32),
            pltpu.VMEM(full_shape, F32),
            pltpu.VMEM(full_shape, F32),
            pltpu.VMEM(mix_full, F32),
            sems((4 + cuts,)),
            sems((6 + cuts,)),
        ],
        name="write_out",
    )(input_grad, value_sums, gate_sums, mix_out, small)
    return (
        input_grad[None],
        value_grad,
        gate_grad,
        mix_grad,
        bias_grad,
        gain_grad.reshape(-1),
        shift_grad.reshape(-1),
    )


def solution(mesh):
    placed = (
        P("dp", "sp", None),
        P("dp", "sp", None),
        P("dp", "sp", None),
        P("dp", "sp", None),
        P("dp", None),
        P("dp", None),
        P(),
        P(),
        P(),
        P(),
    )
    return jax.shard_map(
        shards,
        mesh=mesh,
        in_specs=placed,
        out_specs=(P("dp", "sp", None), P("dp", None), P("dp", None), P(), P(), P(), P()),
        check_vma=False,
    )
```

```python
import functools

import jax
import jax.numpy as jnp
from jax import lax
from jax.experimental import pallas as pl
from jax.experimental.pallas import tpu as pltpu
from jax.sharding import PartitionSpec as P

EPSILON = 1e-06
CORES = 2
MESH = pl.DeviceIdType.MESH
F32 = jnp.float32
BF16 = jnp.bfloat16


def remote(src, dst, send, recv, device):
    return pltpu.make_async_remote_copy(
        src_ref=src, dst_ref=dst, send_sem=send, recv_sem=recv, device_id=device, device_id_type=MESH
    )


def position():
    s, d = lax.axis_index("sp"), lax.axis_index("dp")
    return s, d, d // CORES, d % CORES


def plane_of(ways):
    across = max(k for k in range(1, ways + 1) if ways % k == 0 and k * k <= ways)
    return across, ways // across


def signal_all(ways, levels, s, d, z, c):
    barrier = pltpu.get_barrier_semaphore()
    for k in range(1, ways):
        pl.semaphore_signal(barrier, inc=1, device_id=((s + k) % ways, d), device_id_type=MESH)
    for k in range(1, levels):
        other = ((z + k) % levels) * CORES + c
        pl.semaphore_signal(barrier, inc=1, device_id=(s, other), device_id_type=MESH)
    pl.semaphore_signal(barrier, inc=1, device_id=(s, d + 1 - 2 * c), device_id_type=MESH)
    across, down = plane_of(ways)
    x, y, beside = s % across, s // across, d + 1 - 2 * c
    for k in range(1, across):
        pl.semaphore_signal(barrier, inc=1, device_id=(y * across + (x + k) % across, beside), device_id_type=MESH)
    for k in range(1, down):
        pl.semaphore_signal(barrier, inc=1, device_id=(((y + k) % down) * across + x, beside), device_id_type=MESH)
    return ways - 1 + levels - 1 + 1 + across - 1 + down - 1


def phi(values):
    cdf_part = 0.5 * (1.0 + lax.erf(values * 0.7071067811865476))
    pdf_part = jnp.exp(-0.5 * values * values) * 0.3989422804014327
    return cdf_part, cdf_part + values * pdf_part


def kernel(
    ways, levels,
    tokens_hbm, value_weight, gate_weight, value_hbm, gate_hbm, cotangent_hbm,
    gain_hbm, shift_hbm, mix_hbm, mix_bias_hbm,
    input_grad, value_out, gate_out, mix_out, small_out,
    tokens, value_act, gate_act, cotangent, gain, shift, mix_raw, mix_bias, mix, mix_turned, bias,
    grads, peer_tokens, peer_grads, gathered, spatial_sum, gain_grad, shift_grad,
    spread, low, spatial, grad_norm, product_in,
    held, part, first_x, first_y, run_out_a, run_in_a, run_out_b, run_in_b, own_a, own_b,
    second_out_a, second_in_a, second_out_b, second_in_b, final, sums,
    mix_part, mix_in, mix_low, mix_plane, mix_level, mix_all, mix_ready,
    small, small_in, small_plane, small_level, small_all,
    load_sem, store_sem, result_sem, token_sem, pair_sem, swap_sem, chain_sem, value_sem, gate_sem, relay_sem,
    first_x_sem, first_y_sem, run_sem, second_a_sem, second_b_sem, final_sem, out_x_sem, out_y_sem, out_on_sem,
    mix_sem, mix_level_sem, mix_out_sem, small_sem, small_level_sem,
):
    s, d, z, c = position()
    across, down = plane_of(ways)
    x, y = s % across, s // across
    partner = (s, d + 1 - 2 * c)
    seq_len, channels = value_act.shape
    pairs, double, block_len = mix_turned.shape[0], mix_turned.shape[2], mix_turned.shape[1]
    lanes = channels // pairs
    groups = 2 * pairs
    rows_own = value_weight.shape[0]
    model = tokens.shape[1]
    depth = model // levels
    half = channels // 2
    share = rows_own // ways
    wide, tall = channels // across, channels // down

    def x_peer(k):
        return (y * across + (x + k) % across, d)

    def y_peer(k):
        return (((y + k) % down) * across + x, d)

    def in_plane(k):
        return ((s + k) % ways, d)

    def in_level(k):
        return (s, ((z + k) % levels) * CORES + c)

    loads = [
        pltpu.make_async_copy(value_weight, gathered.at[z, c, 0], load_sem.at[0]),
        pltpu.make_async_copy(gate_weight, gathered.at[z, c, 1], load_sem.at[1]),
        pltpu.make_async_copy(gate_hbm, gate_act, load_sem.at[2]),
        pltpu.make_async_copy(value_hbm, value_act, load_sem.at[3]),
        pltpu.make_async_copy(cotangent_hbm, cotangent, load_sem.at[4]),
        pltpu.make_async_copy(tokens_hbm, tokens, load_sem.at[5]),
        pltpu.make_async_copy(gain_hbm, gain, load_sem.at[6]),
        pltpu.make_async_copy(shift_hbm, shift, load_sem.at[7]),
        pltpu.make_async_copy(mix_hbm, mix_raw, load_sem.at[8]),
        pltpu.make_async_copy(mix_bias_hbm, mix_bias, load_sem.at[9]),
    ]
    greeted = signal_all(ways, levels, s, d, z, c)
    for k in (9, 8, 2, 3, 4, 6, 7, 0, 1, 5):
        loads[k].start()

    row = lax.broadcasted_iota(jnp.int32, (block_len, block_len), 0)
    column = lax.broadcasted_iota(jnp.int32, (block_len, block_len), 1)
    causal = row >= column
    lane = lax.broadcasted_iota(jnp.int32, (block_len, lanes), 1)
    first_half = lane < lanes // 2
    with jax.named_scope("load_mix"):
        loads[9].wait()
        loads[8].wait()
    bias_turned = mix_bias[...].T
    for p in range(pairs):
        for k in range(2):
            own = jnp.where(causal, mix_raw[2 * p + k].astype(F32), 0.0)
            mix[p, pl.ds(k * block_len, block_len), :] = own.astype(BF16)
            mix_turned[p, :, pl.ds(k * block_len, block_len)] = own.T.astype(BF16)
        bias[:, pl.ds(p * lanes, lanes)] = jnp.where(
            first_half, bias_turned[:, 2 * p:2 * p + 1], bias_turned[:, 2 * p + 1:2 * p + 2]
        )

    def strip(level, matrix):
        if matrix == 0:
            return gathered.at[level, c, 0, :, pl.ds(pl.multiple_of(x * wide, wide), wide)]
        return gathered.at[level, c, 1, :, pl.ds(pl.multiple_of(y * tall, tall), tall)]

    def chain(level, way, k, matrix, target):
        block = strip(level, matrix)
        return remote(
            block, block, chain_sem.at[0, way, k - 1, matrix], chain_sem.at[1, way, k - 1, matrix],
            (s, target * CORES + c),
        )

    def nearest(i):
        below, above = z, levels - 1 - z
        shared = jnp.minimum(below, above)
        paired = i < 2 * shared
        k = jnp.where(paired, i // 2 + 1, i - shared + 1)
        way = jnp.where(paired, i % 2, jnp.where(below > above, 0, 1))
        return z - (1 - 2 * way) * k, way, k

    def target_of(i):
        return (z, 0) if i == levels - 1 else nearest(levels - 2 - i)[:2]

    def send_own(act):
        for matrix in range(2):
            @pl.when(z + 1 < levels)
            def _():
                act(chain(z, 0, 1, matrix, z + 1))

            @pl.when(z >= 1)
            def _():
                act(chain(z, 1, 1, matrix, z - 1))

    def pass_on(level, way, k, matrix, act):
        target = z + 1 - 2 * way

        @pl.when((target >= 0) & (target < levels))
        def _():
            act(chain(level, way, k + 1, matrix, target))

    def side(level, way, k, matrix, j):
        block = strip(level, matrix)
        sem = (value_sem, gate_sem)[matrix]
        return remote(
            block, block, sem.at[0, way, k - 1, j - 1], sem.at[1, way, k - 1, j - 1], (x_peer, y_peer)[matrix](j)
        )

    def relay(level, way, k):
        block = gathered.at[level, c]
        return remote(block, block, relay_sem.at[0, way, k - 1], relay_sem.at[1, way, k - 1], partner)

    def both_ways(k, act):
        @pl.when(z >= k)
        def _():
            act(z - k, 0)

        @pl.when(z + k < levels)
        def _():
            act(z + k, 1)

    def arrive(k, matrix):
        def act(level, way):
            chain(level, way, k, matrix, z).wait_recv()
            pass_on(level, way, k, matrix, lambda copy: copy.start())
            for j in range(1, (across, down)[matrix]):
                side(level, way, k, matrix, j).start()

        with jax.named_scope(f"arrive{k}{matrix}"):
            both_ways(k, act)

    def relay_step(k):
        def act(level, way):
            for matrix in range(2):
                for j in range(1, (across, down)[matrix]):
                    side(level, way, k, matrix, j).wait_recv()
            relay(level, way, k).start()

        with jax.named_scope(f"relay{k}"):
            both_ways(k, act)

    def store(level, core):
        index = level * CORES + core
        cut = pl.ds(pl.multiple_of(index * rows_own, rows_own), rows_own)
        return pltpu.make_async_copy(product_in.at[:, cut], input_grad.at[:, cut], store_sem.at[index])

    def project(level, core):
        index = level * CORES + core
        cut = pl.ds(pl.multiple_of(index * rows_own, rows_own), rows_own)
        over = (((1,), (1,)), ((), ()))
        product_in[:, cut] = (
            lax.dot_general(grads[0], gathered[level, core, 0], over, preferred_element_type=F32)
            + lax.dot_general(grads[1], gathered[level, core, 1], over, preferred_element_type=F32)
        ).astype(BF16)
        store(level, core).start()

    def project_level(i):
        level, way, k = nearest(i)
        with jax.named_scope(f"project{i}"):
            relay(level, way, k).wait_recv()
            for core in range(CORES):
                project(level, core)

    def token_swap(i):
        cut = pl.ds(pl.multiple_of(target_of(i)[0] * depth, depth), depth)
        return remote(tokens.at[:, cut], peer_tokens.at[:, cut], token_sem.at[0, i], token_sem.at[1, i], partner)

    shard_swap = remote(
        gathered.at[z, c], gathered.at[z, c], pair_sem.at[0, 1], pair_sem.at[1, 1], partner
    )
    with jax.named_scope("load_acts"):
        for k in (2, 3, 4, 6, 7):
            loads[k].wait()

    gain_grad[...] = jnp.zeros_like(gain_grad)
    shift_grad[...] = jnp.zeros_like(shift_grad)
    turned = (((1,), (1,)), ((), ()))
    grad_swaps = []
    blocks = seq_len // block_len

    def block_grads(b):
        rows = pl.ds(b * block_len, block_len)
        gate = gate_act[rows, :].astype(F32)
        gate_cdf, gate_slope = phi(gate)
        gelu = gate * gate_cdf
        centred = gelu - jnp.mean(gelu, axis=-1, keepdims=True)
        inv_std = lax.rsqrt(jnp.mean(centred * centred, axis=-1, keepdims=True) + EPSILON)
        normed = centred * inv_std
        spread[rows, :] = (normed * gain[...] + shift[...]).astype(BF16)
        value = value_act[rows, :].astype(F32)
        value_cdf, value_slope = phi(value)
        grad_out = cotangent[rows, :].astype(F32)
        grad_spatial = grad_out * (value * value_cdf)
        if b == 0:
            spatial_sum[...] = grad_spatial
        else:
            spatial_sum[...] += grad_spatial
        low[rows, :] = grad_spatial.astype(BF16)
        for p in range(pairs):
            cut = pl.ds(p * lanes, lanes)
            mixed = jnp.dot(mix[p], spread[rows, cut], preferred_element_type=F32)
            spatial[:, cut] = jnp.where(first_half, mixed[:block_len], mixed[block_len:]) + bias[:, cut]
            piece_low = low[rows, cut]
            zero = jnp.zeros_like(piece_low)
            apart = jnp.concatenate(
                (jnp.where(first_half, piece_low, zero), jnp.where(first_half, zero, piece_low)), axis=0
            )
            grad_norm[:, cut] = jnp.dot(mix_turned[p], apart, preferred_element_type=F32)
        back = grad_norm[...]
        gain_grad[...] += jnp.sum(back * normed, axis=0, keepdims=True)
        shift_grad[...] += jnp.sum(back, axis=0, keepdims=True)
        hat = back * gain[...]
        grad_gate = inv_std * (
            hat
            - jnp.mean(hat, axis=-1, keepdims=True)
            - normed * jnp.mean(hat * normed, axis=-1, keepdims=True)
        )
        grads[0, rows, :] = (grad_out * spatial[...] * value_slope).astype(BF16)
        grads[1, rows, :] = (grad_gate * gate_slope).astype(BF16)

    def swap_grads(b):
        rows = pl.ds(b * block_len, block_len)
        grad_swaps.append(remote(
            grads.at[1 - c, rows], peer_grads.at[rows], swap_sem.at[0, b], swap_sem.at[1, b], partner
        ))
        grad_swaps[-1].start()

    with jax.named_scope("block0"):
        block_grads(0)
    with jax.named_scope("barrier"):
        pl.semaphore_wait(pltpu.get_barrier_semaphore(), greeted)
    with jax.named_scope("load_weights"):
        loads[0].wait()
        loads[1].wait()
        send_own(lambda copy: copy.start())
        loads[5].wait()
        token_swap(0).start()
    swap_grads(0)
    for b in range(1, blocks):
        with jax.named_scope(f"block{b}"):
            block_grads(b)
        swap_grads(b)
    for i in range(1, levels):
        token_swap(i).start()

    diagonal = row == column
    per_core = pairs // CORES
    mix_swap = remote(
        mix_part.at[pl.ds((1 - c) * per_core, per_core)], mix_in, pair_sem.at[0, 3], pair_sem.at[1, 3], partner
    )
    small_swap = remote(small.at[1 - c], small_in, pair_sem.at[0, 4], pair_sem.at[1, 4], partner)

    def mix_terms():
        for p in range(pairs):
            cut = pl.ds(p * lanes, lanes)
            straight = jnp.zeros((block_len, block_len), F32)
            flipped = jnp.zeros((block_len, block_len), F32)
            for b in range(blocks):
                rows = pl.ds(b * block_len, block_len)
                inner, piece_low = spread[rows, cut], low[rows, cut]
                zero = jnp.zeros_like(inner)
                straight += lax.dot_general(
                    jnp.where(first_half, piece_low, zero), inner, turned, preferred_element_type=F32
                )
                flipped += lax.dot_general(
                    jnp.where(first_half, zero, inner), piece_low, turned, preferred_element_type=F32
                )
            mix_part[p] = jnp.where(causal, straight, flipped)
            small[1, pairs + p:pairs + p + 1, :] = jnp.sum(jnp.where(diagonal, flipped, 0.0), axis=0, keepdims=True)
        mix_swap.start()
        small[1, pl.ds(2 * pairs, pairs), :] = jnp.zeros((pairs, lanes), F32)
        sums_by_row = jnp.zeros((block_len, lanes), F32)
        for p in range(pairs):
            terms = spatial_sum[:, pl.ds(p * lanes, lanes)]
            left = jnp.sum(jnp.where(first_half, terms, 0.0), axis=1, keepdims=True)
            right = jnp.sum(jnp.where(first_half, 0.0, terms), axis=1, keepdims=True)
            sums_by_row = jnp.where(lane == 2 * p, left, jnp.where(lane == 2 * p + 1, right, sums_by_row))
        small[0, pl.ds(0, groups), :] = sums_by_row.T[:groups]
        for p in range(pairs):
            cut = pl.ds(p * lanes, lanes)
            small[0, groups + p:groups + p + 1, :] = gain_grad[:, cut]
            small[1, p:p + 1, :] = shift_grad[:, cut]
        small_swap.start()

    def first(i, matrix, k):
        if matrix == 0:
            return remote(
                part.at[i, :, :, (x + k) % across, :, pl.ds(0, half)], first_x.at[i, k - 1],
                first_x_sem.at[0, i, k - 1], first_x_sem.at[1, i, k - 1], x_peer(k),
            )
        return remote(
            part.at[i, :, (y + k) % down, :, :, pl.ds(half, half)], first_y.at[i, k - 1],
            first_y_sem.at[0, i, k - 1], first_y_sem.at[1, i, k - 1], y_peer(k),
        )

    def send_chunk(i):
        target = target_of(i)[0]
        cut = pl.ds(pl.multiple_of(target * depth, depth), depth)
        over = (((0,), (0,)), ((), ()))
        def product(left, right, matrix):
            return lax.dot_general(
                left[:, cut], right[:, pl.ds(matrix * half, half)], over, preferred_element_type=F32
            )

        with jax.named_scope(f"chunk{i}"):
            if i == 0:
                for matrix in range(2):
                    held[matrix] = product(tokens, grads.at[c], matrix)
                with jax.named_scope("swaps"):
                    for copy in grad_swaps:
                        copy.wait()
            token_swap(i).wait()
            for matrix in range(2):
                total = held[matrix] if i == 0 else product(tokens, grads.at[c], matrix)
                total = total + product(peer_tokens, peer_grads, matrix)
                part[i, :, :, :, :, pl.ds(matrix * half, half)] = total.reshape(
                    part.shape[1:-1] + (half,)
                ).astype(BF16)
                for k in range(1, (across, down)[matrix]):
                    first(i, matrix, k).start()

    def first_wait(i, matrix):
        for k in range(1, (across, down)[matrix]):
            first(i, matrix, k).wait_recv()

    def pair_sum(i, matrix, r):
        if matrix == 0:
            total = part[i, r, :, x, :, pl.ds(0, half)].astype(F32)
            for k in range(1, across):
                total = total + first_x[i, k - 1, r].astype(F32)
        else:
            total = part[i, r, y, :, :, pl.ds(half, half)].astype(F32)
            for k in range(1, down):
                total = total + first_y[i, k - 1, r].astype(F32)
        return total

    run_out, run_in = (run_out_a, run_out_b), (run_in_a, run_in_b)

    def running(i, level, matrix, upward, r, target):
        return remote(
            run_out[matrix].at[i, r], run_in[matrix].at[level, 1 - upward, r],
            run_sem.at[0, level, matrix, 1 - upward, r], run_sem.at[1, level, matrix, 1 - upward, r],
            (s, target * CORES + c),
        )

    def run(i, matrix):
        level, upward = target_of(i)
        step = 2 * upward - 1
        behind = z - step
        started = (behind >= 0) & (behind < levels)
        with jax.named_scope(f"run{i}{matrix}"):
            first_wait(i, matrix)
            for r in range(CORES):
                total = pair_sum(i, matrix, r)

                @pl.when(started)
                def _():
                    running(i, level, matrix, upward, r, z).wait_recv()
                    run_out[matrix][i, r] = (total + run_in[matrix][level, 1 - upward, r].astype(F32)).astype(BF16)

                @pl.when(jnp.logical_not(started))
                def _():
                    run_out[matrix][i, r] = total.astype(BF16)

                running(i, level, matrix, upward, r, z + step).start()

    def second(matrix, r, j):
        if matrix == 0:
            return remote(
                second_out_a.at[j - 1, r], second_in_a.at[j - 1, r],
                second_a_sem.at[0, j - 1, r], second_a_sem.at[1, j - 1, r], y_peer(j),
            )
        return remote(
            second_out_b.at[j - 1, r], second_in_b.at[j - 1, r],
            second_b_sem.at[0, j - 1, r], second_b_sem.at[1, j - 1, r], x_peer(j),
        )

    def send_second(matrix, r):
        own = (own_a, own_b)[matrix]
        out = (second_out_a, second_out_b)[matrix]
        with jax.named_scope(f"second{matrix}{r}"):
            if r == 0:
                first_wait(levels - 1, matrix)
            own[r] = pair_sum(levels - 1, matrix, r)
            for upward in range(2):
                @pl.when((z >= 1) if upward else (z + 1 < levels))
                def _():
                    running(0, z, matrix, upward, r, z).wait_recv()
                    own[r] += run_in[matrix][z, 1 - upward, r].astype(F32)
            for j in range(1, (down, across)[matrix]):
                index = (y + j) % down if matrix == 0 else (x + j) % across
                out[j - 1, r] = own[r, index].astype(BF16)
                second(matrix, r, j).start()

    def final_swap(matrix):
        return remote(
            final.at[matrix, 1 - c], sums.at[c, s, :, pl.ds(matrix * half, half)],
            final_sem.at[0, matrix], final_sem.at[1, matrix], partner,
        )

    def finish(matrix, r):
        with jax.named_scope(f"finish{matrix}{r}"):
            if matrix == 0:
                total = own_a[r, y]
            else:
                total = own_b[r, x]
            for j in range(1, (down, across)[matrix]):
                second(matrix, r, j).wait_recv()
                total = total + (second_in_a, second_in_b)[matrix][j - 1, r].astype(F32)
            final[matrix, r] = total.astype(BF16)
            for k in range(1, across):
                out_x(r, c, matrix, k).start()
            for k in range(1, down):
                out_y(r, c, matrix, k).start()

            @pl.when(c == r)
            def _():
                sums[c, s, :, pl.ds(matrix * half, half)] = final[matrix, r]

            @pl.when(c != r)
            def _():
                final_swap(matrix).start()

    def out_x(core, matrix, part_at, k):
        return remote(
            final.at[part_at, core], sums.at[matrix, s, :, pl.ds(part_at * half, half)],
            out_x_sem.at[0, part_at, core, k - 1], out_x_sem.at[1, part_at, matrix, k - 1],
            (x_peer(k)[0], z * CORES + core),
        )

    def out_y(core, matrix, part_at, k):
        return remote(
            final.at[part_at, core], sums.at[matrix, s, :, pl.ds(part_at * half, half)],
            out_y_sem.at[0, part_at, core, k - 1], out_y_sem.at[1, part_at, matrix, k - 1],
            (y_peer(k)[0], z * CORES + core),
        )

    def onward(matrix, part_at, k, j):
        columns = pl.ds(part_at * half, half)
        if matrix == 0:
            block = sums.at[0, y * across + (x + across - k) % across, :, columns]
            peer = y_peer(j)
        else:
            block = sums.at[1, ((y + down - k) % down) * across + x, :, columns]
            peer = x_peer(j)
        return remote(
            block, block, out_on_sem.at[0, part_at, matrix, k - 1, j - 1],
            out_on_sem.at[1, part_at, matrix, k - 1, j - 1], peer,
        )

    def out_forward(part_at):
        with jax.named_scope(f"forward{part_at}"):
            for k in range(1, across):
                out_x(0, 0, part_at, k).wait_recv()
                for j in range(1, down):
                    onward(0, part_at, k, j).start()
            for k in range(1, down):
                out_y(0, 1, part_at, k).wait_recv()
                for j in range(1, across):
                    onward(1, part_at, k, j).start()

    def out_end(part_at):
        with jax.named_scope(f"end{part_at}"):
            for k in range(1, across):
                out_x(0, 1, part_at, k).wait_recv()
                for j in range(1, down):
                    onward(0, part_at, k, j).wait()
            for k in range(1, down):
                out_y(0, 0, part_at, k).wait_recv()
                for j in range(1, across):
                    onward(1, part_at, k, j).wait()
            final_swap(part_at).wait()
            for matrix in range(2):
                results[2 * part_at + matrix].start()

    def mix_scatter(k):
        return remote(
            mix_low.at[(s + k) % ways], mix_plane.at[k - 1], mix_sem.at[0, k - 1], mix_sem.at[1, k - 1], in_plane(k)
        )

    def small_scatter(k):
        return remote(
            small_plane.at[s], small_plane.at[s], small_sem.at[0, k - 1], small_sem.at[1, k - 1], in_plane(k)
        )

    def mix_lift(k):
        return remote(
            mix_level.at[z], mix_level.at[z], mix_level_sem.at[0, k - 1], mix_level_sem.at[1, k - 1], in_level(k)
        )

    def small_lift(k):
        return remote(
            small_level.at[z], small_level.at[z],
            small_level_sem.at[0, k - 1], small_level_sem.at[1, k - 1], in_level(k),
        )

    def mix_gather(k):
        block = mix_all.at[c, s]
        return remote(block, block, mix_out_sem.at[0, k - 1], mix_out_sem.at[1, k - 1], in_plane(k))

    small_back = remote(small_all.at[c], small_all.at[c], pair_sem.at[0, 2], pair_sem.at[1, 2], partner)
    mix_back = remote(mix_all.at[c], mix_all.at[c], pair_sem.at[0, 5], pair_sem.at[1, 5], partner)

    def mix_stage(stage):
        with jax.named_scope(f"mix{stage}"):
            mix_step(stage)

    def mix_step(stage):
        if stage == 0:
            mix_swap.wait()
            small_swap.wait()
            mine = mix_part[pl.ds(c * per_core, per_core)] + mix_in[...]
            mix_low[...] = mine.reshape(mix_low.shape).astype(BF16)
            small_plane[s] = small[c] + small_in[...]
            for k in range(1, ways):
                mix_scatter(k).start()
                small_scatter(k).start()
        elif stage == 1:
            total = mix_low[s].astype(F32)
            for k in range(1, ways):
                mix_scatter(k).wait()
                small_scatter(k).wait()
                total = total + mix_plane[k - 1].astype(F32)
            mix_level[z] = total.astype(BF16)
            whole = small_plane[0]
            for k in range(1, ways):
                whole = whole + small_plane[k]
            small_level[z] = whole
            for k in range(1, levels):
                mix_lift(k).start()
                small_lift(k).start()
        elif stage == 2:
            for k in range(1, levels):
                mix_lift(k).wait()
                small_lift(k).wait()
            total = mix_level[0].astype(F32)
            whole = small_level[0]
            for k in range(1, levels):
                total = total + mix_level[k].astype(F32)
                whole = whole + small_level[k]
            mix_all[c, s] = total.astype(BF16)
            small_all[c] = whole
            for k in range(1, ways):
                mix_gather(k).start()
        elif stage == 3:
            for k in range(1, ways):
                mix_gather(k).wait()
            mix_back.start()
            small_back.start()
        else:
            mix_back.wait()
            small_back.wait()
            packed_all = mix_all[...].reshape(pairs, block_len, block_len)
            for p in range(pairs):
                packed = packed_all[p].astype(F32)
                on_diagonal = jnp.where(diagonal, small_all[1, pairs + p:pairs + p + 1, :], 0.0)
                mix_ready[2 * p] = jnp.where(causal, packed, 0.0).astype(BF16)
                mix_ready[2 * p + 1] = jnp.where(row > column, packed.T, on_diagonal).astype(BF16)
            results[4].start()
            results[5].start()

    results = [
        pltpu.make_async_copy(
            sums.at[matrix, :, :, pl.ds(part_at * half, half)],
            (value_out, gate_out)[matrix].at[:, :, pl.ds(part_at * half, half)],
            result_sem.at[2 * part_at + matrix],
        )
        for part_at in range(2) for matrix in range(2)
    ] + [
        pltpu.make_async_copy(mix_ready, mix_out, result_sem.at[4]),
        pltpu.make_async_copy(small_all, small_out, result_sem.at[5]),
    ]

    chunks = list(range(levels))
    send_chunk(chunks.pop(0))
    shard_swap.start()
    send_chunk(chunks.pop(0))
    with jax.named_scope("mix_terms"):
        mix_terms()
    arrive(1, 0)
    if chunks:
        send_chunk(chunks.pop(0))
    arrive(1, 1)
    run(0, 0)
    run(0, 1)
    for i in range(1, levels - 1):
        last = i == levels - 2
        if last:
            run(i, 0)
        arrive(i + 1, 0)
        arrive(i + 1, 1)
        if not last:
            run(i, 0)
        if chunks:
            send_chunk(chunks.pop(0))
        run(i, 1)
        if i == 1:
            mix_stage(0)
    with jax.named_scope("project_own"):
        project(z, c)
        shard_swap.wait()
        project(z, 1 - c)
    for k in range(1, levels - 1):
        relay_step(k)
    send_second(0, 0)
    send_second(0, 1)
    send_second(1, 0)
    send_second(1, 1)
    mix_stage(1)
    finish(0, 0)
    finish(0, 1)
    relay_step(levels - 1)
    finish(1, 0)
    finish(1, 1)
    mix_stage(2)
    out_forward(0)
    project_level(0)
    out_forward(1)
    mix_stage(3)
    for i in range(1, levels - 1):
        project_level(i)
    mix_stage(4)
    out_end(0)
    out_end(1)

    send_own(lambda copy: copy.wait_send())
    for i in range(levels - 1):
        level, way, k = nearest(i)
        for matrix in range(2):
            pass_on(level, way, k, matrix, lambda copy: copy.wait_send())
            for j in range(1, (across, down)[matrix]):
                side(level, way, k, matrix, j).wait_send()
        relay(level, way, k).wait_send()
        level, upward = target_of(i)
        for matrix in range(2):
            for r in range(CORES):
                running(i, level, matrix, upward, r, z + 2 * upward - 1).wait_send()
    for matrix in range(2):
        for i in range(levels):
            for k in range(1, (across, down)[matrix]):
                first(i, matrix, k).wait_send()
        for j in range(1, (down, across)[matrix]):
            for r in range(CORES):
                second(matrix, r, j).wait_send()
        for part_at in range(2):
            for k in range(1, across):
                out_x(matrix, 0, part_at, k).wait_send()
            for k in range(1, down):
                out_y(matrix, 0, part_at, k).wait_send()
    with jax.named_scope("stores"):
        for level in range(levels):
            for core in range(CORES):
                store(level, core).wait()
        for copy in results:
            copy.wait()


def write_out(
    input_grad, value_sums, gate_sums, mix_grad, small,
    input_out, value_out, gate_out, mix_out, bias_out, gain_out, shift_out,
    held, value_low, gate_low, mix_low, few, value_full, gate_full, mix_full, load_sem, store_sem,
):
    cuts = held.shape[0]
    tall = held.shape[1]
    groups = bias_out.shape[0]
    pairs = groups // 2
    loads = [
        pltpu.make_async_copy(value_sums, value_low, load_sem.at[0]),
        pltpu.make_async_copy(gate_sums, gate_low, load_sem.at[1]),
        pltpu.make_async_copy(mix_grad, mix_low, load_sem.at[2]),
        pltpu.make_async_copy(small, few, load_sem.at[3]),
    ] + [
        pltpu.make_async_copy(input_grad.at[pl.ds(i * tall, tall)], held.at[i], load_sem.at[4 + i]) for i in range(cuts)
    ]
    stores = [
        pltpu.make_async_copy(value_full, value_out, store_sem.at[0]),
        pltpu.make_async_copy(gate_full, gate_out, store_sem.at[1]),
        pltpu.make_async_copy(mix_full, mix_out, store_sem.at[2]),
        pltpu.make_async_copy(few.at[0, pl.ds(0, groups)], bias_out, store_sem.at[3]),
        pltpu.make_async_copy(few.at[0, pl.ds(groups, pairs)], gain_out, store_sem.at[4]),
        pltpu.make_async_copy(few.at[1, pl.ds(0, pairs)], shift_out, store_sem.at[5]),
    ] + [
        pltpu.make_async_copy(held.at[i], input_out.at[pl.ds(i * tall, tall)], store_sem.at[6 + i]) for i in range(cuts)
    ]
    for copy in loads[4:] + loads[:4]:
        copy.start()
    for i in range(cuts):
        loads[4 + i].wait()
        stores[6 + i].start()
    for i, (low, full) in enumerate(((value_low, value_full), (gate_low, gate_full), (mix_low, mix_full))):
        loads[i].wait()
        full[...] = low[...].reshape(full.shape).astype(F32)
        stores[i].start()
    loads[3].wait()
    for i in range(3, 6):
        stores[i].start()
    for copy in stores:
        copy.wait()


def shards(
    tokens,
    value_act,
    gate_act,
    cotangent,
    value_weight,
    gate_weight,
    norm_gain,
    norm_bias,
    mix_weight,
    mix_bias,
):
    ways = lax.axis_size("sp")
    levels = lax.axis_size("dp") // CORES
    across, down = plane_of(ways)
    inputs = tokens[0]
    seq_len, width = inputs.shape
    channels = value_act.shape[2]
    groups, block_len = mix_weight.shape[0], mix_weight.shape[1]
    pairs = groups // 2
    lanes = channels // pairs
    rows = value_weight.shape[0]
    share = rows // ways
    half = channels // 2
    anywhere = pl.BlockSpec(memory_space=pl.ANY)
    sems = pltpu.SemaphoreType.DMA
    mix_rows = pairs * block_len // (CORES * ways)
    small_shape = (CORES, 3 * pairs, lanes)
    shape = jax.ShapeDtypeStruct
    input_grad, value_sums, gate_sums, mix_out, small = pl.pallas_call(
        functools.partial(kernel, ways, levels),
        out_shape=(
            shape((seq_len, width), BF16),
            shape((ways, share, channels), BF16),
            shape((ways, share, channels), BF16),
            shape((groups, block_len, block_len), BF16),
            shape(small_shape, F32),
        ),
        in_specs=[anywhere] * 10,
        out_specs=(anywhere,) * 5,
        scratch_shapes=[
            pltpu.VMEM((seq_len, width), BF16),
            pltpu.VMEM((seq_len, channels), BF16),
            pltpu.VMEM((seq_len, channels), BF16),
            pltpu.VMEM((seq_len, channels), BF16),
            pltpu.VMEM((1, channels), F32),
            pltpu.VMEM((1, channels), F32),
            pltpu.VMEM((groups, block_len, block_len), BF16),
            pltpu.VMEM((groups, block_len), F32),
            pltpu.VMEM((pairs, 2 * block_len, block_len), BF16),
            pltpu.VMEM((pairs, block_len, 2 * block_len), BF16),
            pltpu.VMEM((block_len, channels), F32),
            pltpu.VMEM((2, seq_len, channels), BF16),
            pltpu.VMEM((seq_len, width), BF16),
            pltpu.VMEM((seq_len, channels), BF16),
            pltpu.VMEM((levels, CORES, 2, rows, channels), BF16),
            pltpu.VMEM((block_len, channels), F32),
            pltpu.VMEM((1, channels), F32),
            pltpu.VMEM((1, channels), F32),
            pltpu.VMEM((seq_len, channels), BF16),
            pltpu.VMEM((seq_len, channels), BF16),
            pltpu.VMEM((block_len, channels), F32),
            pltpu.VMEM((block_len, channels), F32),
            pltpu.VMEM((seq_len, width), BF16),
            pltpu.VMEM((2, width // levels, half), F32),
            pltpu.VMEM((levels, CORES, down, across, share, channels), BF16),
            pltpu.VMEM((levels, across - 1, CORES, down, share, half), BF16),
            pltpu.VMEM((levels, down - 1, CORES, across, share, half), BF16),
            pltpu.VMEM((levels - 1, CORES, down, share, half), BF16),
            pltpu.VMEM((levels, 2, CORES, down, share, half), BF16),
            pltpu.VMEM((levels - 1, CORES, across, share, half), BF16),
            pltpu.VMEM((levels, 2, CORES, across, share, half), BF16),
            pltpu.VMEM((CORES, down, share, half), F32),
            pltpu.VMEM((CORES, across, share, half), F32),
            pltpu.VMEM((down - 1, CORES, share, half), BF16),
            pltpu.VMEM((down - 1, CORES, share, half), BF16),
            pltpu.VMEM((across - 1, CORES, share, half), BF16),
            pltpu.VMEM((across - 1, CORES, share, half), BF16),
            pltpu.VMEM((2, CORES, share, half), BF16),
            pltpu.VMEM((2, ways, share, channels), BF16),
            pltpu.VMEM((pairs, block_len, block_len), F32),
            pltpu.VMEM((pairs // CORES, block_len, block_len), F32),
            pltpu.VMEM((ways, mix_rows, block_len), BF16),
            pltpu.VMEM((ways - 1, mix_rows, block_len), BF16),
            pltpu.VMEM((levels, mix_rows, block_len), BF16),
            pltpu.VMEM((CORES, ways, mix_rows, block_len), BF16),
            pltpu.VMEM((groups, block_len, block_len), BF16),
            pltpu.VMEM(small_shape, F32),
            pltpu.VMEM(small_shape[1:], F32),
            pltpu.VMEM((ways,) + small_shape[1:], F32),
            pltpu.VMEM((levels,) + small_shape[1:], F32),
            pltpu.VMEM(small_shape, F32),
            sems((10,)),
            sems((levels * CORES,)),
            sems((6,)),
            sems((2, levels)),
            sems((2, 6)),
            sems((2, seq_len // block_len)),
            sems((2, 2, levels - 1, 2)),
            sems((2, 2, levels - 1, across - 1)),
            sems((2, 2, levels - 1, down - 1)),
            sems((2, 2, levels - 1)),
            sems((2, levels, across - 1)),
            sems((2, levels, down - 1)),
            sems((2, levels, 2, 2, CORES)),
            sems((2, down - 1, CORES)),
            sems((2, across - 1, CORES)),
            sems((2, 2)),
            sems((2, 2, 2, across - 1)),
            sems((2, 2, 2, down - 1)),
            sems((2, 2, 2, max(across, down) - 1, max(across, down) - 1)),
            sems((2, ways - 1)),
            sems((2, levels - 1)),
            sems((2, ways - 1)),
            sems((2, ways - 1)),
            sems((2, levels - 1)),
        ],
        compiler_params=pltpu.CompilerParams(
            collective_id=0, has_side_effects=True, vmem_limit_bytes=60 * 1024 * 1024
        ),
        name="unit",
    )(
        inputs, value_weight, gate_weight, value_act[0], gate_act[0], cotangent[0],
        norm_gain[None], norm_bias[None], mix_weight, mix_bias,
    )
    cuts = 6
    low_shape, full_shape, mix_full = (ways, share, channels), (rows, channels), (groups, block_len, block_len)
    input_grad, value_grad, gate_grad, mix_grad, bias_grad, gain_grad, shift_grad = pl.pallas_call(
        write_out,
        out_shape=(
            shape((seq_len, width), BF16),
            shape(full_shape, F32),
            shape(full_shape, F32),
            shape(mix_full, F32),
            shape((groups, block_len), F32),
            shape((pairs, lanes), F32),
            shape((pairs, lanes), F32),
        ),
        in_specs=[anywhere] * 5,
        out_specs=(anywhere,) * 7,
        scratch_shapes=[
            pltpu.VMEM((cuts, seq_len // cuts, width), BF16),
            pltpu.VMEM(low_shape, BF16),
            pltpu.VMEM(low_shape, BF16),
            pltpu.VMEM(mix_full, BF16),
            pltpu.VMEM(small_shape, F32),
            pltpu.VMEM(full_shape, F32),
            pltpu.VMEM(full_shape, F32),
            pltpu.VMEM(mix_full, F32),
            sems((4 + cuts,)),
            sems((6 + cuts,)),
        ],
        name="write_out",
    )(input_grad, value_sums, gate_sums, mix_out, small)
    return (
        input_grad[None],
        value_grad,
        gate_grad,
        mix_grad,
        bias_grad,
        gain_grad.reshape(-1),
        shift_grad.reshape(-1),
    )


def solution(mesh):
    placed = (
        P("dp", "sp", None),
        P("dp", "sp", None),
        P("dp", "sp", None),
        P("dp", "sp", None),
        P("dp", None),
        P("dp", None),
        P(),
        P(),
        P(),
        P(),
    )
    return jax.shard_map(
        shards,
        mesh=mesh,
        in_specs=placed,
        out_specs=(P("dp", "sp", None), P("dp", None), P("dp", None), P(), P(), P(), P()),
        check_vma=False,
    )
```
